512 devices in a mesh: sp: 16 (over z), tp: 32 (over y, x, core).
Axes of the slice: x: 4, y: 4, z: 16, core: 2. Of those that a mesh axis runs over, the one named last changes fastest.
Arguments:
- target_rows: bfloat16 [3072, 2048], P(('sp', 'tp')), may hold values from -6 to 6
- source_rows: bfloat16 [16384, 2048], P(('sp', 'tp')), may hold values from -6 to 6
- target_gain: float32 [2048], replicated, may hold values from 0.55 to 9
- source_gain: float32 [2048], replicated, may hold values from 0.55 to 9
- query_weight: bfloat16 [2048, 2048], P(None, 'tp'), may hold values from -0.125 to 0.125
- key_weight: bfloat16 [2048, 512], P('tp'), may hold values from -0.125 to 0.125
- value_weight: bfloat16 [2048, 512], P('tp'), may hold values from -0.125 to 0.125
- out_weight: bfloat16 [2048, 2048], P('tp'), may hold values from -0.125 to 0.125
- out_cotangent: bfloat16 [3072, 2048], P(('sp', 'tp')), may hold values from -6 to 6
Outputs:
- target_grad: float32 [3072, 2048], P(('sp', 'tp'))
- source_grad: float32 [16384, 2048], P(('sp', 'tp'))
- out_weight_grad: float32 [2048, 2048], P('tp')
The draws below stay inside these ranges and needn't reach their ends.
All inputs are finite; a program needn't handle non-finite values.
Results may differ from the reference program's by a relative error of at most 0.03.
Values may be sent and summed in bfloat16 or wider, within the bound.
A program may use at most 64 MiB of HBM per device.

```python
import jax
import jax.numpy as jnp
from jax import lax

D = 2048
HEADS = 32
HEAD_DIM = 64
KV_HEADS = 8
TGT_ALL = 3072
SRC_ALL = 16384


def gain_draw(seed_key):
    return 1.0 + 0.18 * jax.random.truncated_normal(seed_key, -2.5, 2.5, (D,), jnp.float32)


def draw_target_gain(key, part):
    return gain_draw(jax.random.fold_in(key, 11))


def draw_source_gain(key, part):
    return gain_draw(jax.random.fold_in(key, 23))


def steps_of(key, extent, cuts, least, largest):
    level = 1.0
    for axis_at, blocks in cuts:
        heights = jax.random.uniform(jax.random.fold_in(jax.random.fold_in(key, 6), axis_at), (blocks,), jnp.float32, least / len(cuts), largest / len(cuts))
        level = level * jnp.repeat(jnp.exp(heights), extent[axis_at] // blocks).reshape((-1,) + (1,) * (len(extent) - 1 - axis_at))
    return level


def scatter_about(key, extent, spread, bound, shards=(), kind=jnp.bfloat16):
    drawn = jax.random.normal(key, extent, jnp.float32) * spread
    if len(shards) > 0:
        drawn = steps_of(key, extent, shards, -0.22, 0.18) * drawn
    return jnp.clip(drawn, min=-bound, max=bound).astype(kind)


def setup_inputs(seed: int = 0) -> dict:
    streams_of = jax.random.split(jax.random.key(seed), 10)
    return {
        "target_rows": scatter_about(streams_of[0], (TGT_ALL, D), 1.0, 6.0, ((0, 512),)),
        "source_rows": scatter_about(streams_of[1], (SRC_ALL, D), 1.0, 6.0, ((0, 512),)),
        "target_gain": draw_target_gain(jax.random.fold_in(streams_of[9], 71), 0),
        "source_gain": draw_source_gain(jax.random.fold_in(streams_of[9], 71), 0),
        "query_weight": scatter_about(streams_of[4], (D, HEADS * HEAD_DIM), D ** -0.5, 0.125, ((1, 32),)),
        "key_weight": scatter_about(streams_of[5], (D, KV_HEADS * HEAD_DIM), D ** -0.5, 0.125, ((0, 32),)),
        "value_weight": scatter_about(streams_of[6], (D, KV_HEADS * HEAD_DIM), D ** -0.5, 0.125, ((0, 32),)),
        "out_weight": scatter_about(streams_of[7], (HEADS * HEAD_DIM, D), (HEADS * HEAD_DIM) ** -0.5, 0.125, ((0, 32),)),
        "out_cotangent": scatter_about(streams_of[8], (TGT_ALL, D), 1.0, 6.0, ((0, 512),)),
    }


EPSILON = 1e-06

def normalize(matrix, gain_vector):
    widened = matrix.astype(jnp.float32)
    factor = lax.rsqrt(lax.optimization_barrier(jnp.mean(widened * widened, axis=-1, keepdims=True)) + EPSILON)
    return (widened * factor * gain_vector).astype(jnp.bfloat16)

def norm_back(matrix, gain_vector, upstream):
    widened = matrix.astype(jnp.float32)
    factor = lax.rsqrt(lax.optimization_barrier(jnp.mean(widened * widened, axis=-1, keepdims=True)) + EPSILON)
    weighted = upstream * gain_vector
    inner_sum = lax.optimization_barrier(jnp.mean(weighted * widened, axis=-1, keepdims=True))
    return factor * weighted - widened * factor ** 3 * inner_sum

def reference(target_rows, source_rows, target_gain, source_gain, query_weight, key_weight, value_weight, out_weight, out_cotangent):
    score_scale = HEAD_DIM ** (-0.5)
    group_size = HEADS // KV_HEADS
    normed_t = normalize(target_rows, target_gain)
    normed_s = normalize(source_rows, source_gain)
    queries = jnp.dot(normed_t, query_weight, preferred_element_type=jnp.float32).astype(jnp.bfloat16)
    keys_all = jnp.dot(normed_s, key_weight, preferred_element_type=jnp.float32).astype(jnp.bfloat16)
    values_all = jnp.dot(normed_s, value_weight, preferred_element_type=jnp.float32).astype(jnp.bfloat16)
    query_heads = queries.reshape(TGT_ALL, HEADS, HEAD_DIM).transpose(1, 0, 2)
    key_heads = keys_all.reshape(SRC_ALL, KV_HEADS, HEAD_DIM).transpose(1, 0, 2)
    value_heads = values_all.reshape(SRC_ALL, KV_HEADS, HEAD_DIM).transpose(1, 0, 2)
    out_heads = out_weight.reshape(HEADS, HEAD_DIM, D)

    def one_head(head_index):
        query = query_heads[head_index]
        key_head = key_heads[head_index // group_size]
        value_head = value_heads[head_index // group_size]
        scores = jnp.dot(query, key_head.T, preferred_element_type=jnp.float32) * score_scale
        row_max = lax.optimization_barrier(jnp.max(scores, axis=1, keepdims=True))
        weights = jnp.exp(scores - row_max)
        total = lax.optimization_barrier(jnp.sum(weights, axis=1, keepdims=True))
        attended = (jnp.dot(weights.astype(jnp.bfloat16), value_head, preferred_element_type=jnp.float32) / total).astype(jnp.bfloat16)
        log_total = row_max + jnp.log(total)
        d_attended = jnp.dot(out_cotangent, out_heads[head_index].T, preferred_element_type=jnp.float32).astype(jnp.bfloat16)
        delta = lax.optimization_barrier(jnp.sum(d_attended.astype(jnp.float32) * attended.astype(jnp.float32), axis=1, keepdims=True))
        probs = jnp.exp(scores - log_total)
        d_value = jnp.dot(probs.astype(jnp.bfloat16).T, d_attended, preferred_element_type=jnp.float32)
        d_probs = jnp.dot(d_attended, value_head.T, preferred_element_type=jnp.float32)
        d_scores = (probs * (d_probs - delta)).astype(jnp.bfloat16)
        d_query = jnp.dot(d_scores, key_head, preferred_element_type=jnp.float32) * score_scale
        d_key = jnp.dot(d_scores.T, query, preferred_element_type=jnp.float32) * score_scale
        return (attended, d_query, d_key, d_value)
    attended, d_query, d_key, d_value = lax.map(one_head, jnp.arange(HEADS))
    key_sum = lax.optimization_barrier(jnp.sum(d_key.reshape(KV_HEADS, group_size, SRC_ALL, HEAD_DIM), axis=1))
    value_sum = lax.optimization_barrier(jnp.sum(d_value.reshape(KV_HEADS, group_size, SRC_ALL, HEAD_DIM), axis=1))
    key_grad = key_sum.transpose(1, 0, 2).reshape(SRC_ALL, KV_HEADS * HEAD_DIM).astype(jnp.bfloat16)
    value_grad = value_sum.transpose(1, 0, 2).reshape(SRC_ALL, KV_HEADS * HEAD_DIM).astype(jnp.bfloat16)
    attended_rows = attended.transpose(1, 0, 2).reshape(TGT_ALL, HEADS * HEAD_DIM)
    query_grad = d_query.transpose(1, 0, 2).reshape(TGT_ALL, HEADS * HEAD_DIM).astype(jnp.bfloat16)
    out_weight_grad = jnp.dot(attended_rows.T, out_cotangent, preferred_element_type=jnp.float32)
    d_normed_t = jnp.dot(query_grad, query_weight.T, preferred_element_type=jnp.float32)
    target_grad = out_cotangent.astype(jnp.float32) + norm_back(target_rows, target_gain, d_normed_t)
    d_normed_s = jnp.dot(key_grad, key_weight.T, preferred_element_type=jnp.float32) + jnp.dot(value_grad, value_weight.T, preferred_element_type=jnp.float32)
    source_grad = norm_back(source_rows, source_gain, d_normed_s)
    return (target_grad, source_grad, out_weight_grad)
```

```python
import functools

import jax
import jax.numpy as jnp
from jax import lax
from jax.experimental import pallas as pl
from jax.experimental.pallas import tpu as pltpu
from jax.sharding import Mesh
from jax.sharding import PartitionSpec as P

MESH = pl.DeviceIdType.MESH
HD = 64
EPSILON = 1e-06
F32, BF16 = jnp.float32, jnp.bfloat16
VMEM = pl.BlockSpec(memory_space=pltpu.VMEM)
SIZES = {"y": 4, "x": 4, "c": 2}
PIECES = 2


def dma(n):
    return pltpu.SemaphoreType.DMA((n,))


def params(cid):
    return pltpu.CompilerParams(
        collective_id=cid, has_side_effects=True, vmem_limit_bytes=62 * 1024 * 1024
    )


def group_size(axes):
    n = 1
    for a in axes:
        n *= SIZES[a]
    return n


def group_index(axes):
    i = 0
    for a in axes:
        i = i * SIZES[a] + lax.axis_index(a)
    return i


def coords_of(index, axes):
    out = {}
    for a in reversed(axes):
        out[a] = lax.rem(index, SIZES[a])
        index = index // SIZES[a]
    return out


def greet(axes):
    n, me = group_size(axes), group_index(axes)
    sem = pltpu.get_barrier_semaphore()

    def one(k, carry):
        pl.semaphore_signal(
            sem, inc=1, device_id=coords_of(lax.rem(me + k, n), axes), device_id_type=MESH
        )
        return carry

    lax.fori_loop(1, n, one, 0)
    return n - 1


def greeted(count):
    pl.semaphore_wait(pltpu.get_barrier_semaphore(), count)


class Exchange:
    def __init__(self, axes, src, dst, send, recv, pick=None):
        self.axes, self.src, self.dst, self.send, self.recv = axes, src, dst, send, recv
        self.n, self.me = group_size(axes), group_index(axes)
        self.pick = pick

    def block(self, index):
        if self.pick is None:
            return self.src
        return self.src.at[self.pick(coords_of(index, self.axes), index)]

    def copy(self, k, slot):
        to = lax.rem(self.me + k, self.n)
        return pltpu.make_async_remote_copy(
            src_ref=self.block(to),
            dst_ref=self.dst.at[slot],
            send_sem=self.send.at[k],
            recv_sem=self.recv.at[k],
            device_id=coords_of(to, self.axes),
            device_id_type=MESH,
        )

    def start(self):
        def one(k, carry):
            self.copy(k, self.me).start()
            return carry

        lax.fori_loop(1, self.n, one, 0)
        self.dst[self.me] = self.block(self.me)[...]

    def arrive(self):
        def one(k, carry):
            self.copy(k, lax.rem(self.me + self.n - k, self.n)).wait_recv()
            return carry

        lax.fori_loop(1, self.n, one, 0)

    def drain(self):
        def one(k, carry):
            self.copy(k, self.me).wait_send()
            return carry

        lax.fori_loop(1, self.n, one, 0)


def gather_kernel(rows, weights, pair, targets, kv, w_all, pair_all, t_all, *scratch):
    rows_all, part, part_all, rs, rr, ws, wr, ps, pr, ts, tr, ds, dr = scratch
    seen = greet(("y", "x", "c"))
    greeted(seen)
    by_rows = Exchange(("y", "c"), rows, rows_all, rs, rr, lambda at, i: at["c"])
    by_w = Exchange(("y", "x"), weights, w_all, ws, wr, lambda at, i: at["y"])
    by_t = Exchange(("y", "x"), targets, t_all, ts, tr)
    by_pair = Exchange(("c",), pair, pair_all, ps, pr)
    for e in (by_rows, by_w, by_t, by_pair):
        e.start()
    by_w.arrive()
    by_rows.arrive()
    left = rows_all[...].reshape(256, 1024)
    right = w_all[...].reshape(1024, 256)
    both = jnp.dot(left, right, preferred_element_type=F32)
    part[0] = both[:, :128]
    part[1] = both[:, 128:]
    by_part = Exchange(("c",), part, part_all, ds, dr, lambda at, i: i)
    by_part.start()
    by_part.arrive()
    kv[...] = (part_all[0] + part_all[1]).astype(BF16)
    by_t.arrive()
    by_pair.arrive()
    for e in (by_rows, by_w, by_t, by_pair, by_part):
        e.drain()


def gather(rows, weights, pair, targets):
    return pl.pallas_call(
        gather_kernel,
        out_shape=(
            jax.ShapeDtypeStruct((256, 128), BF16),
            jax.ShapeDtypeStruct((16, 64, 256), BF16),
            jax.ShapeDtypeStruct((2, 2, 64, 2048), BF16),
            jax.ShapeDtypeStruct((16, 16, 2048), BF16),
        ),
        in_specs=[VMEM] * 4,
        out_specs=(VMEM,) * 4,
        scratch_shapes=[
            pltpu.VMEM((8, 32, 1024), BF16),
            pltpu.VMEM((2, 256, 128), F32),
            pltpu.VMEM((2, 256, 128), F32),
            dma(8), dma(8), dma(16), dma(16), dma(2), dma(2), dma(16), dma(16), dma(2), dma(2),
        ],
        compiler_params=params(0),
    )(rows, weights, pair, targets)


class ToReaders:
    def __init__(self, src, dst, send, recv):
        self.src, self.dst, self.send, self.recv = src, dst, send, recv
        self.y, self.x, self.c = (lax.axis_index(a) for a in "yxc")
        self.mine = self.x // 2 == self.c

    def copy(self, k, slot):
        return pltpu.make_async_remote_copy(
            src_ref=self.src,
            dst_ref=self.dst.at[slot],
            send_sem=self.send.at[k],
            recv_sem=self.recv.at[slot],
            device_id={"x": lax.rem(self.x + k, 4), "c": self.x // 2},
            device_id_type=MESH,
        )

    def slot(self):
        return lax.rem(self.x, 2) * 2 + self.c

    def start(self):
        for k in range(1, 4):
            self.copy(k, self.slot()).start()

        @pl.when(jnp.logical_not(self.mine))
        def _():
            self.copy(0, self.slot()).start()

        @pl.when(self.mine)
        def _():
            self.dst[self.slot()] = self.src[...]

    def arrive(self):
        for s in range(4):
            own = jnp.logical_and(2 * self.c + s // 2 == self.x, self.c == s % 2)

            @pl.when(jnp.logical_not(own))
            def _():
                self.copy(1, s).wait_recv()

    def drain(self):
        for k in range(1, 4):
            self.copy(k, self.slot()).wait_send()

        @pl.when(jnp.logical_not(self.mine))
        def _():
            self.copy(0, self.slot()).wait_send()


class ToOwners:
    def __init__(self, src, dst, send, recv):
        self.src, self.dst, self.send, self.recv = src, dst, send, recv
        self.y, self.x, self.c = (lax.axis_index(a) for a in "yxc")

    def copy(self, s, slot):
        return pltpu.make_async_remote_copy(
            src_ref=self.src.at[s],
            dst_ref=self.dst.at[slot],
            send_sem=self.send.at[s],
            recv_sem=self.recv.at[slot],
            device_id={"x": 2 * self.c + s // 2, "c": jnp.int32(s % 2)},
            device_id_type=MESH,
        )

    def own(self, s):
        return jnp.logical_and(2 * self.c + s // 2 == self.x, self.c == s % 2)

    def start(self):
        for s in range(4):
            @pl.when(jnp.logical_not(self.own(s)))
            def _():
                self.copy(s, self.x).start()

            @pl.when(self.own(s))
            def _():
                self.dst[self.x] = self.src[s]

    def arrive(self):
        for j in range(4):
            own = jnp.logical_and(self.x == j, self.x // 2 == self.c)

            @pl.when(jnp.logical_not(own))
            def _():
                self.copy(0, j).wait_recv()

    def drain(self):
        for s in range(4):
            @pl.when(jnp.logical_not(self.own(s)))
            def _():
                self.copy(s, self.x).wait_send()


def readers_kernel(block, out, send, recv):
    greeted(greet(("x", "c")))
    e = ToReaders(block, out, send, recv)
    e.start()
    e.arrive()
    e.drain()


def to_readers(block):
    return pl.pallas_call(
        readers_kernel,
        out_shape=jax.ShapeDtypeStruct((4, *block.shape), block.dtype),
        in_specs=[VMEM],
        out_specs=VMEM,
        scratch_shapes=[dma(4), dma(4)],
        compiler_params=params(1),
    )(block)


def owners_kernel(a, b, a_out, b_out, a_send, a_recv, b_send, b_recv):
    greeted(greet(("x", "c")))
    both = (ToOwners(a, a_out, a_send, a_recv), ToOwners(b, b_out, b_send, b_recv))
    for e in both:
        e.start()
    for e in both:
        e.arrive()
    for e in both:
        e.drain()


def to_owners(a, b):
    return pl.pallas_call(
        owners_kernel,
        out_shape=(jax.ShapeDtypeStruct(a.shape, a.dtype), jax.ShapeDtypeStruct(b.shape, b.dtype)),
        in_specs=[VMEM, VMEM],
        out_specs=(VMEM, VMEM),
        scratch_shapes=[dma(4)] * 4,
        compiler_params=params(3),
    )(a, b)


def lanes_below(shape, bound):
    return lax.broadcasted_iota(jnp.int32, shape, 1) < bound


def contract(a, b, da, db):
    return lax.dot_general(a, b, (((da,), (db,)), ((), ())), preferred_element_type=F32)


def ring_greet(nz):
    z = lax.axis_index("z")
    sem = pltpu.get_barrier_semaphore()
    right, left = lax.rem(z + 1, nz), lax.rem(z + nz - 1, nz)
    for to in (left, right):
        pl.semaphore_signal(sem, inc=1, device_id={"z": to}, device_id_type=MESH)
    return 2


def forward_kernel(nz, qa, kv, kv_all, stats, out, m, l, o, said, heard, rs, rr, ls, lr, ss, sr):
    z = lax.axis_index("z")
    right, left = lax.rem(z + 1, nz), lax.rem(z + nz - 1, nz)
    greeted(ring_greet(nz) + greet(("x",)))
    steps_r = nz // 2
    steps_l = nz - 1 - steps_r
    piece = 256 // PIECES
    kv_all[z] = kv[...]

    def hop(step, p, sign):
        at = lax.rem(z + nz - sign * step, nz)
        ssem, rsem = (rs, rr) if sign > 0 else (ls, lr)
        src = kv_all.at[at, pl.ds(p * piece, piece)]
        return pltpu.make_async_remote_copy(
            src_ref=src,
            dst_ref=src,
            send_sem=ssem.at[step, p],
            recv_sem=rsem.at[step, p],
            device_id={"z": right if sign > 0 else left},
            device_id_type=MESH,
        )

    def landed(step, p, sign):
        at = lax.rem(z + nz - sign * (step + 1), nz)
        ssem, rsem = (rs, rr) if sign > 0 else (ls, lr)
        dst = kv_all.at[at, pl.ds(p * piece, piece)]
        return pltpu.make_async_remote_copy(
            src_ref=dst,
            dst_ref=dst,
            send_sem=ssem.at[step, p],
            recv_sem=rsem.at[step, p],
            device_id={"z": right if sign > 0 else left},
            device_id_type=MESH,
        )

    for p in range(PIECES):
        hop(0, p, 1).start()
        hop(0, p, -1).start()
    m[...] = jnp.full(m.shape, -1e30, F32)
    l[...] = jnp.zeros(l.shape, F32)
    o[...] = jnp.zeros(o.shape, F32)

    def attend(at):
        block = kv_all[at]
        keys = jnp.where(lanes_below(block.shape, HD), block, jnp.zeros_like(block))
        scores = contract(keys, qa[...], 1, 1)
        top = jnp.maximum(m[...], jnp.max(scores, axis=0, keepdims=True))
        weights = jnp.exp(scores - top)
        old = jnp.exp(m[...] - top)
        m[...] = top
        l[...] = l[...] * old + jnp.sum(weights, axis=0, keepdims=True)
        o[...] = o[...] * old + contract(block, weights.astype(BF16), 0, 0)[HD:]

    attend(z)

    def step(s, carry):
        for p in range(PIECES):
            landed(s - 1, p, 1).wait_recv()
            hop(s, p, 1).start()
            landed(s - 1, p, -1).wait_recv()

            @pl.when(s < steps_l)
            def _():
                hop(s, p, -1).start()

        attend(lax.rem(z + nz - s, nz))
        attend(lax.rem(z + s, nz))
        return carry

    lax.fori_loop(1, steps_r, step, 0)
    for p in range(PIECES):
        landed(steps_r - 1, p, 1).wait_recv()
    attend(lax.rem(z + nz - steps_r, nz))
    upright = jnp.transpose(qa[...].astype(F32))
    delta = jnp.sum(upright[HD:] * o[...], axis=0, keepdims=True)
    row = lax.broadcasted_iota(jnp.int32, (8, qa.shape[0]), 0)
    said[...] = jnp.where(row == 0, m[...], jnp.where(row == 1, l[...], delta))
    e = Exchange(("x",), said, heard, ss, sr)
    e.start()
    e.arrive()
    top = jnp.max(heard[:, 0:1], axis=0)
    total = jnp.zeros_like(top)
    both = jnp.zeros_like(top)
    for j in range(4):
        w = jnp.exp(heard[j, 0:1] - top)
        total = total + w * heard[j, 1:2]
        both = both + w * heard[j, 2:3]
    stats[...] = jnp.where(row == 0, top + jnp.log(total), both / total)
    scaled = o[...] * (jnp.exp(m[...] - top) / total)
    out[...] = jnp.transpose(jnp.concatenate([scaled, jnp.zeros_like(scaled)], axis=0)).astype(BF16)
    e.drain()

    def drain(s, carry):
        for p in range(PIECES):
            hop(s, p, 1).wait_send()

            @pl.when(s < steps_l)
            def _():
                hop(s, p, -1).wait_send()

        return carry

    lax.fori_loop(0, steps_r, drain, 0)


def forward(qa, kv, nz):
    t = qa.shape[0]
    sems = pltpu.SemaphoreType.DMA((nz // 2, PIECES))
    return pl.pallas_call(
        functools.partial(forward_kernel, nz),
        out_shape=(
            jax.ShapeDtypeStruct((nz, 256, 128), BF16),
            jax.ShapeDtypeStruct((8, t), F32),
            jax.ShapeDtypeStruct((t, 128), BF16),
        ),
        in_specs=[VMEM, VMEM],
        out_specs=(VMEM,) * 3,
        scratch_shapes=[
            pltpu.VMEM((1, t), F32),
            pltpu.VMEM((1, t), F32),
            pltpu.VMEM((HD, t), F32),
            pltpu.VMEM((8, t), F32),
            pltpu.VMEM((4, 8, t), F32),
            sems, sems, sems, sems, dma(4), dma(4),
        ],
        compiler_params=params(2),
    )(qa, kv)


def backward_kernel(nz, qa, kv_all, stats, kv_grad, q_grad, dq, own, tor, tol, inr, inl, rs, rr, ls, lr):
    z = lax.axis_index("z")
    right, left = lax.rem(z + 1, nz), lax.rem(z + nz - 1, nz)
    greeted(ring_greet(nz))
    steps_l = nz // 2
    steps_r = nz - 1 - steps_l
    piece = 256 // PIECES
    dq[...] = jnp.zeros(dq.shape, F32)

    def grads(at):
        block = kv_all[at]
        low = lanes_below(block.shape, HD)
        none = jnp.zeros_like(block)
        scores = contract(jnp.where(low, block, none), qa[...], 1, 1)
        probs = jnp.exp(scores - stats[0:1])
        d_probs = contract(jnp.where(low, none, block), qa[...], 1, 1)
        d_scores = (probs * (d_probs - stats[1:2])).astype(BF16)
        for_v = contract(probs.astype(BF16), qa[...], 1, 0)
        for_k = contract(d_scores, qa[...], 1, 0)
        dq[...] += contract(block, d_scores, 0, 0)[:HD]
        return jnp.where(lanes_below(for_k.shape, HD), for_k, for_v)

    def hop(s, p, sign):
        ssem, rsem = (rs, rr) if sign > 0 else (ls, lr)
        src, dst = (tor, inr) if sign > 0 else (tol, inl)
        return pltpu.make_async_remote_copy(
            src_ref=src.at[s, pl.ds(p * piece, piece)],
            dst_ref=dst.at[s, pl.ds(p * piece, piece)],
            send_sem=ssem.at[s, p],
            recv_sem=rsem.at[s, p],
            device_id={"z": right if sign > 0 else left},
            device_id_type=MESH,
        )

    def send_first(sign, value):
        ref = tor if sign > 0 else tol
        ref[0] = value.astype(BF16)
        for p in range(PIECES):
            hop(0, p, sign).start()

    def send_on(s, sign):
        ref, arrived = (tor, inr) if sign > 0 else (tol, inl)
        for p in range(PIECES):
            hop(s - 1, p, sign).wait_recv()
            at = pl.ds(p * piece, piece)
            ref[s, at] = (arrived[s - 1, at].astype(F32) + own[at]).astype(BF16)
            hop(s, p, sign).start()

    send_first(-1, grads(lax.rem(z + nz - steps_l, nz)))
    send_first(1, grads(lax.rem(z + steps_r, nz)))

    def step(s, carry):
        own[...] = grads(lax.rem(z + nz - steps_l + s, nz))
        send_on(s, -1)

        @pl.when(s < steps_r)
        def _():
            own[...] = grads(lax.rem(z + steps_r - s, nz))
            send_on(s, 1)

        return carry

    lax.fori_loop(1, steps_l, step, 0)
    own[...] = grads(z)
    q_grad[...] = jnp.transpose(
        jnp.concatenate([dq[...], jnp.zeros_like(dq[...])], axis=0)
    ).astype(BF16)
    for p in range(PIECES):
        at = pl.ds(p * piece, piece)
        hop(steps_l - 1, p, -1).wait_recv()
        hop(steps_r - 1, p, 1).wait_recv()
        kv_grad[at] = (
            inl[steps_l - 1, at].astype(F32) + inr[steps_r - 1, at].astype(F32) + own[at]
        ).astype(BF16)

    def drain(s, carry):
        for p in range(PIECES):
            hop(s, p, -1).wait_send()

            @pl.when(s < steps_r)
            def _():
                hop(s, p, 1).wait_send()

        return carry

    lax.fori_loop(0, steps_l, drain, 0)


def backward(qa, kv_all, stats, nz):
    t = qa.shape[0]
    half = nz // 2
    sems = pltpu.SemaphoreType.DMA((half, PIECES))
    return pl.pallas_call(
        functools.partial(backward_kernel, nz),
        out_shape=(
            jax.ShapeDtypeStruct((256, 128), BF16),
            jax.ShapeDtypeStruct((t, 128), BF16),
        ),
        in_specs=[VMEM] * 3,
        out_specs=(VMEM,) * 2,
        scratch_shapes=[
            pltpu.VMEM((HD, t), F32),
            pltpu.VMEM((256, 128), F32),
            pltpu.VMEM((half, 256, 128), BF16),
            pltpu.VMEM((half, 256, 128), BF16),
            pltpu.VMEM((half, 256, 128), BF16),
            pltpu.VMEM((half, 256, 128), BF16),
            sems, sems, sems, sems,
        ],
        compiler_params=params(4),
    )(qa, kv_all, stats)


def last_kernel(kv_grad, w_all, d_target, s_out, t_out, *scratch):
    grads, parts, ps, pr, ss, sr, ts, tr = scratch
    greeted(greet(("y", "x", "c")))
    by_pair = Exchange(("c",), kv_grad, grads, ps, pr)
    by_pair.start()
    by_t = Exchange(("y", "x"), d_target, t_out, ts, tr, lambda at, i: i)
    by_t.start()
    by_pair.arrive()
    right = w_all[...].reshape(1024, 256)
    d_rows = contract(grads[0], right[:, :128], 1, 1) + contract(grads[1], right[:, 128:], 1, 1)
    parts[...] = d_rows.astype(BF16).reshape(8, 32, 1024)
    by_s = Exchange(("y", "c"), parts, s_out, ss, sr, lambda at, i: i)
    by_s.start()
    by_t.arrive()
    by_s.arrive()
    for e in (by_pair, by_t, by_s):
        e.drain()


def last(kv_grad, w_all, d_target):
    return pl.pallas_call(
        last_kernel,
        out_shape=(
            jax.ShapeDtypeStruct((8, 32, 1024), BF16),
            jax.ShapeDtypeStruct(d_target.shape, BF16),
        ),
        in_specs=[VMEM] * 3,
        out_specs=(VMEM,) * 2,
        scratch_shapes=[
            pltpu.VMEM((2, 256, 128), BF16),
            pltpu.VMEM((8, 32, 1024), BF16),
            dma(2), dma(2), dma(8), dma(8), dma(16), dma(16),
        ],
        compiler_params=params(5),
    )(kv_grad, w_all, d_target)


def total_kernel(nz, part, out, halves, terms, sums, all_sums, mine_sum, cs, cr, ss, sr, gs, gr):
    greeted(greet(("c",)) + greet(("z",)))
    swap = Exchange(("c",), part, halves, cs, cr, lambda at, i: i)
    swap.start()
    swap.arrive()
    terms[...] = (halves[0].astype(F32) + halves[1].astype(F32)).astype(BF16)
    by_z = Exchange(("z",), terms, sums, ss, sr, lambda at, i: i)
    by_z.start()
    by_z.arrive()
    mine = jnp.zeros(sums.shape[1:], F32)
    for i in range(nz):
        mine = mine + sums[i].astype(F32)
    mine_sum[...] = mine.astype(BF16)
    back = Exchange(("z",), mine_sum, all_sums, gs, gr)
    back.start()
    back.arrive()
    out[...] = all_sums[...].astype(F32)
    for e in (swap, by_z, back):
        e.drain()


def total(part, nz):
    shape = part.shape[1:]
    return pl.pallas_call(
        functools.partial(total_kernel, nz),
        out_shape=jax.ShapeDtypeStruct(shape, F32),
        in_specs=[VMEM],
        out_specs=VMEM,
        scratch_shapes=[
            pltpu.VMEM((2, *shape), BF16),
            pltpu.VMEM(shape, BF16),
            pltpu.VMEM(shape, BF16),
            pltpu.VMEM(shape, BF16),
            pltpu.VMEM(shape[1:], BF16),
            dma(2), dma(2), dma(nz), dma(nz), dma(nz), dma(nz),
        ],
        compiler_params=params(6),
    )(part)


def normalize(matrix, gain):
    wide = matrix.astype(F32)
    factor = lax.rsqrt(jnp.mean(wide * wide, axis=-1, keepdims=True) + EPSILON)
    return (wide * factor * gain).astype(BF16)


def norm_back(matrix, gain, upstream):
    wide = matrix.astype(F32)
    factor = lax.rsqrt(jnp.mean(wide * wide, axis=-1, keepdims=True) + EPSILON)
    weighted = upstream * gain
    inner = jnp.mean(weighted * wide, axis=-1, keepdims=True)
    return factor * weighted - wide * factor**3 * inner


def pad_rows(a, rows):
    return jnp.pad(a, ((0, rows - a.shape[0]), (0, 0)))


def body(nz, target_rows, source_rows, t_gain, s_gain, wq, wk, wv, wo, cot):
    normed_s = normalize(source_rows, s_gain)
    normed_t = normalize(target_rows, t_gain)
    rows = normed_s.reshape(32, 16, 2, 64).transpose(2, 0, 1, 3).reshape(2, 32, 1024)
    weights = jnp.stack([wk.reshape(64, 4, 2, 64), wv.reshape(64, 4, 2, 64)], axis=3)
    weights = weights.transpose(1, 0, 2, 3, 4).reshape(4, 64, 256)
    pair = jnp.stack([wq.T, wo])
    targets = jnp.concatenate([pad_rows(normed_t, 8), pad_rows(cot, 8)])
    kv, w_all, pair_all, t_all = gather(rows, weights, pair, targets)
    wq2 = pair_all[:, 0].reshape(128, 2048)
    wo2 = pair_all[:, 1].reshape(128, 2048)
    t_all = t_all.reshape(16, 2, 8, 2048)
    normed2 = t_all[:, 0].reshape(128, 2048)
    cot2 = t_all[:, 1].reshape(128, 2048)

    def six(a):
        return a.reshape(16, 8, 2, HD)[:, :6].reshape(96, 2, HD).transpose(1, 0, 2)

    q2 = six((contract(normed2, wq2, 1, 1)).astype(BF16) * jnp.asarray(HD**-0.5, BF16))
    da2 = six(contract(cot2, wo2, 1, 1).astype(BF16))
    qa = to_readers(jnp.concatenate([q2, da2], axis=-1).reshape(192, 128)).reshape(768, 128)
    kv_all, stats, out = forward(qa, kv, nz)
    kv_grad, q_grad = backward(qa, kv_all, stats, nz)
    outs, q_grads = to_owners(out.reshape(4, 192, 128), q_grad.reshape(4, 192, 128))

    def pair_of(a):
        s = jnp.sum(a.astype(F32), axis=0)[:, :HD].reshape(2, 96, HD)
        return s.transpose(1, 0, 2).reshape(96, 128)

    attended = pair_of(outs).astype(BF16)
    query_grad = (pair_of(q_grads) * HD**-0.5).astype(BF16)
    padded = jnp.pad(attended.reshape(16, 6, 128), ((0, 0), (0, 2), (0, 0))).reshape(128, 128)
    o_part = contract(padded, cot2, 0, 0)
    d_target = jnp.dot(query_grad, wq2, preferred_element_type=F32).astype(BF16)
    d_target = jnp.pad(d_target.reshape(16, 6, 2048), ((0, 0), (0, 2), (0, 0)))
    s_back, t_back = last(kv_grad, w_all, d_target)
    d_normed_s = jnp.sum(s_back.reshape(4, 2, 32, 1024).astype(F32), axis=0)
    d_normed_s = d_normed_s.reshape(2, 32, 16, 64).transpose(1, 2, 0, 3).reshape(32, 2048)
    source_grad = norm_back(source_rows, s_gain, d_normed_s)
    d_normed_t = jnp.sum(t_back.astype(F32), axis=0)[:6]
    target_grad = cot.astype(F32) + norm_back(target_rows, t_gain, d_normed_t)
    o_grad = total(o_part.astype(BF16).reshape(2, nz, 64 * 2048 // nz // 128, 128), nz)
    return target_grad, source_grad, o_grad.reshape(64, 2048)


def solution(mesh):
    nz = mesh.shape["sp"]
    SIZES["z"] = nz
    fine = Mesh(mesh.devices.reshape(nz, 4, 4, 2), ("z", "y", "x", "c"))
    every, plane = ("z", "y", "x", "c"), ("y", "x", "c")
    return jax.shard_map(
        functools.partial(body, nz),
        mesh=fine,
        in_specs=(
            P(every, None), P(every, None), P(), P(),
            P(None, plane), P(plane, None), P(plane, None), P(plane, None), P(every, None),
        ),
        out_specs=(P(every, None), P(every, None), P(plane, None)),
        check_vma=False,
    )
```

```python
import functools

import jax
import jax.numpy as jnp
from jax import lax
from jax.experimental import pallas as pl
from jax.experimental.pallas import tpu as pltpu
from jax.sharding import Mesh
from jax.sharding import PartitionSpec as P

MESH = pl.DeviceIdType.MESH
HD = 64
EPSILON = 1e-06
F32, BF16 = jnp.float32, jnp.bfloat16
VMEM = pl.BlockSpec(memory_space=pltpu.VMEM)
SIZES = {"y": 4, "x": 4, "c": 2}
PIECES = 2


def dma(n):
    return pltpu.SemaphoreType.DMA((n,))


def params(cid):
    return pltpu.CompilerParams(
        collective_id=cid, has_side_effects=True, vmem_limit_bytes=62 * 1024 * 1024
    )


def group_size(axes):
    n = 1
    for a in axes:
        n *= SIZES[a]
    return n


def group_index(axes):
    i = 0
    for a in axes:
        i = i * SIZES[a] + lax.axis_index(a)
    return i


def coords_of(index, axes):
    out = {}
    for a in reversed(axes):
        out[a] = lax.rem(index, SIZES[a])
        index = index // SIZES[a]
    return out


def greet(axes):
    n, me = group_size(axes), group_index(axes)
    sem = pltpu.get_barrier_semaphore()

    def one(k, carry):
        pl.semaphore_signal(
            sem, inc=1, device_id=coords_of(lax.rem(me + k, n), axes), device_id_type=MESH
        )
        return carry

    lax.fori_loop(1, n, one, 0)
    return n - 1


def greeted(count):
    pl.semaphore_wait(pltpu.get_barrier_semaphore(), count)


class Exchange:
    def __init__(self, axes, src, dst, send, recv, pick=None):
        self.axes, self.src, self.dst, self.send, self.recv = axes, src, dst, send, recv
        self.n, self.me = group_size(axes), group_index(axes)
        self.pick = pick

    def block(self, index):
        if self.pick is None:
            return self.src
        return self.src.at[self.pick(coords_of(index, self.axes), index)]

    def copy(self, k, slot):
        to = lax.rem(self.me + k, self.n)
        return pltpu.make_async_remote_copy(
            src_ref=self.block(to),
            dst_ref=self.dst.at[slot],
            send_sem=self.send.at[k],
            recv_sem=self.recv.at[k],
            device_id=coords_of(to, self.axes),
            device_id_type=MESH,
        )

    def start(self):
        def one(k, carry):
            self.copy(k, self.me).start()
            return carry

        lax.fori_loop(1, self.n, one, 0)
        self.dst[self.me] = self.block(self.me)[...]

    def arrive(self):
        def one(k, carry):
            self.copy(k, lax.rem(self.me + self.n - k, self.n)).wait_recv()
            return carry

        lax.fori_loop(1, self.n, one, 0)

    def drain(self):
        def one(k, carry):
            self.copy(k, self.me).wait_send()
            return carry

        lax.fori_loop(1, self.n, one, 0)


class ToReaders:
    def __init__(self, src, dst, send, recv):
        self.src, self.dst, self.send, self.recv = src, dst, send, recv
        self.y, self.x, self.c = (lax.axis_index(a) for a in "yxc")
        self.mine = self.x // 2 == self.c

    def copy(self, k, slot):
        return pltpu.make_async_remote_copy(
            src_ref=self.src,
            dst_ref=self.dst.at[slot],
            send_sem=self.send.at[k],
            recv_sem=self.recv.at[slot],
            device_id={"x": lax.rem(self.x + k, 4), "c": self.x // 2},
            device_id_type=MESH,
        )

    def slot(self):
        return lax.rem(self.x, 2) * 2 + self.c

    def start(self):
        for k in range(1, 4):
            self.copy(k, self.slot()).start()

        @pl.when(jnp.logical_not(self.mine))
        def _():
            self.copy(0, self.slot()).start()

        @pl.when(self.mine)
        def _():
            self.dst[self.slot()] = self.src[...]

    def arrive(self):
        for s in range(4):
            own = jnp.logical_and(2 * self.c + s // 2 == self.x, self.c == s % 2)

            @pl.when(jnp.logical_not(own))
            def _():
                self.copy(1, s).wait_recv()

    def drain(self):
        for k in range(1, 4):
            self.copy(k, self.slot()).wait_send()

        @pl.when(jnp.logical_not(self.mine))
        def _():
            self.copy(0, self.slot()).wait_send()


class ToOwners:
    def __init__(self, src, dst, send, recv):
        self.src, self.dst, self.send, self.recv = src, dst, send, recv
        self.y, self.x, self.c = (lax.axis_index(a) for a in "yxc")

    def copy(self, s, slot):
        return pltpu.make_async_remote_copy(
            src_ref=self.src.at[s],
            dst_ref=self.dst.at[slot],
            send_sem=self.send.at[s],
            recv_sem=self.recv.at[slot],
            device_id={"x": 2 * self.c + s // 2, "c": jnp.int32(s % 2)},
            device_id_type=MESH,
        )

    def own(self, s):
        return jnp.logical_and(2 * self.c + s // 2 == self.x, self.c == s % 2)

    def start(self):
        for s in range(4):
            @pl.when(jnp.logical_not(self.own(s)))
            def _():
                self.copy(s, self.x).start()

            @pl.when(self.own(s))
            def _():
                self.dst[self.x] = self.src[s]

    def arrive(self):
        for j in range(4):
            own = jnp.logical_and(self.x == j, self.x // 2 == self.c)

            @pl.when(jnp.logical_not(own))
            def _():
                self.copy(0, j).wait_recv()

    def drain(self):
        for s in range(4):
            @pl.when(jnp.logical_not(self.own(s)))
            def _():
                self.copy(s, self.x).wait_send()


def lanes_below(shape, bound):
    return lax.broadcasted_iota(jnp.int32, shape, 1) < bound


def contract(a, b, da, db):
    return lax.dot_general(a, b, (((da,), (db,)), ((), ())), preferred_element_type=F32)


def ring_greet(nz):
    z = lax.axis_index("z")
    sem = pltpu.get_barrier_semaphore()
    right, left = lax.rem(z + 1, nz), lax.rem(z + nz - 1, nz)
    for to in (left, right):
        pl.semaphore_signal(sem, inc=1, device_id={"z": to}, device_id_type=MESH)
    return 2


class RingGather:
    def __init__(self, axis, piece, count, send, recv):
        self.axis, self.piece, self.count, self.send, self.recv = axis, piece, count, send, recv
        self.me = lax.axis_index(axis)

    def at(self, offset):
        return lax.rem(self.me + offset + 4, 4)

    def copy(self, slot, p, sign, kind):
        ref = self.piece(slot, p)
        return pltpu.make_async_remote_copy(
            src_ref=ref,
            dst_ref=ref,
            send_sem=self.send.at[kind, p],
            recv_sem=self.recv.at[kind, p],
            device_id={self.axis: self.at(sign)},
            device_id_type=MESH,
        )

    def start(self, p):
        self.copy(self.me, p, 1, 0).start()
        self.copy(self.me, p, -1, 1).start()

    def relay(self, p):
        self.copy(self.at(-1), p, 1, 0).wait_recv()
        self.copy(self.at(1), p, -1, 1).wait_recv()
        if p < self.count // 2:
            self.copy(self.at(-1), p, 1, 2).start()
        else:
            self.copy(self.at(1), p, -1, 2).start()

    def arrive(self, p):
        self.copy(self.at(2), p, 1, 2).wait_recv()

    def drain(self):
        for p in range(self.count):
            for kind in range(3):
                self.copy(self.me, p, 1, kind).wait_send()


class RowGather:
    def __init__(self, halves, out, send, recv):
        self.halves, self.out, self.send, self.recv = halves, out, send, recv
        self.y, self.c = lax.axis_index("y"), lax.axis_index("c")

    def at(self, offset):
        return lax.rem(self.y + offset + 4, 4)

    def first(self, sign, core, slot_y, slot_c):
        kind = 0 if sign > 0 else 1
        return pltpu.make_async_remote_copy(
            src_ref=self.halves.at[core],
            dst_ref=self.out.at[slot_y, slot_c],
            send_sem=self.send.at[kind, core],
            recv_sem=self.recv.at[kind, slot_c],
            device_id={"y": self.at(sign), "c": jnp.int32(core)},
            device_id_type=MESH,
        )

    def partner(self, slot_c):
        return pltpu.make_async_remote_copy(
            src_ref=self.halves.at[1 - self.c],
            dst_ref=self.out.at[self.y, slot_c],
            send_sem=self.send.at[4, 0],
            recv_sem=self.recv.at[4, 0],
            device_id={"c": 1 - self.c},
            device_id_type=MESH,
        )

    def second(self, sign, slot_y, slot_c):
        kind = 2 if sign > 0 else 3
        ref = self.out.at[slot_y, slot_c, pl.ds(0 if sign > 0 else 16, 16)]
        return pltpu.make_async_remote_copy(
            src_ref=ref,
            dst_ref=ref,
            send_sem=self.send.at[kind, slot_c],
            recv_sem=self.recv.at[kind, slot_c],
            device_id={"y": self.at(sign)},
            device_id_type=MESH,
        )

    def start(self):
        for core in range(2):
            self.first(1, core, self.y, self.c).start()
            self.first(-1, core, self.y, self.c).start()
        self.partner(self.c).start()
        self.out[self.y, self.c] = self.halves[self.c]

    def relay(self):
        for core in range(2):
            self.first(1, 0, self.at(-1), core).wait_recv()
            self.second(1, self.at(-1), core).start()
            self.first(-1, 0, self.at(1), core).wait_recv()
            self.second(-1, self.at(1), core).start()

    def arrive(self):
        self.partner(1 - self.c).wait_recv()
        for core in range(2):
            self.second(1, self.at(2), core).wait_recv()
            self.second(-1, self.at(2), core).wait_recv()

    def drain(self):
        self.partner(self.c).wait_send()
        for core in range(2):
            self.first(1, core, self.y, self.c).wait_send()
            self.first(-1, core, self.y, self.c).wait_send()
            self.second(1, self.y, core).wait_send()
            self.second(-1, self.y, core).wait_send()


class WeightColumn:
    def __init__(self, wk, wv, out, send, recv):
        self.parts, self.out, self.send, self.recv = (wk, wv), out, send, recv
        self.y, self.x = lax.axis_index("y"), lax.axis_index("x")

    def lanes(self, y):
        return pl.ds(pl.multiple_of(y * 128, 128), 128)

    def copy(self, k, i, slot_y):
        to = lax.rem(self.y + k, 4)
        return pltpu.make_async_remote_copy(
            src_ref=self.parts[i].at[:, self.lanes(to)],
            dst_ref=self.out.at[self.x, slot_y, i],
            send_sem=self.send.at[k, i],
            recv_sem=self.recv.at[k, i],
            device_id={"y": to},
            device_id_type=MESH,
        )

    def start(self):
        for k in (2, 1, 3):
            for i in range(2):
                self.copy(k, i, self.y).start()
        for i in range(2):
            self.out[self.x, self.y, i] = self.parts[i][:, self.lanes(self.y)]

    def arrive(self):
        for k in range(1, 4):
            for i in range(2):
                self.copy(k, i, lax.rem(self.y + 4 - k, 4)).wait_recv()

    def drain(self):
        for k in range(1, 4):
            for i in range(2):
                self.copy(k, i, self.y).wait_send()


def unit_rows(matrix, gain):
    wide = matrix.astype(F32)
    factor = lax.rsqrt(jnp.mean(wide * wide, axis=-1, keepdims=True) + EPSILON)
    return wide * factor * gain


def swap_halves(a):
    return pltpu.roll(a, HD, 1)


def forward_kernel(
    nz, target_rows, source_rows, t_gain, s_gain, pair, wk, wv, cot, pick,
    kv_all, stats, out, qa, t_all, pair_all, w_all,
    halves, rows_all, part, part_all, block, blocks, m, l, o, said, heard,
    row_s, row_r, wy_s, wy_r, wx_s, wx_r, ty_s, ty_r, tx_s, tx_r, pair_s, pair_r,
    part_s, part_r, q_s, q_r, rs, rr, ls, lr, ss, sr,
):
    z, y, x, c = (lax.axis_index(a) for a in "zyxc")
    right, left = lax.rem(z + 1, nz), lax.rem(z + nz - 1, nz)
    met = greet(("y", "x", "c")) + ring_greet(nz)

    normed = unit_rows(source_rows[...], s_gain[...])
    low = lanes_below((32, 128), HD)
    for j in range(8):
        chip = (2 * j % 4) * 4 + j // 2
        first, second = (normed[:, 128 * i : 128 * i + 128] for i in (chip, chip + 4))
        halves[0, :, 128 * j : 128 * j + 128] = jnp.where(low, first, swap_halves(second)).astype(BF16)
        halves[1, :, 128 * j : 128 * j + 128] = jnp.where(low, swap_halves(first), second).astype(BF16)
    greeted(met)

    by_rows = RowGather(halves, rows_all, row_s, row_r)
    by_wy = WeightColumn(wk, wv, w_all, wy_s, wy_r)
    by_wx = RingGather("x", lambda slot, p: w_all.at[slot, p], 4, wx_s, wx_r)
    by_ty = RingGather("y", lambda slot, p: t_all.at[x, slot, :, pl.ds(1024 * p, 1024)], 2, ty_s, ty_r)
    by_tx = RingGather("x", lambda slot, p: t_all.at[slot, p], 4, tx_s, tx_r)
    by_pair = Exchange(("c",), pair, pair_all, pair_s, pair_r)
    by_wy.start()
    by_rows.start()
    zero = jnp.zeros((2, target_rows.shape[1]), F32)
    t_all[x, y] = jnp.concatenate(
        [unit_rows(target_rows[...], t_gain[...]), zero, cot[...].astype(F32), zero], axis=0
    ).astype(BF16)
    for p in range(2):
        by_ty.start(p)
    by_pair.start()

    by_wy.arrive()
    for p in range(4):
        by_wx.start(p)
    by_rows.relay()
    for p in range(2):
        by_ty.relay(p)
    for p in range(4):
        by_wx.relay(p)
    for p in range(2):
        by_ty.arrive(p)
    for p in range(4):
        by_tx.start(p)
    by_rows.arrive()
    for p in range(4):
        by_wx.arrive(p)

    rows = rows_all[...].reshape(256, 1024)
    k2 = jnp.dot(rows, w_all[:, :, 0].reshape(1024, 128), preferred_element_type=F32)
    v2 = jnp.dot(rows, w_all[:, :, 1].reshape(1024, 128), preferred_element_type=F32)
    wide_low = lanes_below((256, 128), HD)
    part[0] = jnp.where(wide_low, k2, swap_halves(v2))
    part[1] = jnp.where(wide_low, swap_halves(k2), v2)
    by_part = Exchange(("c",), part, part_all, part_s, part_r, lambda at, i: i)
    by_part.start()
    for p in range(4):
        by_tx.relay(p)
    by_part.arrive()
    kv_all[z] = (part_all[0] + part_all[1]).astype(BF16)

    steps_r = nz // 2
    steps_l = nz - 1 - steps_r
    piece = 256 // PIECES

    def hop(step, p, sign, ahead=0):
        at = lax.rem(z + 2 * nz - sign * (step + ahead), nz)
        ssem, rsem = (rs, rr) if sign > 0 else (ls, lr)
        ref = kv_all.at[at, pl.ds(p * piece, piece)]
        return pltpu.make_async_remote_copy(
            src_ref=ref,
            dst_ref=ref,
            send_sem=ssem.at[step, p],
            recv_sem=rsem.at[step, p],
            device_id={"z": right if sign > 0 else left},
            device_id_type=MESH,
        )

    for p in range(PIECES):
        hop(0, p, 1).start()
        hop(0, p, -1).start()

    def pass_on(s):
        for p in range(PIECES):
            hop(s - 1, p, 1, 1).wait_recv()
            hop(s, p, 1).start()
            hop(s - 1, p, -1, 1).wait_recv()

            @pl.when(s < steps_l)
            def _():
                hop(s, p, -1).start()

    by_pair.arrive()
    for p in range(4):
        by_tx.arrive(p)
    everything = t_all[...].reshape(256, 2048)
    scale = jnp.where(lanes_below((256, 128), HD), HD**-0.5, 1.0)
    for a in range(2):
        both = (contract(everything, pair_all[a], 1, 1) * scale).astype(BF16)
        chosen = jnp.dot(pick[...], both, preferred_element_type=F32)
        block[96 * a : 96 * a + 96] = jnp.where(
            lanes_below((96, 128), HD), chosen[:96], chosen[96:]
        ).astype(BF16)
    by_q = ToReaders(block, blocks, q_s, q_r)
    by_q.start()
    pass_on(jnp.int32(1))
    m[...] = jnp.full(m.shape, -1e30, F32)
    l[...] = jnp.zeros(l.shape, F32)
    o[...] = jnp.zeros(o.shape, F32)
    by_q.arrive()
    qa[...] = blocks[...].reshape(qa.shape)

    def attend(at):
        block = kv_all[at]
        keys = jnp.where(lanes_below(block.shape, HD), block, jnp.zeros_like(block))
        scores = contract(keys, qa[...], 1, 1)
        top = jnp.maximum(m[...], jnp.max(scores, axis=0, keepdims=True))
        weights = jnp.exp(scores - top)
        old = jnp.exp(m[...] - top)
        m[...] = top
        l[...] = l[...] * old + jnp.sum(weights, axis=0, keepdims=True)
        o[...] = o[...] * old + contract(block, weights.astype(BF16), 0, 0)[HD:]

    attend(z)

    def step(s, carry):
        pass_on(s)
        attend(lax.rem(z + nz - s + 1, nz))
        attend(lax.rem(z + s - 1, nz))
        return carry

    lax.fori_loop(2, steps_r, step, 0)
    for p in range(PIECES):
        hop(steps_r - 1, p, 1, 1).wait_recv()

    attend(lax.rem(z + nz - steps_r + 1, nz))
    attend(lax.rem(z + steps_r - 1, nz))
    attend(lax.rem(z + nz - steps_r, nz))
    upright = jnp.transpose(qa[...].astype(F32))
    delta = jnp.sum(upright[HD:] * o[...], axis=0, keepdims=True)
    row = lax.broadcasted_iota(jnp.int32, (8, qa.shape[0]), 0)
    said[...] = jnp.where(row == 0, m[...], jnp.where(row == 1, l[...], delta))
    e = Exchange(("x",), said, heard, ss, sr)
    e.start()
    for by in (by_rows, by_wy, by_wx, by_ty, by_tx, by_pair, by_part, by_q):
        by.drain()

    def drain(s, carry):
        for p in range(PIECES):
            hop(s, p, 1).wait_send()

            @pl.when(s < steps_l)
            def _():
                hop(s, p, -1).wait_send()

        return carry

    lax.fori_loop(0, steps_r, drain, 0)
    e.arrive()
    top = jnp.max(heard[:, 0:1], axis=0)
    total = jnp.zeros_like(top)
    both = jnp.zeros_like(top)
    for j in range(4):
        w = jnp.exp(heard[j, 0:1] - top)
        total = total + w * heard[j, 1:2]
        both = both + w * heard[j, 2:3]
    stats[...] = jnp.where(row == 0, top + jnp.log(total), both / total)
    scaled = o[...] * (jnp.exp(m[...] - top) / total)
    out[...] = jnp.transpose(jnp.concatenate([scaled, jnp.zeros_like(scaled)], axis=0)).astype(BF16)
    e.drain()


def sems(*shape):
    return pltpu.SemaphoreType.DMA(shape)


def forward(args, nz):
    t = 768
    ring = sems(nz // 2, PIECES)
    return pl.pallas_call(
        functools.partial(forward_kernel, nz),
        out_shape=(
            jax.ShapeDtypeStruct((nz, 256, 128), BF16),
            jax.ShapeDtypeStruct((8, t), F32),
            jax.ShapeDtypeStruct((t, 128), BF16),
            jax.ShapeDtypeStruct((t, 128), BF16),
            jax.ShapeDtypeStruct((4, 4, 16, 2048), BF16),
            jax.ShapeDtypeStruct((2, 128, 2048), BF16),
            jax.ShapeDtypeStruct((4, 4, 2, 64, 128), BF16),
        ),
        in_specs=[VMEM] * len(args),
        out_specs=(VMEM,) * 7,
        scratch_shapes=[
            pltpu.VMEM((2, 32, 1024), BF16),
            pltpu.VMEM((4, 2, 32, 1024), BF16),
            pltpu.VMEM((2, 256, 128), F32),
            pltpu.VMEM((2, 256, 128), F32),
            pltpu.VMEM((192, 128), BF16),
            pltpu.VMEM((4, 192, 128), BF16),
            pltpu.VMEM((1, t), F32),
            pltpu.VMEM((1, t), F32),
            pltpu.VMEM((HD, t), F32),
            pltpu.VMEM((8, t), F32),
            pltpu.VMEM((4, 8, t), F32),
            sems(5, 2), sems(5, 2), sems(4, 2), sems(4, 2), sems(3, 4), sems(3, 4),
            sems(3, 2), sems(3, 2), sems(3, 4), sems(3, 4), dma(2), dma(2),
            dma(2), dma(2), dma(4), dma(4), ring, ring, ring, ring, dma(4), dma(4),
        ],
        compiler_params=params(0),
    )(*args)


def backward_kernel(
    nz, qa, kv_all, stats, out, t_all, pair_all, w_all, pick, pick8,
    s_out, t_out, w_out,
    dq, own, tor, tol, inr, inl, outs, dq_block, dqs, o_part, swapped, terms, sums, mine_sum, all_sums,
    kv_grad, grads2, parts, d_parts, s_in, t_in,
    rs, rr, ls, lr, o_s, o_r, dq_s, dq_r, sw_s, sw_r, z_s, z_r, back_s, back_r,
    pair_s, pair_r, s_s, s_r, t_s, t_r,
):
    z, c = lax.axis_index("z"), lax.axis_index("c")
    right, left = lax.rem(z + 1, nz), lax.rem(z + nz - 1, nz)
    greeted(greet(("y", "x", "c")) + greet(("z",)))
    by_o = ToOwners(out, outs, o_s, o_r)
    by_o.start()
    steps_l = nz // 2
    steps_r = nz - 1 - steps_l
    piece = 256 // PIECES
    dq[...] = jnp.zeros(dq.shape, F32)

    def grads(at):
        block = kv_all[at]
        low = lanes_below(block.shape, HD)
        none = jnp.zeros_like(block)
        scores = contract(jnp.where(low, block, none), qa[...], 1, 1)
        probs = jnp.exp(scores - stats[0:1])
        d_probs = contract(jnp.where(low, none, block), qa[...], 1, 1)
        d_scores = (probs * (d_probs - stats[1:2])).astype(BF16)
        for_v = contract(probs.astype(BF16), qa[...], 1, 0)
        for_k = contract(d_scores, qa[...], 1, 0)
        dq[...] += contract(block, d_scores, 0, 0)[:HD]
        return jnp.where(lanes_below(for_k.shape, HD), for_k, for_v)

    def hop(s, p, sign):
        ssem, rsem = (rs, rr) if sign > 0 else (ls, lr)
        src, dst = (tor, inr) if sign > 0 else (tol, inl)
        return pltpu.make_async_remote_copy(
            src_ref=src.at[s, pl.ds(p * piece, piece)],
            dst_ref=dst.at[s, pl.ds(p * piece, piece)],
            send_sem=ssem.at[s, p],
            recv_sem=rsem.at[s, p],
            device_id={"z": right if sign > 0 else left},
            device_id_type=MESH,
        )

    def send_first(sign, value):
        ref = tor if sign > 0 else tol
        ref[0] = value.astype(BF16)
        for p in range(PIECES):
            hop(0, p, sign).start()

    def send_on(s, sign):
        ref, arrived = (tor, inr) if sign > 0 else (tol, inl)
        for p in range(PIECES):
            hop(s - 1, p, sign).wait_recv()
            at = pl.ds(p * piece, piece)
            ref[s, at] = (arrived[s - 1, at].astype(F32) + own[at]).astype(BF16)
            hop(s, p, sign).start()

    send_first(-1, grads(lax.rem(z + nz - steps_l, nz)))
    send_first(1, grads(lax.rem(z + steps_r, nz)))

    by_o.arrive()
    attended = jnp.sum(outs[...].astype(F32), axis=0).astype(BF16)
    everything = t_all[...].reshape(256, 2048)
    for a in range(2):
        spread = contract(pick[96:], attended[96 * a : 96 * a + 96], 0, 0).astype(BF16)
        product = contract(spread, everything, 0, 0)[:HD].astype(BF16)
        for i in range(nz):
            o_part[a, i] = product[:, 128 * i : 128 * i + 128]
    swap = Exchange(("c",), o_part, swapped, sw_s, sw_r, lambda at, i: i)
    swap.start()
    by_z = Exchange(("z",), terms, sums, z_s, z_r, lambda at, i: i)
    back = Exchange(("z",), mine_sum, all_sums, back_s, back_r)

    def step(s, carry):
        own[...] = grads(lax.rem(z + nz - steps_l + s, nz))
        send_on(s, -1)

        @pl.when(s < steps_r)
        def _():
            own[...] = grads(lax.rem(z + steps_r - s, nz))
            send_on(s, 1)

        @pl.when(s == 1)
        def _():
            swap.arrive()
            terms[...] = (swapped[0].astype(F32) + swapped[1].astype(F32)).astype(BF16)
            by_z.start()

        @pl.when(s == steps_l - 1)
        def _():
            by_z.arrive()
            mine_sum[...] = jnp.sum(sums[...].astype(F32), axis=0).astype(BF16)
            back.start()

        return carry

    lax.fori_loop(1, steps_l, step, 0)
    own[...] = grads(z)
    dq_block[...] = (
        jnp.transpose(jnp.concatenate([dq[...], jnp.zeros_like(dq[...])], axis=0)) * HD**-0.5
    ).astype(BF16).reshape(4, 192, 128)
    by_dq = ToOwners(dq_block, dqs, dq_s, dq_r)
    by_dq.start()
    for p in range(PIECES):
        at = pl.ds(p * piece, piece)
        hop(steps_l - 1, p, -1).wait_recv()
        hop(steps_r - 1, p, 1).wait_recv()
        kv_grad[at] = (
            inl[steps_l - 1, at].astype(F32) + inr[steps_r - 1, at].astype(F32) + own[at]
        ).astype(BF16)
    by_pair = Exchange(("c",), kv_grad, grads2, pair_s, pair_r)
    by_pair.start()
    by_dq.arrive()
    query_grad = jnp.sum(dqs[...].astype(F32), axis=0).astype(BF16)
    d_target = jnp.zeros((128, 2048), F32)
    for a in range(2):
        spread = contract(pick8[...], query_grad[96 * a : 96 * a + 96], 0, 0).astype(BF16)
        d_target = d_target + jnp.dot(spread, pair_all[a], preferred_element_type=F32)
    d_parts[...] = d_target.astype(BF16).reshape(16, 8, 2048)
    by_pair.arrive()
    low = lanes_below((256, 128), HD)
    g0, g1 = grads2[0].astype(F32), grads2[1].astype(F32)
    k2 = jnp.where(low, g0, swap_halves(g1)).astype(BF16)
    v2 = jnp.where(low, swap_halves(g0), g1).astype(BF16)
    d_rows = contract(k2, w_all[:, :, 0].reshape(1024, 128), 1, 1)
    d_rows = d_rows + contract(v2, w_all[:, :, 1].reshape(1024, 128), 1, 1)
    parts[...] = d_rows.astype(BF16).reshape(8, 32, 1024)
    by_s = Exchange(("y", "c"), parts, s_in, s_s, s_r, lambda at, i: i)
    by_s.start()
    by_t = Exchange(("x", "y"), d_parts, t_in, t_s, t_r, lambda at, i: i)
    by_t.start()
    back.arrive()
    for i in range(nz):
        w_out[:, 128 * i : 128 * i + 128] = all_sums[i].astype(F32)
    by_t.arrive()
    t_out[...] = jnp.sum(t_in[...].astype(F32), axis=0)
    by_s.arrive()
    low = lanes_below((32, 128), HD)
    for core in range(2):
        got = s_in[core].astype(F32)
        for i in range(1, 4):
            got = got + s_in[2 * i + core].astype(F32)
        parts_f = got
        if core == 0:
            got0 = parts_f
        else:
            got1 = parts_f
    for j in range(8):
        chip = (2 * j % 4) * 4 + j // 2
        a, b = got0[:, 128 * j : 128 * j + 128], got1[:, 128 * j : 128 * j + 128]
        s_out[:, 128 * chip : 128 * chip + 128] = jnp.where(low, a, swap_halves(b))
        s_out[:, 128 * chip + 512 : 128 * chip + 640] = jnp.where(low, swap_halves(a), b)
    for e in (by_o, by_dq, swap, by_z, back, by_pair, by_s, by_t):
        e.drain()

    def drain(s, carry):
        for p in range(PIECES):
            hop(s, p, -1).wait_send()

            @pl.when(s < steps_r)
            def _():
                hop(s, p, 1).wait_send()

        return carry

    lax.fori_loop(0, steps_l, drain, 0)


def backward(args, nz):
    t = 768
    half = nz // 2
    ring = sems(half, PIECES)
    slots = pltpu.VMEM((half, 256, 128), BF16)
    owned = pltpu.VMEM((4, 192, 128), BF16)
    return pl.pallas_call(
        functools.partial(backward_kernel, nz),
        out_shape=(
            jax.ShapeDtypeStruct((32, 2048), F32),
            jax.ShapeDtypeStruct((8, 2048), F32),
            jax.ShapeDtypeStruct((64, 2048), F32),
        ),
        in_specs=[VMEM] * len(args),
        out_specs=(VMEM,) * 3,
        scratch_shapes=[
            pltpu.VMEM((HD, t), F32),
            pltpu.VMEM((256, 128), F32),
            slots, slots, slots, slots,
            owned, owned, owned,
            pltpu.VMEM((2, nz, HD, 128), BF16),
            pltpu.VMEM((2, nz, HD, 128), BF16),
            pltpu.VMEM((nz, HD, 128), BF16),
            pltpu.VMEM((nz, HD, 128), BF16),
            pltpu.VMEM((HD, 128), BF16),
            pltpu.VMEM((nz, HD, 128), BF16),
            pltpu.VMEM((256, 128), BF16),
            pltpu.VMEM((2, 256, 128), BF16),
            pltpu.VMEM((8, 32, 1024), BF16),
            pltpu.VMEM((16, 8, 2048), BF16),
            pltpu.VMEM((8, 32, 1024), BF16),
            pltpu.VMEM((16, 8, 2048), BF16),
            ring, ring, ring, ring, dma(4), dma(4), dma(4), dma(4), dma(2), dma(2),
            dma(nz), dma(nz), dma(nz), dma(nz), dma(2), dma(2), dma(8), dma(8), dma(16), dma(16),
        ],
        compiler_params=params(1),
    )(*args)


def norm_back(matrix, gain, upstream):
    wide = matrix.astype(F32)
    factor = lax.rsqrt(jnp.mean(wide * wide, axis=-1, keepdims=True) + EPSILON)
    weighted = upstream * gain
    inner = jnp.mean(weighted * wide, axis=-1, keepdims=True)
    return factor * weighted - wide * factor**3 * inner


def picks():
    r = jnp.arange(96)
    at = 16 * (r // 6) + r % 6
    pick = jnp.concatenate([at, at + 8])[:, None] == jnp.arange(256)[None]
    pick8 = (8 * (r // 6) + r % 6)[:, None] == jnp.arange(128)[None]
    return pick.astype(BF16), pick8.astype(BF16)


def body(nz, target_rows, source_rows, t_gain, s_gain, wq, wk, wv, wo, cot):
    pick, pick8 = picks()
    pair = jnp.concatenate([wq.T, wo])
    kv_all, stats, out, qa, t_all, pair_all, w_all = forward(
        (target_rows, source_rows, t_gain[None], s_gain[None], pair, wk, wv, cot, pick), nz
    )
    d_source, d_target, o_grad = backward(
        (qa, kv_all, stats, out.reshape(4, 192, 128), t_all, pair_all, w_all, pick, pick8), nz
    )
    source_grad = norm_back(source_rows, s_gain, d_source)
    target_grad = cot.astype(F32) + norm_back(target_rows, t_gain, d_target[:6])
    return target_grad, source_grad, o_grad


def solution(mesh):
    nz = mesh.shape["sp"]
    SIZES["z"] = nz
    fine = Mesh(mesh.devices.reshape(nz, 4, 4, 2), ("z", "y", "x", "c"))
    every, plane = ("z", "y", "x", "c"), ("y", "x", "c")
    return jax.shard_map(
        functools.partial(body, nz),
        mesh=fine,
        in_specs=(
            P(every, None), P(every, None), P(), P(),
            P(None, plane), P(plane, None), P(plane, None), P(plane, None), P(every, None),
        ),
        out_specs=(P(every, None), P(every, None), P(plane, None)),
        check_vma=False,
    )
```

```python
import functools

import jax
import jax.numpy as jnp
from jax import lax
from jax.experimental import pallas as pl
from jax.experimental.pallas import tpu as pltpu
from jax.sharding import Mesh
from jax.sharding import PartitionSpec as P

MESH = pl.DeviceIdType.MESH
HD = 64
EPSILON = 1e-06
F32, BF16 = jnp.float32, jnp.bfloat16
VMEM = pl.BlockSpec(memory_space=pltpu.VMEM)
SIZES = {"y": 4, "x": 4, "c": 2}
PIECES = 2
REACH = 4


def dma(n):
    return pltpu.SemaphoreType.DMA((n,))


def params(cid):
    return pltpu.CompilerParams(
        collective_id=cid, has_side_effects=True, vmem_limit_bytes=62 * 1024 * 1024
    )


def group_size(axes):
    n = 1
    for a in axes:
        n *= SIZES[a]
    return n


def group_index(axes):
    i = 0
    for a in axes:
        i = i * SIZES[a] + lax.axis_index(a)
    return i


def coords_of(index, axes):
    out = {}
    for a in reversed(axes):
        out[a] = lax.rem(index, SIZES[a])
        index = index // SIZES[a]
    return out


def greet(axes):
    n, me = group_size(axes), group_index(axes)
    sem = pltpu.get_barrier_semaphore()

    def one(k, carry):
        pl.semaphore_signal(
            sem, inc=1, device_id=coords_of(lax.rem(me + k, n), axes), device_id_type=MESH
        )
        return carry

    lax.fori_loop(1, n, one, 0)
    return n - 1


def greeted(count):
    pl.semaphore_wait(pltpu.get_barrier_semaphore(), count)


class Exchange:
    def __init__(self, axes, src, dst, send, recv, pick=None):
        self.axes, self.src, self.dst, self.send, self.recv = axes, src, dst, send, recv
        self.n, self.me = group_size(axes), group_index(axes)
        self.pick = pick

    def block(self, index):
        if self.pick is None:
            return self.src
        return self.src.at[self.pick(coords_of(index, self.axes), index)]

    def copy(self, k, slot):
        to = lax.rem(self.me + k, self.n)
        return pltpu.make_async_remote_copy(
            src_ref=self.block(to),
            dst_ref=self.dst.at[slot],
            send_sem=self.send.at[k],
            recv_sem=self.recv.at[k],
            device_id=coords_of(to, self.axes),
            device_id_type=MESH,
        )

    def start(self):
        def one(k, carry):
            self.copy(k, self.me).start()
            return carry

        lax.fori_loop(1, self.n, one, 0)
        self.dst[self.me] = self.block(self.me)[...]

    def arrive(self):
        def one(k, carry):
            self.copy(k, lax.rem(self.me + self.n - k, self.n)).wait_recv()
            return carry

        lax.fori_loop(1, self.n, one, 0)

    def drain(self):
        def one(k, carry):
            self.copy(k, self.me).wait_send()
            return carry

        lax.fori_loop(1, self.n, one, 0)


class ToReaders:
    def __init__(self, src, dst, send, recv):
        self.src, self.dst, self.send, self.recv = src, dst, send, recv
        self.y, self.x, self.c = (lax.axis_index(a) for a in "yxc")
        self.mine = self.x // 2 == self.c

    def copy(self, k, slot):
        return pltpu.make_async_remote_copy(
            src_ref=self.src,
            dst_ref=self.dst.at[slot],
            send_sem=self.send.at[k],
            recv_sem=self.recv.at[slot],
            device_id={"x": lax.rem(self.x + k, 4), "c": self.x // 2},
            device_id_type=MESH,
        )

    def slot(self):
        return lax.rem(self.x, 2) * 2 + self.c

    def start(self):
        for k in range(1, 4):
            self.copy(k, self.slot()).start()

        @pl.when(jnp.logical_not(self.mine))
        def _():
            self.copy(0, self.slot()).start()

        @pl.when(self.mine)
        def _():
            self.dst[self.slot()] = self.src[...]

    def arrive(self):
        for s in range(4):
            own = jnp.logical_and(2 * self.c + s // 2 == self.x, self.c == s % 2)

            @pl.when(jnp.logical_not(own))
            def _():
                self.copy(1, s).wait_recv()

    def drain(self):
        for k in range(1, 4):
            self.copy(k, self.slot()).wait_send()

        @pl.when(jnp.logical_not(self.mine))
        def _():
            self.copy(0, self.slot()).wait_send()


class ToOwners:
    def __init__(self, src, dst, send, recv):
        self.src, self.dst, self.send, self.recv = src, dst, send, recv
        self.y, self.x, self.c = (lax.axis_index(a) for a in "yxc")

    def copy(self, s, slot):
        return pltpu.make_async_remote_copy(
            src_ref=self.src.at[s],
            dst_ref=self.dst.at[slot],
            send_sem=self.send.at[s],
            recv_sem=self.recv.at[slot],
            device_id={"x": 2 * self.c + s // 2, "c": jnp.int32(s % 2)},
            device_id_type=MESH,
        )

    def own(self, s):
        return jnp.logical_and(2 * self.c + s // 2 == self.x, self.c == s % 2)

    def start(self):
        for s in range(4):
            @pl.when(jnp.logical_not(self.own(s)))
            def _():
                self.copy(s, self.x).start()

            @pl.when(self.own(s))
            def _():
                self.dst[self.x] = self.src[s]

    def arrive(self):
        for j in range(4):
            own = jnp.logical_and(self.x == j, self.x // 2 == self.c)

            @pl.when(jnp.logical_not(own))
            def _():
                self.copy(0, j).wait_recv()

    def drain(self):
        for s in range(4):
            @pl.when(jnp.logical_not(self.own(s)))
            def _():
                self.copy(s, self.x).wait_send()


def lanes_below(shape, bound):
    return lax.broadcasted_iota(jnp.int32, shape, 1) < bound


def contract(a, b, da, db):
    return lax.dot_general(a, b, (((da,), (db,)), ((), ())), preferred_element_type=F32)


def ring_greet(nz):
    z = lax.axis_index("z")
    sem = pltpu.get_barrier_semaphore()
    right, left = lax.rem(z + 1, nz), lax.rem(z + nz - 1, nz)
    for to in (left, right):
        pl.semaphore_signal(sem, inc=1, device_id={"z": to}, device_id_type=MESH)
    return 2


class RingGather:
    def __init__(self, axis, piece, count, send, recv):
        self.axis, self.piece, self.count, self.send, self.recv = axis, piece, count, send, recv
        self.me = lax.axis_index(axis)

    def at(self, offset):
        return lax.rem(self.me + offset + 4, 4)

    def copy(self, slot, p, sign, kind):
        ref = self.piece(slot, p)
        return pltpu.make_async_remote_copy(
            src_ref=ref,
            dst_ref=ref,
            send_sem=self.send.at[kind, p],
            recv_sem=self.recv.at[kind, p],
            device_id={self.axis: self.at(sign)},
            device_id_type=MESH,
        )

    def start(self, p):
        self.copy(self.me, p, 1, 0).start()
        self.copy(self.me, p, -1, 1).start()

    def relay(self, p):
        self.copy(self.at(-1), p, 1, 0).wait_recv()
        self.copy(self.at(1), p, -1, 1).wait_recv()
        if p < self.count // 2:
            self.copy(self.at(-1), p, 1, 2).start()
        else:
            self.copy(self.at(1), p, -1, 2).start()

    def arrive(self, p):
        self.copy(self.at(2), p, 1, 2).wait_recv()

    def drain(self):
        for p in range(self.count):
            for kind in range(3):
                self.copy(self.me, p, 1, kind).wait_send()


class RowGather:
    def __init__(self, halves, out, send, recv):
        self.halves, self.out, self.send, self.recv = halves, out, send, recv
        self.y, self.c = lax.axis_index("y"), lax.axis_index("c")

    def at(self, offset):
        return lax.rem(self.y + offset + 4, 4)

    def first(self, sign, core, slot_y, slot_c):
        kind = 0 if sign > 0 else 1
        return pltpu.make_async_remote_copy(
            src_ref=self.halves.at[core],
            dst_ref=self.out.at[slot_y, slot_c],
            send_sem=self.send.at[kind, core],
            recv_sem=self.recv.at[kind, slot_c],
            device_id={"y": self.at(sign), "c": jnp.int32(core)},
            device_id_type=MESH,
        )

    def partner(self, slot_c):
        return pltpu.make_async_remote_copy(
            src_ref=self.halves.at[1 - self.c],
            dst_ref=self.out.at[self.y, slot_c],
            send_sem=self.send.at[4, 0],
            recv_sem=self.recv.at[4, 0],
            device_id={"c": 1 - self.c},
            device_id_type=MESH,
        )

    def second(self, sign, slot_y, slot_c):
        kind = 2 if sign > 0 else 3
        ref = self.out.at[slot_y, slot_c, pl.ds(0 if sign > 0 else 16, 16)]
        return pltpu.make_async_remote_copy(
            src_ref=ref,
            dst_ref=ref,
            send_sem=self.send.at[kind, slot_c],
            recv_sem=self.recv.at[kind, slot_c],
            device_id={"y": self.at(sign)},
            device_id_type=MESH,
        )

    def start(self):
        for core in range(2):
            self.first(1, core, self.y, self.c).start()
            self.first(-1, core, self.y, self.c).start()
        self.partner(self.c).start()
        self.out[self.y, self.c] = self.halves[self.c]

    def relay(self):
        for core in range(2):
            self.first(1, 0, self.at(-1), core).wait_recv()
            self.second(1, self.at(-1), core).start()
            self.first(-1, 0, self.at(1), core).wait_recv()
            self.second(-1, self.at(1), core).start()

    def arrive(self):
        self.partner(1 - self.c).wait_recv()
        for core in range(2):
            self.second(1, self.at(2), core).wait_recv()
            self.second(-1, self.at(2), core).wait_recv()

    def drain(self):
        self.partner(self.c).wait_send()
        for core in range(2):
            self.first(1, core, self.y, self.c).wait_send()
            self.first(-1, core, self.y, self.c).wait_send()
            self.second(1, self.y, core).wait_send()
            self.second(-1, self.y, core).wait_send()


class WeightColumn:
    def __init__(self, wk, wv, out, send, recv):
        self.parts, self.out, self.send, self.recv = (wk, wv), out, send, recv
        self.y, self.x = lax.axis_index("y"), lax.axis_index("x")

    def lanes(self, y):
        return pl.ds(pl.multiple_of(y * 128, 128), 128)

    def copy(self, k, i, slot_y):
        to = lax.rem(self.y + k, 4)
        return pltpu.make_async_remote_copy(
            src_ref=self.parts[i].at[:, self.lanes(to)],
            dst_ref=self.out.at[self.x, slot_y, i],
            send_sem=self.send.at[k, i],
            recv_sem=self.recv.at[k, i],
            device_id={"y": to},
            device_id_type=MESH,
        )

    def start(self):
        for k in (2, 1, 3):
            for i in range(2):
                self.copy(k, i, self.y).start()
        for i in range(2):
            self.out[self.x, self.y, i] = self.parts[i][:, self.lanes(self.y)]

    def arrive(self):
        for k in range(1, 4):
            for i in range(2):
                self.copy(k, i, lax.rem(self.y + 4 - k, 4)).wait_recv()

    def drain(self):
        for k in range(1, 4):
            for i in range(2):
                self.copy(k, i, self.y).wait_send()


def unit_rows(matrix, gain):
    wide = matrix.astype(F32)
    factor = lax.rsqrt(jnp.mean(wide * wide, axis=-1, keepdims=True) + EPSILON)
    return wide * factor * gain


def swap_halves(a):
    return pltpu.roll(a, HD, 1)


class RingSum:
    def __init__(self, nz, term, out, arrived, send, recv, pieces):
        self.nz, self.term, self.out, self.arrived = nz, term, out, arrived
        self.send, self.recv, self.pieces = send, recv, pieces
        self.rows = out.shape[2] // pieces
        self.last = (nz // 2 - 1, nz // 2 - 2)
        z = lax.axis_index("z")
        self.to = (lax.rem(z + nz - 1, nz), lax.rem(z + 1, nz))

    def hop(self, side, s, p):
        at = pl.ds(p * self.rows, self.rows)
        return pltpu.make_async_remote_copy(
            src_ref=self.out.at[side, s, at],
            dst_ref=self.arrived.at[side, s, at],
            send_sem=self.send.at[side, s, p],
            recv_sem=self.recv.at[side, s, p],
            device_id={"z": self.to[side]},
            device_id_type=MESH,
        )

    def first(self, side):
        self.out[side, 0] = self.term(side, 0, pl.ds(0, self.rows * self.pieces)).astype(BF16)
        for p in range(self.pieces):
            self.hop(side, 0, p).start()

    def step(self, s, side):
        for p in range(self.pieces):
            at = pl.ds(p * self.rows, self.rows)
            self.hop(side, s - 1, p).wait_recv()
            value = self.arrived[side, s - 1, at].astype(F32) + self.term(side, s, at)
            self.out[side, s, at] = value.astype(BF16)
            self.hop(side, s, p).start()

    def total(self, p):
        at = pl.ds(p * self.rows, self.rows)
        value = self.term(1, self.nz // 2 - 1, at)
        for side in (1, 0):
            self.hop(side, self.last[side], p).wait_recv()
            value = value + self.arrived[side, self.last[side], at].astype(F32)
        return value

    def drain(self):
        def one(s, carry):
            for p in range(self.pieces):
                self.hop(0, s, p).wait_send()
                self.hop(1, s, p).wait_send()
            return carry

        lax.fori_loop(0, self.last[1] + 1, one, 0)
        for p in range(self.pieces):
            self.hop(0, self.last[0], p).wait_send()


class FarGather:
    def __init__(self, nz, src, dst, send, recv):
        self.nz, self.src, self.dst, self.send, self.recv = nz, src, dst, send, recv
        self.z = lax.axis_index("z")
        self.far = {1: nz // 2 - REACH, -1: nz - 1 - nz // 2 - REACH}

    def at(self, offset):
        return lax.rem(self.z + offset + self.nz, self.nz)

    def copy(self, slot, sign, d, relay):
        i, j = (2 if relay else 0) + (0 if sign > 0 else 1), d - 1
        return pltpu.make_async_remote_copy(
            src_ref=self.dst.at[slot] if relay else self.src,
            dst_ref=self.dst.at[slot],
            send_sem=self.send.at[i, j],
            recv_sem=self.recv.at[i, j],
            device_id={"z": self.at(sign * d)},
            device_id_type=MESH,
        )

    def start(self):
        for d in range(REACH, 0, -1):
            for sign in (1, -1):
                self.copy(self.z, sign, d, False).start()
        self.dst[self.z] = self.src[...]

    def relay(self):
        for sign in (1, -1):
            slot = self.at(-sign * REACH)
            self.copy(slot, sign, REACH, False).wait_recv()
            for d in range(self.far[sign], 0, -1):
                self.copy(slot, sign, d, True).start()

    def arrive(self):
        for sign in (1, -1):
            for d in range(1, REACH):
                self.copy(self.at(-sign * d), sign, d, False).wait_recv()
            for d in range(1, self.far[sign] + 1):
                self.copy(self.at(-sign * (REACH + d)), sign, d, True).wait_recv()

    def drain(self):
        for sign in (1, -1):
            for d in range(1, REACH + 1):
                self.copy(self.z, sign, d, False).wait_send()
            for d in range(1, self.far[sign] + 1):
                self.copy(self.z, sign, d, True).wait_send()


def reach_greet(nz):
    z = lax.axis_index("z")
    for d in range(1, REACH + 1):
        for sign in (1, -1):
            pl.semaphore_signal(
                pltpu.get_barrier_semaphore(),
                inc=1,
                device_id={"z": lax.rem(z + sign * d + nz, nz)},
                device_id_type=MESH,
            )
    return 2 * REACH


def sems(*shape):
    return pltpu.SemaphoreType.DMA(shape)


def kernel(
    nz, target_rows, source_rows, t_gain, s_gain, pair, wk, wv, cot, pick, pick8,
    s_out, t_out, w_out,
    kv_all, stats, out, qa, t_all, pair_all, w_all,
    halves, rows_all, part, part_all, block, blocks, m, l, o, said, heard,
    dq, mine, ring_out, ring_in, w_ring_out, w_ring_in, outs, dq_block, dqs, o_part, swapped,
    mine_sum, all_sums, kv_grad, grads2, parts, d_parts, s_in, t_in,
    row_s, row_r, wy_s, wy_r, wx_s, wx_r, ty_s, ty_r, tx_s, tx_r, pair_s, pair_r,
    part_s, part_r, q_s, q_r, rs, rr, ls, lr, ss, sr,
    o_s, o_r, dq_s, dq_r, sw_s, sw_r, g_s, g_r, h_s, h_r, back_s, back_r,
    kv_s, kv_r, s_s, s_r, t_s, t_r,
):
    z, y, x, c = (lax.axis_index(a) for a in "zyxc")
    right, left = lax.rem(z + 1, nz), lax.rem(z + nz - 1, nz)
    met = greet(("y", "x", "c")) + reach_greet(nz)

    normed = unit_rows(source_rows[...], s_gain[...])
    low = lanes_below((32, 128), HD)
    for j in range(8):
        chip = (2 * j % 4) * 4 + j // 2
        first, second = (normed[:, 128 * i : 128 * i + 128] for i in (chip, chip + 4))
        halves[0, :, 128 * j : 128 * j + 128] = jnp.where(low, first, swap_halves(second)).astype(BF16)
        halves[1, :, 128 * j : 128 * j + 128] = jnp.where(low, swap_halves(first), second).astype(BF16)
    greeted(met)

    by_rows = RowGather(halves, rows_all, row_s, row_r)
    by_wy = WeightColumn(wk, wv, w_all, wy_s, wy_r)
    by_wx = RingGather("x", lambda slot, p: w_all.at[slot, p], 4, wx_s, wx_r)
    by_ty = RingGather("y", lambda slot, p: t_all.at[x, slot, :, pl.ds(1024 * p, 1024)], 2, ty_s, ty_r)
    by_tx = RingGather("x", lambda slot, p: t_all.at[slot, p], 4, tx_s, tx_r)
    by_pair = Exchange(("c",), pair, pair_all, pair_s, pair_r)
    by_wy.start()
    by_rows.start()
    zero = jnp.zeros((2, target_rows.shape[1]), F32)
    t_all[x, y] = jnp.concatenate(
        [unit_rows(target_rows[...], t_gain[...]), zero, cot[...].astype(F32), zero], axis=0
    ).astype(BF16)
    for p in range(2):
        by_ty.start(p)
    by_pair.start()

    by_wy.arrive()
    for p in range(4):
        by_wx.start(p)
    by_rows.relay()
    for p in range(2):
        by_ty.relay(p)
    for p in range(4):
        by_wx.relay(p)
    for p in range(2):
        by_ty.arrive(p)
    for p in range(4):
        by_tx.start(p)
    by_rows.arrive()
    for p in range(4):
        by_wx.arrive(p)

    rows = rows_all[...].reshape(256, 1024)
    k2 = jnp.dot(rows, w_all[:, :, 0].reshape(1024, 128), preferred_element_type=F32)
    v2 = jnp.dot(rows, w_all[:, :, 1].reshape(1024, 128), preferred_element_type=F32)
    wide_low = lanes_below((256, 128), HD)
    part[0] = jnp.where(wide_low, k2, swap_halves(v2))
    part[1] = jnp.where(wide_low, swap_halves(k2), v2)
    by_part = Exchange(("c",), part, part_all, part_s, part_r, lambda at, i: i)
    by_part.start()
    by_part.arrive()
    kv_all[z] = (part_all[0] + part_all[1]).astype(BF16)

    steps_r = nz // 2
    steps_l = nz - 1 - steps_r
    piece = 256 // PIECES

    def hop(step, p, sign, ahead=0):
        at = lax.rem(z + 2 * nz - sign * (step + ahead), nz)
        ssem, rsem = (rs, rr) if sign > 0 else (ls, lr)
        ref = kv_all.at[at, pl.ds(p * piece, piece)]
        return pltpu.make_async_remote_copy(
            src_ref=ref,
            dst_ref=ref,
            send_sem=ssem.at[step, p],
            recv_sem=rsem.at[step, p],
            device_id={"z": right if sign > 0 else left},
            device_id_type=MESH,
        )

    for p in range(PIECES):
        hop(0, p, 1).start()
        hop(0, p, -1).start()

    def pass_on(s):
        for p in range(PIECES):
            hop(s - 1, p, 1, 1).wait_recv()
            hop(s, p, 1).start()
            hop(s - 1, p, -1, 1).wait_recv()

            @pl.when(s < steps_l)
            def _():
                hop(s, p, -1).start()

    for p in range(4):
        by_tx.relay(p)
    pass_on(jnp.int32(1))
    by_pair.arrive()
    for p in range(4):
        by_tx.arrive(p)
    everything = t_all[...].reshape(256, 2048)
    scale = jnp.where(lanes_below((256, 128), HD), HD**-0.5, 1.0)
    for a in range(2):
        both = (contract(everything, pair_all[a], 1, 1) * scale).astype(BF16)
        chosen = jnp.dot(pick[...], both, preferred_element_type=F32)
        block[96 * a : 96 * a + 96] = jnp.where(
            lanes_below((96, 128), HD), chosen[:96], chosen[96:]
        ).astype(BF16)
    by_q = ToReaders(block, blocks, q_s, q_r)
    by_q.start()
    pass_on(jnp.int32(2))
    m[...] = jnp.full(m.shape, -1e30, F32)
    l[...] = jnp.zeros(l.shape, F32)
    o[...] = jnp.zeros(o.shape, F32)
    by_q.arrive()
    qa[...] = blocks[...].reshape(qa.shape)

    def attend(at):
        block = kv_all[at]
        keys = jnp.where(lanes_below(block.shape, HD), block, jnp.zeros_like(block))
        scores = contract(keys, qa[...], 1, 1)
        top = jnp.maximum(m[...], jnp.max(scores, axis=0, keepdims=True))
        weights = jnp.exp(scores - top)
        old = jnp.exp(m[...] - top)
        m[...] = top
        l[...] = l[...] * old + jnp.sum(weights, axis=0, keepdims=True)
        o[...] = o[...] * old + contract(block, weights.astype(BF16), 0, 0)[HD:]

    def attend_both(d):
        attend(lax.rem(z + nz - d, nz))
        attend(lax.rem(z + d, nz))

    attend(z)
    attend_both(1)

    def step(s, carry):
        pass_on(s)
        attend_both(s - 1)
        return carry

    lax.fori_loop(3, steps_r, step, 0)
    attend_both(steps_r - 1)
    for p in range(PIECES):
        hop(steps_r - 1, p, 1, 1).wait_recv()
    attend(lax.rem(z + nz - steps_r, nz))
    upright = jnp.transpose(qa[...].astype(F32))
    delta = jnp.sum(upright[HD:] * o[...], axis=0, keepdims=True)
    row = lax.broadcasted_iota(jnp.int32, (8, qa.shape[0]), 0)
    said[...] = jnp.where(row == 0, m[...], jnp.where(row == 1, l[...], delta))
    by_stats = Exchange(("x",), said, heard, ss, sr)
    by_stats.start()
    by_stats.arrive()
    top = jnp.max(heard[:, 0:1], axis=0)
    total = jnp.zeros_like(top)
    both = jnp.zeros_like(top)
    for j in range(4):
        w = jnp.exp(heard[j, 0:1] - top)
        total = total + w * heard[j, 1:2]
        both = both + w * heard[j, 2:3]
    stats[...] = jnp.where(row == 0, top + jnp.log(total), both / total)
    scaled = o[...] * (jnp.exp(m[...] - top) / total)
    upright = jnp.concatenate([scaled, jnp.zeros_like(scaled)], axis=0)
    out[...] = jnp.transpose(upright).astype(BF16).reshape(out.shape)

    by_o = ToOwners(out, outs, o_s, o_r)
    by_o.start()
    dq[...] = jnp.zeros(dq.shape, F32)

    def grads(side, j):
        at = lax.rem(z + nz - nz // 2 + j, nz) if side == 0 else lax.rem(z + nz // 2 - 1 - j, nz)
        block = kv_all[at]
        low = lanes_below(block.shape, HD)
        none = jnp.zeros_like(block)
        scores = contract(jnp.where(low, block, none), qa[...], 1, 1)
        probs = jnp.exp(scores - stats[0:1])
        d_probs = contract(jnp.where(low, none, block), qa[...], 1, 1)
        d_scores = (probs * (d_probs - stats[1:2])).astype(BF16)
        for_v = contract(probs.astype(BF16), qa[...], 1, 0)
        for_k = contract(d_scores, qa[...], 1, 0)
        dq[...] += contract(block, d_scores, 0, 0)[:HD]
        mine[side, j] = jnp.where(lanes_below(for_k.shape, HD), for_k, for_v)

    main = RingSum(nz, lambda side, j, at: mine[side, j, at], ring_out, ring_in, g_s, g_r, PIECES)

    def own_weight(side, j, at):
        to = lax.rem(z + nz - nz // 2 + j, nz) if side == 0 else lax.rem(z + nz // 2 - 1 - j, nz)
        return swapped[0, to, at].astype(F32) + swapped[1, to, at].astype(F32)

    weight = RingSum(nz, own_weight, w_ring_out, w_ring_in, h_s, h_r, 1)
    for side in range(2):
        grads(side, 0)
        main.first(side)
    for side in range(2):
        grads(side, 1)

    by_o.arrive()
    attended = jnp.sum(outs[...].astype(F32), axis=0).astype(BF16)
    for a in range(2):
        spread = contract(pick[96:], attended[96 * a : 96 * a + 96], 0, 0).astype(BF16)
        product = contract(spread, t_all[...].reshape(256, 2048), 0, 0)[:HD].astype(BF16)
        for i in range(nz):
            o_part[a, i] = product[:, 128 * i : 128 * i + 128]
    swap = Exchange(("c",), o_part, swapped, sw_s, sw_r, lambda at, i: i)
    swap.start()
    for side in range(2):
        main.step(1, side)
    for side in range(2):
        grads(side, 2)
        grads(side, 3)
    swap.arrive()
    for side in range(2):
        weight.first(side)

    def ahead(s, carry):
        for side in range(2):
            main.step(s, side)
        for side in range(2):
            weight.step(s - 1, side)
        for side in range(2):
            grads(side, 2 * s)
            grads(side, 2 * s + 1)
        return carry

    lax.fori_loop(2, nz // 4, ahead, 0)
    upright = jnp.concatenate([dq[...], jnp.zeros_like(dq[...])], axis=0) * HD**-0.5
    dq_block[...] = jnp.transpose(upright).astype(BF16).reshape(4, 192, 128)
    by_dq = ToOwners(dq_block, dqs, dq_s, dq_r)
    by_dq.start()
    by_t = Exchange(("x", "y"), d_parts, t_in, t_s, t_r, lambda at, i: i)

    def behind(s, carry):
        main.step(s, 0)

        @pl.when(s < nz // 2 - 1)
        def _():
            main.step(s, 1)

        for side in range(2):
            weight.step(s - 1, side)

        @pl.when(s == nz // 4)
        def _():
            by_dq.arrive()
            query_grad = jnp.sum(dqs[...].astype(F32), axis=0).astype(BF16)
            d_target = jnp.zeros((128, 2048), F32)
            for a in range(2):
                spread = contract(pick8[...], query_grad[96 * a : 96 * a + 96], 0, 0).astype(BF16)
                d_target = d_target + jnp.dot(spread, pair_all[a], preferred_element_type=F32)
            d_parts[...] = d_target.astype(BF16).reshape(16, 8, 2048)
            by_t.start()

        return carry

    lax.fori_loop(nz // 4, nz // 2, behind, 0)
    weight.step(nz // 2 - 1, 0)
    for p in range(PIECES):
        kv_grad[pl.ds(p * piece, piece)] = main.total(p).astype(BF16)
    by_kv = Exchange(("c",), kv_grad, grads2, kv_s, kv_r)
    by_kv.start()
    by_kv.arrive()
    g0, g1 = grads2[0].astype(F32), grads2[1].astype(F32)
    k2 = jnp.where(wide_low, g0, swap_halves(g1)).astype(BF16)
    v2 = jnp.where(wide_low, swap_halves(g0), g1).astype(BF16)
    d_rows = contract(k2, w_all[:, :, 0].reshape(1024, 128), 1, 1)
    d_rows = d_rows + contract(v2, w_all[:, :, 1].reshape(1024, 128), 1, 1)
    parts[...] = d_rows.astype(BF16).reshape(8, 32, 1024)
    by_s = Exchange(("y", "c"), parts, s_in, s_s, s_r, lambda at, i: i)
    by_s.start()
    mine_sum[...] = weight.total(0).astype(BF16)
    back = FarGather(nz, mine_sum, all_sums, back_s, back_r)
    back.start()
    by_t.arrive()
    t_out[...] = jnp.sum(t_in[...].astype(F32), axis=0)
    back.relay()
    by_s.arrive()
    got = []
    for core in range(2):
        total = s_in[core].astype(F32)
        for i in range(1, 4):
            total = total + s_in[2 * i + core].astype(F32)
        got.append(total)
    for j in range(8):
        chip = (2 * j % 4) * 4 + j // 2
        a, b = (g[:, 128 * j : 128 * j + 128] for g in got)
        s_out[:, 128 * chip : 128 * chip + 128] = jnp.where(low, a, swap_halves(b))
        s_out[:, 128 * chip + 512 : 128 * chip + 640] = jnp.where(low, swap_halves(a), b)
    back.arrive()
    for i in range(nz):
        w_out[:, 128 * i : 128 * i + 128] = all_sums[i].astype(F32)
    for by in (by_stats, by_o, by_dq, swap, back, by_kv, by_s, by_t, main, weight):
        by.drain()
    for by in (by_rows, by_wy, by_wx, by_ty, by_tx, by_pair, by_part, by_q):
        by.drain()

    def drain_gather(s, carry):
        for p in range(PIECES):
            hop(s, p, 1).wait_send()

            @pl.when(s < steps_l)
            def _():
                hop(s, p, -1).wait_send()

        return carry

    lax.fori_loop(0, steps_r, drain_gather, 0)


def whole(args, nz):
    t = 768
    half = nz // 2
    ring = sems(half, PIECES)

    def bf16(*shape):
        return pltpu.VMEM(shape, BF16)

    def f32(*shape):
        return pltpu.VMEM(shape, F32)

    return pl.pallas_call(
        functools.partial(kernel, nz),
        out_shape=(
            jax.ShapeDtypeStruct((32, 2048), F32),
            jax.ShapeDtypeStruct((8, 2048), F32),
            jax.ShapeDtypeStruct((64, 2048), F32),
        ),
        in_specs=[VMEM] * len(args),
        out_specs=(VMEM,) * 3,
        scratch_shapes=[
            bf16(nz, 256, 128), f32(8, t), bf16(4, 192, 128), bf16(t, 128),
            bf16(4, 4, 16, 2048), bf16(2, 128, 2048), bf16(4, 4, 2, 64, 128),
            bf16(2, 32, 1024), bf16(4, 2, 32, 1024), f32(2, 256, 128), f32(2, 256, 128),
            bf16(192, 128), bf16(4, 192, 128), f32(1, t), f32(1, t), f32(HD, t), f32(8, t), f32(4, 8, t),
            f32(HD, t), f32(2, half, 256, 128), bf16(2, half, 256, 128), bf16(2, half, 256, 128),
            bf16(2, half, HD, 128), bf16(2, half, HD, 128),
            bf16(4, 192, 128), bf16(4, 192, 128), bf16(4, 192, 128),
            bf16(2, nz, HD, 128), bf16(2, nz, HD, 128), bf16(HD, 128), bf16(nz, HD, 128),
            bf16(256, 128), bf16(2, 256, 128), bf16(8, 32, 1024), bf16(16, 8, 2048),
            bf16(8, 32, 1024), bf16(16, 8, 2048),
            sems(5, 2), sems(5, 2), sems(4, 2), sems(4, 2), sems(3, 4), sems(3, 4),
            sems(3, 2), sems(3, 2), sems(3, 4), sems(3, 4), dma(2), dma(2),
            dma(2), dma(2), dma(4), dma(4), ring, ring, ring, ring, dma(4), dma(4),
            dma(4), dma(4), dma(4), dma(4), dma(2), dma(2),
            sems(2, half, PIECES), sems(2, half, PIECES), sems(2, half, 1), sems(2, half, 1),
            sems(4, REACH), sems(4, REACH),
            dma(2), dma(2), dma(8), dma(8), dma(16), dma(16),
        ],
        compiler_params=params(0),
    )(*args)


def norm_back(matrix, gain, upstream):
    wide = matrix.astype(F32)
    factor = lax.rsqrt(jnp.mean(wide * wide, axis=-1, keepdims=True) + EPSILON)
    weighted = upstream * gain
    inner = jnp.mean(weighted * wide, axis=-1, keepdims=True)
    return factor * weighted - wide * factor**3 * inner


def picks():
    r = jnp.arange(96)
    at = 16 * (r // 6) + r % 6
    pick = jnp.concatenate([at, at + 8])[:, None] == jnp.arange(256)[None]
    pick8 = (8 * (r // 6) + r % 6)[:, None] == jnp.arange(128)[None]
    return pick.astype(BF16), pick8.astype(BF16)


def body(nz, target_rows, source_rows, t_gain, s_gain, wq, wk, wv, wo, cot):
    pick, pick8 = picks()
    pair = jnp.concatenate([wq.T, wo])
    d_source, d_target, o_grad = whole(
        (target_rows, source_rows, t_gain[None], s_gain[None], pair, wk, wv, cot, pick, pick8), nz
    )
    source_grad = norm_back(source_rows, s_gain, d_source)
    target_grad = cot.astype(F32) + norm_back(target_rows, t_gain, d_target[:6])
    return target_grad, source_grad, o_grad


def solution(mesh):
    nz = mesh.shape["sp"]
    SIZES["z"] = nz
    fine = Mesh(mesh.devices.reshape(nz, 4, 4, 2), ("z", "y", "x", "c"))
    every, plane = ("z", "y", "x", "c"), ("y", "x", "c")
    return jax.shard_map(
        functools.partial(body, nz),
        mesh=fine,
        in_specs=(
            P(every, None), P(every, None), P(), P(),
            P(None, plane), P(plane, None), P(plane, None), P(plane, None), P(every, None),
        ),
        out_specs=(P(every, None), P(every, None), P(plane, None)),
        check_vma=False,
    )
```

```python
import functools

import jax
import jax.numpy as jnp
import numpy as np
from jax import lax
from jax.experimental import pallas as pl
from jax.experimental.pallas import tpu as pltpu
from jax.sharding import Mesh
from jax.sharding import PartitionSpec as P

MESH = pl.DeviceIdType.MESH
HD = 64
EPSILON = 1e-06
F32, BF16 = jnp.float32, jnp.bfloat16
VMEM = pl.BlockSpec(memory_space=pltpu.VMEM)
SIZES = {"y": 4, "x": 4, "c": 2}
PIECES = 2
REACH = 4


def dma(n):
    return pltpu.SemaphoreType.DMA((n,))


def params(cid):
    return pltpu.CompilerParams(
        collective_id=cid, has_side_effects=True, vmem_limit_bytes=62 * 1024 * 1024
    )


def group_size(axes):
    n = 1
    for a in axes:
        n *= SIZES[a]
    return n


def group_index(axes):
    i = 0
    for a in axes:
        i = i * SIZES[a] + lax.axis_index(a)
    return i


def coords_of(index, axes):
    out = {}
    for a in reversed(axes):
        out[a] = lax.rem(index, SIZES[a])
        index = index // SIZES[a]
    return out


def greet(axes):
    n, me = group_size(axes), group_index(axes)
    sem = pltpu.get_barrier_semaphore()

    def one(k, carry):
        pl.semaphore_signal(
            sem, inc=1, device_id=coords_of(lax.rem(me + k, n), axes), device_id_type=MESH
        )
        return carry

    lax.fori_loop(1, n, one, 0)
    return n - 1


def greeted(count):
    pl.semaphore_wait(pltpu.get_barrier_semaphore(), count)


class Exchange:
    def __init__(self, axes, src, dst, send, recv, pick=None):
        self.axes, self.src, self.dst, self.send, self.recv = axes, src, dst, send, recv
        self.n, self.me = group_size(axes), group_index(axes)
        self.pick = pick

    def block(self, index):
        if self.pick is None:
            return self.src
        return self.src.at[self.pick(coords_of(index, self.axes), index)]

    def copy(self, k, slot):
        to = lax.rem(self.me + k, self.n)
        return pltpu.make_async_remote_copy(
            src_ref=self.block(to),
            dst_ref=self.dst.at[slot],
            send_sem=self.send.at[0],
            recv_sem=self.recv.at[0],
            device_id=coords_of(to, self.axes),
            device_id_type=MESH,
        )

    def start(self):
        def one(k, carry):
            self.copy(k, self.me).start()
            return carry

        lax.fori_loop(1, self.n, one, 0)
        self.dst[self.me] = self.block(self.me)[...]

    def others(self):
        return bulk(self.dst.at[pl.ds(0, self.n - 1)], self.send, self.recv)

    def arrive(self):
        self.others().wait_recv()

    def drain(self):
        self.others().wait_send()


def bulk(ref, send, recv):
    return pltpu.make_async_remote_copy(
        src_ref=ref,
        dst_ref=ref,
        send_sem=send.at[0],
        recv_sem=recv.at[0],
        device_id={"c": 1 - lax.axis_index("c")},
        device_id_type=MESH,
    )


class ToReaders:
    def __init__(self, src, dst, send, recv):
        self.src, self.dst, self.send, self.recv = src, dst, send, recv
        self.y, self.x, self.c = (lax.axis_index(a) for a in "yxc")
        self.mine = self.x // 2 == self.c

    def copy(self, k, slot):
        return pltpu.make_async_remote_copy(
            src_ref=self.src,
            dst_ref=self.dst.at[slot],
            send_sem=self.send.at[k],
            recv_sem=self.recv.at[slot],
            device_id={"x": lax.rem(self.x + k, 4), "c": self.x // 2},
            device_id_type=MESH,
        )

    def slot(self):
        return lax.rem(self.x, 2) * 2 + self.c

    def start(self):
        for k in range(1, 4):
            self.copy(k, self.slot()).start()

        @pl.when(jnp.logical_not(self.mine))
        def _():
            self.copy(0, self.slot()).start()

        @pl.when(self.mine)
        def _():
            self.dst[self.slot()] = self.src[...]

    def arrive(self):
        for s in range(4):
            own = jnp.logical_and(2 * self.c + s // 2 == self.x, self.c == s % 2)

            @pl.when(jnp.logical_not(own))
            def _():
                self.copy(1, s).wait_recv()

    def drain(self):
        for k in range(1, 4):
            self.copy(k, self.slot()).wait_send()

        @pl.when(jnp.logical_not(self.mine))
        def _():
            self.copy(0, self.slot()).wait_send()


class ToOwners:
    def __init__(self, src, dst, send, recv):
        self.src, self.dst, self.send, self.recv = src, dst, send, recv
        self.y, self.x, self.c = (lax.axis_index(a) for a in "yxc")

    def copy(self, s, slot):
        return pltpu.make_async_remote_copy(
            src_ref=self.src.at[s],
            dst_ref=self.dst.at[slot],
            send_sem=self.send.at[s],
            recv_sem=self.recv.at[slot],
            device_id={"x": 2 * self.c + s // 2, "c": jnp.int32(s % 2)},
            device_id_type=MESH,
        )

    def own(self, s):
        return jnp.logical_and(2 * self.c + s // 2 == self.x, self.c == s % 2)

    def start(self):
        for s in range(4):
            @pl.when(jnp.logical_not(self.own(s)))
            def _():
                self.copy(s, self.x).start()

            @pl.when(self.own(s))
            def _():
                self.dst[self.x] = self.src[s]

    def arrive(self):
        for j in range(4):
            own = jnp.logical_and(self.x == j, self.x // 2 == self.c)

            @pl.when(jnp.logical_not(own))
            def _():
                self.copy(0, j).wait_recv()

    def drain(self):
        for s in range(4):
            @pl.when(jnp.logical_not(self.own(s)))
            def _():
                self.copy(s, self.x).wait_send()


def lanes_below(shape, bound):
    return lax.broadcasted_iota(jnp.int32, shape, 1) < bound


def contract(a, b, da, db):
    return lax.dot_general(a, b, (((da,), (db,)), ((), ())), preferred_element_type=F32)


def ring_greet(nz):
    z = lax.axis_index("z")
    sem = pltpu.get_barrier_semaphore()
    right, left = lax.rem(z + 1, nz), lax.rem(z + nz - 1, nz)
    for to in (left, right):
        pl.semaphore_signal(sem, inc=1, device_id={"z": to}, device_id_type=MESH)
    return 2


class RingGather:
    def __init__(self, axis, piece, count, three, send, recv):
        self.axis, self.piece, self.count, self.send, self.recv = axis, piece, count, send, recv
        self.three = three
        self.me = lax.axis_index(axis)

    def at(self, offset):
        return lax.rem(self.me + offset + 4, 4)

    def copy(self, slot, p, sign, kind):
        ref = self.piece(slot, p)
        return pltpu.make_async_remote_copy(
            src_ref=ref,
            dst_ref=ref,
            send_sem=self.send.at[0],
            recv_sem=self.recv.at[kind, p],
            device_id={self.axis: self.at(sign)},
            device_id_type=MESH,
        )

    def start(self, p):
        self.copy(self.me, p, 1, 0).start()
        self.copy(self.me, p, -1, 1).start()

    def relay(self, p):
        self.copy(self.at(-1), p, 1, 0).wait_recv()
        self.copy(self.at(1), p, -1, 1).wait_recv()
        if p < self.count // 2:
            self.copy(self.at(-1), p, 1, 2).start()
        else:
            self.copy(self.at(1), p, -1, 2).start()

    def arrive(self, p):
        self.copy(self.at(2), p, 1, 2).wait_recv()

    def drain(self):
        bulk(self.three, self.send, self.send).wait_send()


class RowGather:
    def __init__(self, halves, out, send, recv):
        self.halves, self.out, self.send, self.recv = halves, out, send, recv
        self.y, self.c = lax.axis_index("y"), lax.axis_index("c")

    def at(self, offset):
        return lax.rem(self.y + offset + 4, 4)

    def first(self, sign, core, slot_y, slot_c):
        kind = 0 if sign > 0 else 1
        return pltpu.make_async_remote_copy(
            src_ref=self.halves.at[core],
            dst_ref=self.out.at[slot_y, slot_c],
            send_sem=self.send.at[kind, core],
            recv_sem=self.recv.at[kind, slot_c],
            device_id={"y": self.at(sign), "c": jnp.int32(core)},
            device_id_type=MESH,
        )

    def partner(self, slot_c):
        return pltpu.make_async_remote_copy(
            src_ref=self.halves.at[1 - self.c],
            dst_ref=self.out.at[self.y, slot_c],
            send_sem=self.send.at[4, 0],
            recv_sem=self.recv.at[4, 0],
            device_id={"c": 1 - self.c},
            device_id_type=MESH,
        )

    def second(self, sign, slot_y, slot_c):
        kind = 2 if sign > 0 else 3
        ref = self.out.at[slot_y, slot_c, pl.ds(0 if sign > 0 else 16, 16)]
        return pltpu.make_async_remote_copy(
            src_ref=ref,
            dst_ref=ref,
            send_sem=self.send.at[kind, slot_c],
            recv_sem=self.recv.at[kind, slot_c],
            device_id={"y": self.at(sign)},
            device_id_type=MESH,
        )

    def start(self):
        for core in range(2):
            self.first(1, core, self.y, self.c).start()
            self.first(-1, core, self.y, self.c).start()
        self.partner(self.c).start()
        self.out[self.y, self.c] = self.halves[self.c]

    def relay(self):
        for core in range(2):
            self.first(1, 0, self.at(-1), core).wait_recv()
            self.second(1, self.at(-1), core).start()
            self.first(-1, 0, self.at(1), core).wait_recv()
            self.second(-1, self.at(1), core).start()

    def arrive(self):
        self.partner(1 - self.c).wait_recv()
        for core in range(2):
            self.second(1, self.at(2), core).wait_recv()
            self.second(-1, self.at(2), core).wait_recv()

    def drain(self):
        self.partner(self.c).wait_send()
        for core in range(2):
            self.first(1, core, self.y, self.c).wait_send()
            self.first(-1, core, self.y, self.c).wait_send()
            self.second(1, self.y, core).wait_send()
            self.second(-1, self.y, core).wait_send()


class WeightColumn:
    def __init__(self, wk, wv, out, send, recv):
        self.parts, self.out, self.send, self.recv = (wk, wv), out, send, recv
        self.y, self.x = lax.axis_index("y"), lax.axis_index("x")

    def lanes(self, y):
        return pl.ds(pl.multiple_of(y * 128, 128), 128)

    def copy(self, k, i, slot_y):
        to = lax.rem(self.y + k, 4)
        return pltpu.make_async_remote_copy(
            src_ref=self.parts[i].at[:, self.lanes(to)],
            dst_ref=self.out.at[self.x, slot_y, i],
            send_sem=self.send.at[0],
            recv_sem=self.recv.at[0],
            device_id={"y": to},
            device_id_type=MESH,
        )

    def start(self):
        for k in (2, 1, 3):
            for i in range(2):
                self.copy(k, i, self.y).start()
        for i in range(2):
            self.out[self.x, self.y, i] = self.parts[i][:, self.lanes(self.y)]

    def others(self):
        return bulk(self.out.at[self.x, pl.ds(0, 3)], self.send, self.recv)

    def arrive(self):
        self.others().wait_recv()

    def drain(self):
        self.others().wait_send()


def unit_rows(matrix, gain):
    wide = matrix.astype(F32)
    factor = lax.rsqrt(jnp.mean(wide * wide, axis=-1, keepdims=True) + EPSILON)
    return wide * factor * gain


def swap_halves(a):
    return pltpu.roll(a, HD, 1)


class StrideGather:
    def __init__(self, nz, blocks, send, recv):
        self.nz, self.blocks, self.send, self.recv = nz, blocks, send, recv
        self.z = lax.axis_index("z")
        self.rows = blocks.shape[1] // PIECES
        self.far = {1: nz // 2, -1: nz - 1 - nz // 2}

    def at(self, offset):
        return lax.rem(self.z + offset + self.nz, self.nz)

    def copy(self, sign, distance, d, p):
        ref = self.blocks.at[self.at(-sign * distance), pl.ds(p * self.rows, self.rows)]
        return pltpu.make_async_remote_copy(
            src_ref=ref,
            dst_ref=ref,
            send_sem=self.send.at[0],
            recv_sem=self.recv.at[0 if sign > 0 else 1, distance + d - 1, p],
            device_id={"z": self.at(sign * d)},
            device_id_type=MESH,
        )

    def arrived(self, sign, distance, p):
        ref = self.blocks.at[self.at(-sign * distance), pl.ds(p * self.rows, self.rows)]
        return pltpu.make_async_remote_copy(
            src_ref=ref,
            dst_ref=ref,
            send_sem=self.send.at[0],
            recv_sem=self.recv.at[0 if sign > 0 else 1, distance - 1, p],
            device_id={"z": self.at(sign)},
            device_id_type=MESH,
        )

    def start(self):
        for d in (2, 1):
            for p in range(PIECES):
                for sign in (1, -1):
                    self.copy(sign, 0, d, p).start()

    def relay(self, distance):
        for p in range(PIECES):
            for sign in (1, -1):
                if distance <= self.far[sign]:
                    self.arrived(sign, distance, p).wait_recv()
                if distance + 2 <= self.far[sign]:
                    self.copy(sign, distance, 2, p).start()
        for p in range(PIECES):
            for sign in (1, -1):
                if distance + 1 <= self.far[sign]:
                    self.copy(sign, distance, 1, p).start()

    def arrive(self, distance):
        for sign in (1, -1):
            if distance <= self.far[sign]:
                for p in range(PIECES):
                    self.arrived(sign, distance, p).wait_recv()

    def drain(self):
        bulk(self.blocks.at[pl.ds(0, self.nz - 1)], self.send, self.send).wait_send()


class StrideSum:
    def __init__(self, nz, term, out, arrived, send, recv, pieces):
        self.nz, self.term, self.out, self.arrived = nz, term, out, arrived
        self.send, self.recv, self.pieces = send, recv, pieces
        self.rows = out.shape[2] // pieces
        self.z = lax.axis_index("z")

    def chained(self, side, j):
        return (j + side) % 2 == 0

    def hop(self, side, j, p):
        at = pl.ds(p * self.rows, self.rows)
        d = (2 if self.chained(side, j) else 1) * (1 if side else -1)
        return pltpu.make_async_remote_copy(
            src_ref=self.out.at[side, j, at],
            dst_ref=self.arrived.at[side, j, at],
            send_sem=self.send.at[side],
            recv_sem=self.recv.at[side, j, p],
            device_id={"z": lax.rem(self.z + d + self.nz, self.nz)},
            device_id_type=MESH,
        )

    def joined(self, side, j, p, value):
        at = pl.ds(p * self.rows, self.rows)
        for i in (j - 1, j - 2):
            if i >= 0:
                self.hop(side, i, p).wait_recv()
                value = value + self.arrived[side, i, at].astype(F32)
        return value

    def step(self, side, j):
        for p in range(self.pieces):
            at = pl.ds(p * self.rows, self.rows)
            value = self.term(side, j, at)
            if self.chained(side, j):
                value = self.joined(side, j, p, value)
            self.out[side, j, at] = value.astype(BF16)
            self.hop(side, j, p).start()

    def total(self, p):
        half = self.nz // 2
        at = pl.ds(p * self.rows, self.rows)
        value = self.joined(1, half - 1, p, self.term(1, half - 1, at))
        return self.joined(0, half, p, value)

    def drain(self):
        half = self.nz // 2
        for side in range(2):
            sem = self.send.at[pl.ds(side, 1)]
            bulk(self.out.at[side, pl.ds(0, half - side)], sem, sem).wait_send()


class FarGather:
    def __init__(self, nz, src, dst, send, recv):
        self.nz, self.src, self.dst, self.send, self.recv = nz, src, dst, send, recv
        self.z = lax.axis_index("z")
        self.far = {1: nz // 2 - REACH, -1: nz - 1 - nz // 2 - REACH}

    def at(self, offset):
        return lax.rem(self.z + offset + self.nz, self.nz)

    def copy(self, slot, sign, d, relay):
        kind = 3 if relay else 2 if d < REACH else 0 if sign > 0 else 1
        return pltpu.make_async_remote_copy(
            src_ref=self.dst.at[slot] if relay else self.src,
            dst_ref=self.dst.at[slot],
            send_sem=self.send.at[0],
            recv_sem=self.recv.at[kind],
            device_id={"z": self.at(sign * d)},
            device_id_type=MESH,
        )

    def several(self, count, kind):
        return bulk(self.dst.at[pl.ds(0, count)], self.send, self.recv.at[pl.ds(kind, 1)])

    def start(self):
        for d in range(REACH, 0, -1):
            for sign in (1, -1):
                self.copy(self.z, sign, d, False).start()
        self.dst[self.z] = self.src[...]

    def relay(self):
        for sign in (1, -1):
            slot = self.at(-sign * REACH)
            self.copy(slot, sign, REACH, False).wait_recv()
            for d in range(self.far[sign], 0, -1):
                self.copy(slot, sign, d, True).start()

    def arrive(self):
        self.several(2 * REACH - 2, 2).wait_recv()
        self.several(self.nz - 1 - 2 * REACH, 3).wait_recv()

    def drain(self):
        self.several(self.nz - 1, 0).wait_send()


def reach_greet(nz):
    z = lax.axis_index("z")
    for d in range(1, REACH + 1):
        for sign in (1, -1):
            pl.semaphore_signal(
                pltpu.get_barrier_semaphore(),
                inc=1,
                device_id={"z": lax.rem(z + sign * d + nz, nz)},
                device_id_type=MESH,
            )
    return 2 * REACH


def sems(*shape):
    return pltpu.SemaphoreType.DMA(shape)


def norm_back(matrix, gain, upstream):
    wide = matrix.astype(F32)
    factor = lax.rsqrt(jnp.mean(wide * wide, axis=-1, keepdims=True) + EPSILON)
    weighted = upstream * gain
    inner = jnp.mean(weighted * wide, axis=-1, keepdims=True)
    return factor * weighted - wide * factor**3 * inner


def kernel(
    nz, target_rows, source_rows, t_gain, s_gain, wq, wk, wv, wo, cot, pick, pick8,
    s_out, t_out, w_out,
    pair, kv_all, stats, out, qa, t_all, pair_all, w_all,
    halves, rows_all, part, part_all, block, blocks, m, l, o, said, heard,
    dq, mine, ring_out, ring_in, w_ring_out, w_ring_in, outs, dq_block, dqs, o_part, swapped,
    mine_sum, all_sums, upstream_s, kv_grad, grads2, parts, d_parts, s_in, t_in,
    row_s, row_r, wy_s, wy_r, wx_s, wx_r, ya_s, ya_r, xb_s, xb_r, xa_s, xa_r, yb_s, yb_r, pair_s, pair_r,
    part_s, part_r, q_s, q_r, z_s, z_r, ss, sr,
    o_s, o_r, dq_s, dq_r, sw_s, sw_r, g_s, g_r, h_s, h_r, back_s, back_r,
    kv_s, kv_r, s_s, s_r, t_s, t_r,
):
    z, y, x, c = (lax.axis_index(a) for a in "zyxc")
    met = greet(("y", "x", "c")) + reach_greet(nz)

    normed = unit_rows(source_rows[...], s_gain[...])
    low = lanes_below((32, 128), HD)
    for j in range(8):
        chip = (2 * j % 4) * 4 + j // 2
        first, second = (normed[:, 128 * i : 128 * i + 128] for i in (chip, chip + 4))
        halves[0, :, 128 * j : 128 * j + 128] = jnp.where(low, first, swap_halves(second)).astype(BF16)
        halves[1, :, 128 * j : 128 * j + 128] = jnp.where(low, swap_halves(first), second).astype(BF16)
    pair[:HD] = jnp.transpose(wq[...].astype(F32)).astype(BF16)
    pair[HD:] = wo[...]
    greeted(met)

    by_rows = RowGather(halves, rows_all, row_s, row_r)
    by_wy = WeightColumn(wk, wv, w_all, wy_s, wy_r)
    by_wx = RingGather("x", lambda slot, p: w_all.at[slot, p], 4, w_all.at[pl.ds(0, 3)], wx_s, wx_r)
    three, first, second = pl.ds(0, 3), pl.ds(0, 1024), pl.ds(1024, 1024)
    by_ya = RingGather(
        "y", lambda slot, p: t_all.at[x, slot, :, pl.ds(512 * p, 512)], 2,
        t_all.at[x, three, :, first], ya_s, ya_r,
    )
    by_xb = RingGather(
        "x", lambda slot, p: t_all.at[slot, y, :, pl.ds(1024 + 512 * p, 512)], 2,
        t_all.at[three, y, :, second], xb_s, xb_r,
    )
    by_xa = RingGather(
        "x", lambda slot, p: t_all.at[slot, p, :, first], 4, t_all.at[three, :, :, first], xa_s, xa_r
    )
    by_yb = RingGather(
        "y", lambda slot, p: t_all.at[p, slot, :, second], 4, t_all.at[:, three, :, second], yb_s, yb_r
    )
    by_pair = Exchange(("c",), pair, pair_all, pair_s, pair_r)
    by_wy.start()
    by_rows.start()
    zero = jnp.zeros((2, target_rows.shape[1]), F32)
    t_all[x, y] = jnp.concatenate(
        [unit_rows(target_rows[...], t_gain[...]), zero, cot[...].astype(F32), zero], axis=0
    ).astype(BF16)
    for p in range(2):
        by_xb.start(p)
        by_ya.start(p)
    by_pair.start()

    by_wy.arrive()
    for p in range(4):
        by_wx.start(p)
    by_rows.relay()
    for p in range(4):
        by_wx.relay(p)
    for p in range(2):
        by_xb.relay(p)
        by_ya.relay(p)
    by_rows.arrive()
    for p in range(4):
        by_wx.arrive(p)

    rows = rows_all[...].reshape(256, 1024)
    k2 = jnp.dot(rows, w_all[:, :, 0].reshape(1024, 128), preferred_element_type=F32)
    v2 = jnp.dot(rows, w_all[:, :, 1].reshape(1024, 128), preferred_element_type=F32)
    wide_low = lanes_below((256, 128), HD)
    part[0] = jnp.where(wide_low, k2, swap_halves(v2))
    part[1] = jnp.where(wide_low, swap_halves(k2), v2)
    by_part = Exchange(("c",), part, part_all, part_s, part_r, lambda at, i: i)
    by_part.start()
    for p in range(2):
        by_xb.arrive(p)
        by_ya.arrive(p)
    for p in range(4):
        by_xa.start(p)
        by_yb.start(p)
    by_part.arrive()
    kv_all[z] = (part_all[0] + part_all[1]).astype(BF16)

    by_z = StrideGather(nz, kv_all, z_s, z_r)
    by_z.start()
    for p in range(4):
        by_xa.relay(p)
        by_yb.relay(p)
    by_z.relay(2)
    by_pair.arrive()
    for p in range(4):
        by_xa.arrive(p)
        by_yb.arrive(p)
    everything = t_all[...].reshape(256, 2048)
    scale = jnp.where(lanes_below((256, 128), HD), HD**-0.5, 1.0)
    for a in range(2):
        both = (contract(everything, pair_all[a], 1, 1) * scale).astype(BF16)
        chosen = jnp.dot(pick[...], both, preferred_element_type=F32)
        block[96 * a : 96 * a + 96] = jnp.where(
            lanes_below((96, 128), HD), chosen[:96], chosen[96:]
        ).astype(BF16)
    by_q = ToReaders(block, blocks, q_s, q_r)
    by_q.start()
    by_z.relay(4)
    m[...] = jnp.full(m.shape, -1e30, F32)
    l[...] = jnp.zeros(l.shape, F32)
    o[...] = jnp.zeros(o.shape, F32)
    by_q.arrive()
    qa[...] = blocks[...].reshape(qa.shape)

    def attend(at):
        block = kv_all[at]
        keys = jnp.where(lanes_below(block.shape, HD), block, jnp.zeros_like(block))
        scores = contract(keys, qa[...], 1, 1)
        top = jnp.maximum(m[...], jnp.max(scores, axis=0, keepdims=True))
        weights = jnp.exp(scores - top)
        old = jnp.exp(m[...] - top)
        m[...] = top
        l[...] = l[...] * old + jnp.sum(weights, axis=0, keepdims=True)
        o[...] = o[...] * old + contract(block, weights.astype(BF16), 0, 0)[HD:]

    def attend_from(low, high):
        def one(i, carry):
            d = low + i // 2
            attend(lax.rem(z + nz + jnp.where(lax.rem(i, 2) == 0, d, -d), nz))
            return carry

        lax.fori_loop(0, 2 * (high - low + 1), one, 0)

    attend(z)
    by_z.arrive(1)
    attend_from(1, 2)
    by_z.relay(6)
    by_z.arrive(3)
    by_z.arrive(5)
    attend_from(3, 6)
    by_z.arrive(7)
    attend_from(7, 7)
    by_z.arrive(8)
    attend(lax.rem(z + nz // 2, nz))
    upright = jnp.transpose(qa[...].astype(F32))
    delta = jnp.sum(upright[HD:] * o[...], axis=0, keepdims=True)
    row = lax.broadcasted_iota(jnp.int32, (8, qa.shape[0]), 0)
    said[...] = jnp.where(row == 0, m[...], jnp.where(row == 1, l[...], delta))
    by_stats = Exchange(("x",), said, heard, ss, sr)
    by_stats.start()
    by_stats.arrive()
    top = jnp.max(heard[:, 0:1], axis=0)
    total = jnp.zeros_like(top)
    both = jnp.zeros_like(top)
    for j in range(4):
        w = jnp.exp(heard[j, 0:1] - top)
        total = total + w * heard[j, 1:2]
        both = both + w * heard[j, 2:3]
    stats[...] = jnp.where(row == 0, top + jnp.log(total), both / total)
    scaled = o[...] * (jnp.exp(m[...] - top) / total)
    upright = jnp.concatenate([scaled, jnp.zeros_like(scaled)], axis=0)
    out[...] = jnp.transpose(upright).astype(BF16).reshape(out.shape)

    by_o = ToOwners(out, outs, o_s, o_r)
    by_o.start()
    dq[...] = jnp.zeros(dq.shape, F32)

    def plane_of(side, j):
        offset = jnp.where(side == 0, j - nz // 2, nz // 2 - 1 - j)
        return lax.rem(z + nz + offset, nz)

    def grads(side, j):
        at = plane_of(side, j)
        block = kv_all[at]
        low = lanes_below(block.shape, HD)
        none = jnp.zeros_like(block)
        scores = contract(jnp.where(low, block, none), qa[...], 1, 1)
        probs = jnp.exp(scores - stats[0:1])
        d_probs = contract(jnp.where(low, none, block), qa[...], 1, 1)
        d_scores = (probs * (d_probs - stats[1:2])).astype(BF16)
        for_v = contract(probs.astype(BF16), qa[...], 1, 0)
        for_k = contract(d_scores, qa[...], 1, 0)
        dq[...] += contract(block, d_scores, 0, 0)[:HD]
        mine[side, j] = jnp.where(lanes_below(for_k.shape, HD), for_k, for_v)

    def both_grads(low, high):
        def one(i, carry):
            side = lax.rem(i, 2)
            grads(side, low + i // 2 - side)
            return carry

        lax.fori_loop(0, 2 * (high - low + 1), one, 0)

    main = StrideSum(nz, lambda side, j, at: mine[side, j, at], ring_out, ring_in, g_s, g_r, PIECES)

    def own_weight(side, j, at):
        to = plane_of(side, j)
        return swapped[0, to, at].astype(F32) + swapped[1, to, at].astype(F32)

    weight = StrideSum(nz, own_weight, w_ring_out, w_ring_in, h_s, h_r, 1)

    def two(ring, j):
        ring.step(0, j)
        ring.step(1, j - 1)

    grads(jnp.int32(0), jnp.int32(0))
    main.step(0, 0)
    both_grads(1, 1)
    two(main, 1)
    by_o.arrive()
    attended = jnp.sum(outs[...].astype(F32), axis=0).astype(BF16)
    for a in range(2):
        spread = contract(pick[96:], attended[96 * a : 96 * a + 96], 0, 0).astype(BF16)
        product = contract(spread, t_all[...].reshape(256, 2048), 0, 0)[:HD].astype(BF16)
        for i in range(nz):
            o_part[a, i] = product[:, 128 * i : 128 * i + 128]
    swap = Exchange(("c",), o_part, swapped, sw_s, sw_r, lambda at, i: i)
    swap.start()
    both_grads(2, 3)
    two(main, 3)
    two(main, 2)
    swap.arrive()
    weight.step(0, 0)
    for j in range(1, nz // 2, 2):
        two(weight, j)
    both_grads(4, 5)
    two(main, 5)
    two(main, 4)
    both_grads(6, 7)
    two(main, 7)
    two(weight, 2)
    grads(jnp.int32(1), jnp.int32(7))
    upright = jnp.concatenate([dq[...], jnp.zeros_like(dq[...])], axis=0) * HD**-0.5
    dq_block[...] = jnp.transpose(upright).astype(BF16).reshape(4, 192, 128)
    by_dq = ToOwners(dq_block, dqs, dq_s, dq_r)
    by_dq.start()
    two(main, 6)
    two(weight, 4)
    by_dq.arrive()
    query_grad = jnp.sum(dqs[...].astype(F32), axis=0).astype(BF16)
    d_target = jnp.zeros((128, 2048), F32)
    for a in range(2):
        spread = contract(pick8[...], query_grad[96 * a : 96 * a + 96], 0, 0).astype(BF16)
        d_target = d_target + jnp.dot(spread, pair_all[a], preferred_element_type=F32)
    d_parts[...] = d_target.astype(BF16).reshape(16, 8, 2048)
    by_t = Exchange(("x", "y"), d_parts, t_in, t_s, t_r, lambda at, i: i)
    by_t.start()
    piece = 256 // PIECES
    for p in range(PIECES):
        kv_grad[pl.ds(p * piece, piece)] = main.total(p).astype(BF16)
    by_kv = Exchange(("c",), kv_grad, grads2, kv_s, kv_r)
    by_kv.start()
    two(weight, 6)
    by_kv.arrive()
    g0, g1 = grads2[0].astype(F32), grads2[1].astype(F32)
    k2 = jnp.where(wide_low, g0, swap_halves(g1)).astype(BF16)
    v2 = jnp.where(wide_low, swap_halves(g0), g1).astype(BF16)
    d_rows = contract(k2, w_all[:, :, 0].reshape(1024, 128), 1, 1)
    d_rows = d_rows + contract(v2, w_all[:, :, 1].reshape(1024, 128), 1, 1)
    parts[...] = d_rows.astype(BF16).reshape(8, 32, 1024)
    by_s = Exchange(("y", "c"), parts, s_in, s_s, s_r, lambda at, i: i)
    by_s.start()
    mine_sum[...] = weight.total(0).astype(BF16)
    back = FarGather(nz, mine_sum, all_sums, back_s, back_r)
    back.start()
    by_t.arrive()
    upstream = jnp.sum(t_in[...].astype(F32), axis=0)[:6]
    t_out[...] = cot[...].astype(F32) + norm_back(target_rows[...], t_gain[...], upstream)
    back.relay()
    by_s.arrive()
    got = []
    for core in range(2):
        total = s_in[core].astype(F32)
        for i in range(1, 4):
            total = total + s_in[2 * i + core].astype(F32)
        got.append(total)
    for j in range(8):
        chip = (2 * j % 4) * 4 + j // 2
        a, b = (g[:, 128 * j : 128 * j + 128] for g in got)
        upstream_s[:, 128 * chip : 128 * chip + 128] = jnp.where(low, a, swap_halves(b))
        upstream_s[:, 128 * chip + 512 : 128 * chip + 640] = jnp.where(low, swap_halves(a), b)
    s_out[...] = norm_back(source_rows[...], s_gain[...], upstream_s[...])
    back.arrive()
    for i in range(nz):
        w_out[:, 128 * i : 128 * i + 128] = all_sums[i].astype(F32)
    for by in (by_rows, by_wy, by_wx, by_ya, by_xb, by_xa, by_yb, by_pair, by_part, by_q, by_z, by_stats):
        by.drain()
    for by in (by_o, by_dq, swap, back, by_kv, by_s, by_t, main, weight):
        by.drain()


def whole(args, nz):
    t = 768
    half = nz // 2

    def bf16(*shape):
        return pltpu.VMEM(shape, BF16)

    def f32(*shape):
        return pltpu.VMEM(shape, F32)

    return pl.pallas_call(
        functools.partial(kernel, nz),
        out_shape=(
            jax.ShapeDtypeStruct((32, 2048), F32),
            jax.ShapeDtypeStruct((6, 2048), F32),
            jax.ShapeDtypeStruct((64, 2048), F32),
        ),
        in_specs=[VMEM] * len(args),
        out_specs=(VMEM,) * 3,
        scratch_shapes=[
            bf16(128, 2048), bf16(nz, 256, 128), f32(8, t), bf16(4, 192, 128), bf16(t, 128),
            bf16(4, 4, 16, 2048), bf16(2, 128, 2048), bf16(4, 4, 2, 64, 128),
            bf16(2, 32, 1024), bf16(4, 2, 32, 1024), f32(2, 256, 128), f32(2, 256, 128),
            bf16(192, 128), bf16(4, 192, 128), f32(1, t), f32(1, t), f32(HD, t), f32(8, t), f32(4, 8, t),
            f32(HD, t), f32(2, half, 256, 128), bf16(2, half, 256, 128), bf16(2, half, 256, 128),
            bf16(2, half, HD, 128), bf16(2, half, HD, 128),
            bf16(4, 192, 128), bf16(4, 192, 128), bf16(4, 192, 128),
            bf16(2, nz, HD, 128), bf16(2, nz, HD, 128), bf16(HD, 128), bf16(nz, HD, 128),
            f32(32, 2048), bf16(256, 128), bf16(2, 256, 128), bf16(8, 32, 1024), bf16(16, 8, 2048),
            bf16(8, 32, 1024), bf16(16, 8, 2048),
            sems(5, 2), sems(5, 2), dma(1), dma(1), dma(1), sems(3, 4),
            dma(1), sems(3, 2), dma(1), sems(3, 2), dma(1), sems(3, 4), dma(1), sems(3, 4), dma(1), dma(1),
            dma(1), dma(1), dma(4), dma(4), dma(1), sems(2, half, PIECES), dma(1), dma(1),
            dma(4), dma(4), dma(4), dma(4), dma(1), dma(1),
            dma(2), sems(2, half, PIECES), dma(2), sems(2, half, 1),
            dma(1), dma(4), dma(1), dma(1), dma(1), dma(1), dma(1), dma(1),
        ],
        compiler_params=params(0),
    )(*args)


def picks():
    r = np.arange(96)
    at = 16 * (r // 6) + r % 6
    pick = np.concatenate([at, at + 8])[:, None] == np.arange(256)[None]
    pick8 = (8 * (r // 6) + r % 6)[:, None] == np.arange(128)[None]
    return jnp.asarray(pick.astype(BF16)), jnp.asarray(pick8.astype(BF16))


def body(nz, target_rows, source_rows, t_gain, s_gain, wq, wk, wv, wo, cot):
    args = (target_rows, source_rows, t_gain[None], s_gain[None], wq, wk, wv, wo, cot, *picks())
    source_grad, target_grad, o_grad = whole(args, nz)
    return target_grad, source_grad, o_grad


def solution(mesh):
    nz = mesh.shape["sp"]
    SIZES["z"] = nz
    fine = Mesh(mesh.devices.reshape(nz, 4, 4, 2), ("z", "y", "x", "c"))
    every, plane = ("z", "y", "x", "c"), ("y", "x", "c")
    return jax.shard_map(
        functools.partial(body, nz),
        mesh=fine,
        in_specs=(
            P(every, None), P(every, None), P(), P(),
            P(None, plane), P(plane, None), P(plane, None), P(plane, None), P(every, None),
        ),
        out_specs=(P(every, None), P(every, None), P(plane, None)),
        check_vma=False,
    )
```

```python
import functools

import jax
import jax.numpy as jnp
import numpy as np
from jax import lax
from jax.experimental import pallas as pl
from jax.experimental.pallas import tpu as pltpu
from jax.sharding import Mesh
from jax.sharding import PartitionSpec as P

MESH = pl.DeviceIdType.MESH
HD = 64
EPSILON = 1e-06
F32, BF16 = jnp.float32, jnp.bfloat16
VMEM = pl.BlockSpec(memory_space=pltpu.VMEM)
SIZES = {"y": 4, "x": 4, "c": 2}
PIECES = 2
REACH = 4


def dma(n):
    return pltpu.SemaphoreType.DMA((n,))


def params(cid):
    return pltpu.CompilerParams(
        collective_id=cid, has_side_effects=True, vmem_limit_bytes=62 * 1024 * 1024
    )


def group_size(axes):
    n = 1
    for a in axes:
        n *= SIZES[a]
    return n


def group_index(axes):
    i = 0
    for a in axes:
        i = i * SIZES[a] + lax.axis_index(a)
    return i


def coords_of(index, axes):
    out = {}
    for a in reversed(axes):
        out[a] = lax.rem(index, SIZES[a])
        index = index // SIZES[a]
    return out


def greet(axes):
    n, me = group_size(axes), group_index(axes)
    sem = pltpu.get_barrier_semaphore()

    def one(k, carry):
        pl.semaphore_signal(
            sem, inc=1, device_id=coords_of(lax.rem(me + k, n), axes), device_id_type=MESH
        )
        return carry

    lax.fori_loop(1, n, one, 0)
    return n - 1


def greeted(count):
    pl.semaphore_wait(pltpu.get_barrier_semaphore(), count)


class Exchange:
    def __init__(self, axes, src, dst, send, recv, pick=None):
        self.axes, self.src, self.dst, self.send, self.recv = axes, src, dst, send, recv
        self.n, self.me = group_size(axes), group_index(axes)
        self.pick = pick

    def block(self, index):
        if self.pick is None:
            return self.src
        return self.src.at[self.pick(coords_of(index, self.axes), index)]

    def copy(self, k, slot):
        to = lax.rem(self.me + k, self.n)
        return pltpu.make_async_remote_copy(
            src_ref=self.block(to),
            dst_ref=self.dst.at[slot],
            send_sem=self.send.at[0],
            recv_sem=self.recv.at[0],
            device_id=coords_of(to, self.axes),
            device_id_type=MESH,
        )

    def start(self):
        def one(k, carry):
            self.copy(k, self.me).start()
            return carry

        lax.fori_loop(1, self.n, one, 0)
        self.dst[self.me] = self.block(self.me)[...]

    def others(self):
        return bulk(self.dst.at[pl.ds(0, self.n - 1)], self.send, self.recv)

    def arrive(self):
        self.others().wait_recv()

    def drain(self):
        self.others().wait_send()


def bulk(ref, send, recv):
    return pltpu.make_async_remote_copy(
        src_ref=ref,
        dst_ref=ref,
        send_sem=send.at[0],
        recv_sem=recv.at[0],
        device_id={"c": 1 - lax.axis_index("c")},
        device_id_type=MESH,
    )


class ToReaders:
    def __init__(self, src, dst, send, recv):
        self.src, self.dst, self.send, self.recv = src, dst, send, recv
        self.y, self.x, self.c = (lax.axis_index(a) for a in "yxc")
        self.mine = self.x // 2 == self.c

    def copy(self, k, slot):
        return pltpu.make_async_remote_copy(
            src_ref=self.src,
            dst_ref=self.dst.at[slot],
            send_sem=self.send.at[k],
            recv_sem=self.recv.at[slot],
            device_id={"x": lax.rem(self.x + k, 4), "c": self.x // 2},
            device_id_type=MESH,
        )

    def slot(self):
        return lax.rem(self.x, 2) * 2 + self.c

    def start(self):
        for k in range(1, 4):
            self.copy(k, self.slot()).start()

        @pl.when(jnp.logical_not(self.mine))
        def _():
            self.copy(0, self.slot()).start()

        @pl.when(self.mine)
        def _():
            self.dst[self.slot()] = self.src[...]

    def arrive(self):
        for s in range(4):
            own = jnp.logical_and(2 * self.c + s // 2 == self.x, self.c == s % 2)

            @pl.when(jnp.logical_not(own))
            def _():
                self.copy(1, s).wait_recv()

    def drain(self):
        for k in range(1, 4):
            self.copy(k, self.slot()).wait_send()

        @pl.when(jnp.logical_not(self.mine))
        def _():
            self.copy(0, self.slot()).wait_send()


class ToOwners:
    def __init__(self, src, dst, send, recv):
        self.src, self.dst, self.send, self.recv = src, dst, send, recv
        self.y, self.x, self.c = (lax.axis_index(a) for a in "yxc")

    def copy(self, s, slot):
        return pltpu.make_async_remote_copy(
            src_ref=self.src.at[s],
            dst_ref=self.dst.at[slot],
            send_sem=self.send.at[s],
            recv_sem=self.recv.at[slot],
            device_id={"x": 2 * self.c + s // 2, "c": jnp.int32(s % 2)},
            device_id_type=MESH,
        )

    def own(self, s):
        return jnp.logical_and(2 * self.c + s // 2 == self.x, self.c == s % 2)

    def start(self):
        for s in range(4):
            @pl.when(jnp.logical_not(self.own(s)))
            def _():
                self.copy(s, self.x).start()

            @pl.when(self.own(s))
            def _():
                self.dst[self.x] = self.src[s]

    def arrive(self):
        for j in range(4):
            own = jnp.logical_and(self.x == j, self.x // 2 == self.c)

            @pl.when(jnp.logical_not(own))
            def _():
                self.copy(0, j).wait_recv()

    def drain(self):
        for s in range(4):
            @pl.when(jnp.logical_not(self.own(s)))
            def _():
                self.copy(s, self.x).wait_send()


def lanes_below(shape, bound):
    return lax.broadcasted_iota(jnp.int32, shape, 1) < bound


def contract(a, b, da, db):
    return lax.dot_general(a, b, (((da,), (db,)), ((), ())), preferred_element_type=F32)


def ring_greet(nz):
    z = lax.axis_index("z")
    sem = pltpu.get_barrier_semaphore()
    right, left = lax.rem(z + 1, nz), lax.rem(z + nz - 1, nz)
    for to in (left, right):
        pl.semaphore_signal(sem, inc=1, device_id={"z": to}, device_id_type=MESH)
    return 2


class RingGather:
    def __init__(self, axis, piece, count, three, send, recv):
        self.axis, self.piece, self.count, self.send, self.recv = axis, piece, count, send, recv
        self.three = three
        self.me = lax.axis_index(axis)

    def at(self, offset):
        return lax.rem(self.me + offset + 4, 4)

    def copy(self, slot, p, sign, kind):
        ref = self.piece(slot, p)
        return pltpu.make_async_remote_copy(
            src_ref=ref,
            dst_ref=ref,
            send_sem=self.send.at[0],
            recv_sem=self.recv.at[kind, p],
            device_id={self.axis: self.at(sign)},
            device_id_type=MESH,
        )

    def start(self, p):
        self.copy(self.me, p, 1, 0).start()
        self.copy(self.me, p, -1, 1).start()

    def relay(self, p):
        self.copy(self.at(-1), p, 1, 0).wait_recv()
        self.copy(self.at(1), p, -1, 1).wait_recv()
        if p < self.count // 2:
            self.copy(self.at(-1), p, 1, 2).start()
        else:
            self.copy(self.at(1), p, -1, 2).start()

    def arrive(self, p):
        self.copy(self.at(2), p, 1, 2).wait_recv()

    def drain(self):
        bulk(self.three, self.send, self.send).wait_send()


class RowGather:
    def __init__(self, halves, out, send, recv):
        self.halves, self.out, self.send, self.recv = halves, out, send, recv
        self.y, self.c = lax.axis_index("y"), lax.axis_index("c")

    def at(self, offset):
        return lax.rem(self.y + offset + 4, 4)

    def first(self, sign, core, slot_y, slot_c):
        kind = 0 if sign > 0 else 1
        return pltpu.make_async_remote_copy(
            src_ref=self.halves.at[core],
            dst_ref=self.out.at[slot_y, slot_c],
            send_sem=self.send.at[kind, core],
            recv_sem=self.recv.at[kind, slot_c],
            device_id={"y": self.at(sign), "c": jnp.int32(core)},
            device_id_type=MESH,
        )

    def partner(self, slot_c):
        return pltpu.make_async_remote_copy(
            src_ref=self.halves.at[1 - self.c],
            dst_ref=self.out.at[self.y, slot_c],
            send_sem=self.send.at[4, 0],
            recv_sem=self.recv.at[4, 0],
            device_id={"c": 1 - self.c},
            device_id_type=MESH,
        )

    def second(self, sign, slot_y, slot_c):
        kind = 2 if sign > 0 else 3
        ref = self.out.at[slot_y, slot_c, pl.ds(0 if sign > 0 else 16, 16)]
        return pltpu.make_async_remote_copy(
            src_ref=ref,
            dst_ref=ref,
            send_sem=self.send.at[kind, slot_c],
            recv_sem=self.recv.at[kind, slot_c],
            device_id={"y": self.at(sign)},
            device_id_type=MESH,
        )

    def start(self):
        for core in range(2):
            self.first(1, core, self.y, self.c).start()
            self.first(-1, core, self.y, self.c).start()
        self.partner(self.c).start()
        self.out[self.y, self.c] = self.halves[self.c]

    def relay(self):
        for core in range(2):
            self.first(1, 0, self.at(-1), core).wait_recv()
            self.second(1, self.at(-1), core).start()
            self.first(-1, 0, self.at(1), core).wait_recv()
            self.second(-1, self.at(1), core).start()

    def arrive(self):
        self.partner(1 - self.c).wait_recv()
        for core in range(2):
            self.second(1, self.at(2), core).wait_recv()
            self.second(-1, self.at(2), core).wait_recv()

    def drain(self):
        self.partner(self.c).wait_send()
        for core in range(2):
            self.first(1, core, self.y, self.c).wait_send()
            self.first(-1, core, self.y, self.c).wait_send()
            self.second(1, self.y, core).wait_send()
            self.second(-1, self.y, core).wait_send()


class WeightColumn:
    def __init__(self, wk, wv, out, send, recv):
        self.parts, self.out, self.send, self.recv = (wk, wv), out, send, recv
        self.y, self.x = lax.axis_index("y"), lax.axis_index("x")

    def lanes(self, y):
        return pl.ds(pl.multiple_of(y * 128, 128), 128)

    def copy(self, k, i, slot_y):
        to = lax.rem(self.y + k, 4)
        return pltpu.make_async_remote_copy(
            src_ref=self.parts[i].at[:, self.lanes(to)],
            dst_ref=self.out.at[self.x, slot_y, i],
            send_sem=self.send.at[0],
            recv_sem=self.recv.at[0],
            device_id={"y": to},
            device_id_type=MESH,
        )

    def start(self):
        for k in (2, 1, 3):
            for i in range(2):
                self.copy(k, i, self.y).start()
        for i in range(2):
            self.out[self.x, self.y, i] = self.parts[i][:, self.lanes(self.y)]

    def others(self):
        return bulk(self.out.at[self.x, pl.ds(0, 3)], self.send, self.recv)

    def arrive(self):
        self.others().wait_recv()

    def drain(self):
        self.others().wait_send()


def unit_rows(matrix, gain):
    wide = matrix.astype(F32)
    factor = lax.rsqrt(jnp.mean(wide * wide, axis=-1, keepdims=True) + EPSILON)
    return wide * factor * gain


def swap_halves(a):
    return pltpu.roll(a, HD, 1)


class StrideGather:
    def __init__(self, nz, blocks, send, recv):
        self.nz, self.blocks, self.send, self.recv = nz, blocks, send, recv
        self.z = lax.axis_index("z")
        self.rows = blocks.shape[1] // PIECES
        self.far = {1: nz // 2, -1: nz - 1 - nz // 2}

    def at(self, offset):
        return lax.rem(self.z + offset + self.nz, self.nz)

    def copy(self, sign, distance, d, p):
        ref = self.blocks.at[self.at(-sign * distance), pl.ds(p * self.rows, self.rows)]
        return pltpu.make_async_remote_copy(
            src_ref=ref,
            dst_ref=ref,
            send_sem=self.send.at[0],
            recv_sem=self.recv.at[0 if sign > 0 else 1, distance + d - 1, p],
            device_id={"z": self.at(sign * d)},
            device_id_type=MESH,
        )

    def arrived(self, sign, distance, p):
        ref = self.blocks.at[self.at(-sign * distance), pl.ds(p * self.rows, self.rows)]
        return pltpu.make_async_remote_copy(
            src_ref=ref,
            dst_ref=ref,
            send_sem=self.send.at[0],
            recv_sem=self.recv.at[0 if sign > 0 else 1, distance - 1, p],
            device_id={"z": self.at(sign)},
            device_id_type=MESH,
        )

    def start(self):
        for d in (2, 1):
            for p in range(PIECES):
                for sign in (1, -1):
                    self.copy(sign, 0, d, p).start()

    def relay(self, distance):
        for p in range(PIECES):
            for sign in (1, -1):
                if distance <= self.far[sign]:
                    self.arrived(sign, distance, p).wait_recv()
                if distance + 2 <= self.far[sign]:
                    self.copy(sign, distance, 2, p).start()
        for p in range(PIECES):
            for sign in (1, -1):
                if distance + 1 <= self.far[sign]:
                    self.copy(sign, distance, 1, p).start()

    def arrive(self, distance):
        for sign in (1, -1):
            if distance <= self.far[sign]:
                for p in range(PIECES):
                    self.arrived(sign, distance, p).wait_recv()

    def drain(self):
        bulk(self.blocks.at[pl.ds(0, self.nz - 1)], self.send, self.send).wait_send()


class StrideSum:
    def __init__(self, nz, term, out, arrived, send, recv, pieces):
        self.nz, self.term, self.out, self.arrived = nz, term, out, arrived
        self.send, self.recv, self.pieces = send, recv, pieces
        self.rows = out.shape[2] // pieces
        self.z = lax.axis_index("z")

    def chained(self, side, j):
        return (j + side) % 2 == 0

    def hop(self, side, j, p):
        at = pl.ds(p * self.rows, self.rows)
        d = (2 if self.chained(side, j) else 1) * (1 if side else -1)
        return pltpu.make_async_remote_copy(
            src_ref=self.out.at[side, j, at],
            dst_ref=self.arrived.at[side, j, at],
            send_sem=self.send.at[side],
            recv_sem=self.recv.at[side, j, p],
            device_id={"z": lax.rem(self.z + d + self.nz, self.nz)},
            device_id_type=MESH,
        )

    def joined(self, side, j, p, value):
        at = pl.ds(p * self.rows, self.rows)
        for i in (j - 1, j - 2):
            if i >= 0:
                self.hop(side, i, p).wait_recv()
                value = value + self.arrived[side, i, at].astype(F32)
        return value

    def step(self, side, j):
        for p in range(self.pieces):
            at = pl.ds(p * self.rows, self.rows)
            value = self.term(side, j, at)
            if self.chained(side, j):
                value = self.joined(side, j, p, value)
            self.out[side, j, at] = value.astype(BF16)
            self.hop(side, j, p).start()

    def total(self, p):
        half = self.nz // 2
        at = pl.ds(p * self.rows, self.rows)
        value = self.joined(1, half - 1, p, self.term(1, half - 1, at))
        return self.joined(0, half, p, value)

    def drain(self):
        half = self.nz // 2
        for side in range(2):
            sem = self.send.at[pl.ds(side, 1)]
            bulk(self.out.at[side, pl.ds(0, half - side)], sem, sem).wait_send()


class FarGather:
    def __init__(self, nz, src, dst, send, recv):
        self.nz, self.src, self.dst, self.send, self.recv = nz, src, dst, send, recv
        self.z = lax.axis_index("z")
        self.far = {1: nz // 2 - REACH, -1: nz - 1 - nz // 2 - REACH}

    def at(self, offset):
        return lax.rem(self.z + offset + self.nz, self.nz)

    def copy(self, slot, sign, d, relay):
        kind = 3 if relay else 2 if d < REACH else 0 if sign > 0 else 1
        return pltpu.make_async_remote_copy(
            src_ref=self.dst.at[slot] if relay else self.src,
            dst_ref=self.dst.at[slot],
            send_sem=self.send.at[0],
            recv_sem=self.recv.at[kind],
            device_id={"z": self.at(sign * d)},
            device_id_type=MESH,
        )

    def several(self, count, kind):
        return bulk(self.dst.at[pl.ds(0, count)], self.send, self.recv.at[pl.ds(kind, 1)])

    def start(self):
        for d in range(REACH, 0, -1):
            for sign in (1, -1):
                self.copy(self.z, sign, d, False).start()
        self.dst[self.z] = self.src[...]

    def relay(self):
        for sign in (1, -1):
            slot = self.at(-sign * REACH)
            self.copy(slot, sign, REACH, False).wait_recv()
            for d in range(self.far[sign], 0, -1):
                self.copy(slot, sign, d, True).start()

    def arrive(self):
        self.several(2 * REACH - 2, 2).wait_recv()
        self.several(self.nz - 1 - 2 * REACH, 3).wait_recv()

    def drain(self):
        self.several(self.nz - 1, 0).wait_send()


def reach_greet(nz):
    z = lax.axis_index("z")
    for d in range(1, REACH + 1):
        for sign in (1, -1):
            pl.semaphore_signal(
                pltpu.get_barrier_semaphore(),
                inc=1,
                device_id={"z": lax.rem(z + sign * d + nz, nz)},
                device_id_type=MESH,
            )
    return 2 * REACH


def sems(*shape):
    return pltpu.SemaphoreType.DMA(shape)


def norm_back(matrix, gain, upstream):
    wide = matrix.astype(F32)
    factor = lax.rsqrt(jnp.mean(wide * wide, axis=-1, keepdims=True) + EPSILON)
    weighted = upstream * gain
    inner = jnp.mean(weighted * wide, axis=-1, keepdims=True)
    return factor * weighted - wide * factor**3 * inner


def kernel(
    nz, target_rows_h, source_rows_h, t_gain_h, s_gain_h, wq_h, wk_h, wv_h, wo_h, cot_h, pick_h, pick8_h,
    s_out, t_out, all_sums,
    target_rows, source_rows, t_gain, s_gain, wk, wv, cot, pick, pick8, loads,
    pair, kv_all, stats, out, qa, t_all, pair_all, w_all,
    halves, rows_all, part, part_all, block, blocks, m, l, o, said, heard,
    dq, mine, ring_out, ring_in, w_ring_out, w_ring_in, outs, dq_block, dqs, o_part, swapped,
    mine_sum, kv_grad, grads2, parts, d_parts, s_in, t_in,
    row_s, row_r, wy_s, wy_r, wx_s, wx_r, ya_s, ya_r, xb_s, xb_r, xa_s, xa_r, yb_s, yb_r, pair_s, pair_r,
    part_s, part_r, q_s, q_r, z_s, z_r, ss, sr,
    o_s, o_r, dq_s, dq_r, sw_s, sw_r, g_s, g_r, h_s, h_r, back_s, back_r,
    kv_s, kv_r, s_s, s_r, t_s, t_r,
):
    z, y, x, c = (lax.axis_index(a) for a in "zyxc")
    met = greet(("y", "x", "c")) + reach_greet(nz)

    staged = (
        (source_rows_h, source_rows), (s_gain_h, s_gain), (wk_h, wk), (wv_h, wv),
        (target_rows_h, target_rows), (t_gain_h, t_gain), (cot_h, cot),
        (wq_h, pair.at[pl.ds(0, HD)]), (wo_h, pair.at[pl.ds(HD, HD)]), (pick_h, pick), (pick8_h, pick8),
    )
    copies = [pltpu.make_async_copy(a, b, loads.at[i]) for i, (a, b) in enumerate(staged)]
    for copy in copies:
        copy.start()
    for copy in copies[:2]:
        copy.wait()
    normed = unit_rows(source_rows[...], s_gain[...])
    low = lanes_below((32, 128), HD)
    for j in range(8):
        chip = (2 * j % 4) * 4 + j // 2
        first, second = (normed[:, 128 * i : 128 * i + 128] for i in (chip, chip + 4))
        halves[0, :, 128 * j : 128 * j + 128] = jnp.where(low, first, swap_halves(second)).astype(BF16)
        halves[1, :, 128 * j : 128 * j + 128] = jnp.where(low, swap_halves(first), second).astype(BF16)
    for copy in copies[2:]:
        copy.wait()
    greeted(met)

    by_rows = RowGather(halves, rows_all, row_s, row_r)
    by_wy = WeightColumn(wk, wv, w_all, wy_s, wy_r)
    by_wx = RingGather("x", lambda slot, p: w_all.at[slot, p], 4, w_all.at[pl.ds(0, 3)], wx_s, wx_r)
    three, first, second = pl.ds(0, 3), pl.ds(0, 1024), pl.ds(1024, 1024)
    by_ya = RingGather(
        "y", lambda slot, p: t_all.at[x, slot, :, pl.ds(512 * p, 512)], 2,
        t_all.at[x, three, :, first], ya_s, ya_r,
    )
    by_xb = RingGather(
        "x", lambda slot, p: t_all.at[slot, y, :, pl.ds(1024 + 512 * p, 512)], 2,
        t_all.at[three, y, :, second], xb_s, xb_r,
    )
    by_xa = RingGather(
        "x", lambda slot, p: t_all.at[slot, p, :, first], 4, t_all.at[three, :, :, first], xa_s, xa_r
    )
    by_yb = RingGather(
        "y", lambda slot, p: t_all.at[p, slot, :, second], 4, t_all.at[:, three, :, second], yb_s, yb_r
    )
    by_pair = Exchange(("c",), pair, pair_all, pair_s, pair_r)
    by_wy.start()
    by_rows.start()
    zero = jnp.zeros((2, target_rows.shape[1]), F32)
    t_all[x, y] = jnp.concatenate(
        [unit_rows(target_rows[...], t_gain[...]), zero, cot[...].astype(F32), zero], axis=0
    ).astype(BF16)
    for p in range(2):
        by_xb.start(p)
        by_ya.start(p)
    by_pair.start()

    by_wy.arrive()
    for p in range(4):
        by_wx.start(p)
    by_rows.relay()
    for p in range(4):
        by_wx.relay(p)
    for p in range(2):
        by_xb.relay(p)
        by_ya.relay(p)
    for p in range(2):
        by_xb.arrive(p)
        by_ya.arrive(p)
    for p in range(4):
        by_xa.start(p)
        by_yb.start(p)
    by_rows.arrive()
    for p in range(4):
        by_wx.arrive(p)

    rows = rows_all[...].reshape(256, 1024)
    k2 = jnp.dot(rows, w_all[:, :, 0].reshape(1024, 128), preferred_element_type=F32)
    v2 = jnp.dot(rows, w_all[:, :, 1].reshape(1024, 128), preferred_element_type=F32)
    wide_low = lanes_below((256, 128), HD)
    part[0] = jnp.where(wide_low, k2, swap_halves(v2))
    part[1] = jnp.where(wide_low, swap_halves(k2), v2)
    by_part = Exchange(("c",), part, part_all, part_s, part_r, lambda at, i: i)
    by_part.start()
    by_part.arrive()
    kv_all[z] = (part_all[0] + part_all[1]).astype(BF16)

    by_z = StrideGather(nz, kv_all, z_s, z_r)
    by_z.start()
    for p in range(4):
        by_xa.relay(p)
        by_yb.relay(p)
    by_z.relay(2)
    by_pair.arrive()
    for p in range(4):
        by_xa.arrive(p)
        by_yb.arrive(p)
    everything = t_all[...].reshape(256, 2048)
    wide = lax.broadcasted_iota(jnp.int32, (256, 256), 1)
    scale = jnp.where(lax.rem(wide, 128) < HD, HD**-0.5, 1.0)
    projected = contract(everything, pair_all[...].reshape(256, 2048), 1, 1) * scale
    chosen = jnp.dot(pick[...], projected.astype(BF16), preferred_element_type=F32)
    narrow = lanes_below((96, 128), HD)
    for a in range(2):
        at = slice(128 * a, 128 * a + 128)
        block[96 * a : 96 * a + 96] = jnp.where(narrow, chosen[:96, at], chosen[96:, at]).astype(BF16)
    by_q = ToReaders(block, blocks, q_s, q_r)
    by_q.start()
    by_z.relay(4)
    m[...] = jnp.full(m.shape, -1e30, F32)
    l[...] = jnp.zeros(l.shape, F32)
    o[...] = jnp.zeros(o.shape, F32)
    by_q.arrive()
    qa[...] = blocks[...].reshape(qa.shape)

    def blocks_of(planes):
        return jnp.concatenate([kv_all[at] for at in planes], axis=0)

    def attend(*planes):
        block = blocks_of(planes)
        keys = jnp.where(lanes_below(block.shape, HD), block, jnp.zeros_like(block))
        scores = contract(keys, qa[...], 1, 1)
        top = jnp.maximum(m[...], jnp.max(scores, axis=0, keepdims=True))
        weights = jnp.exp(scores - top)
        old = jnp.exp(m[...] - top)
        m[...] = top
        l[...] = l[...] * old + jnp.sum(weights, axis=0, keepdims=True)
        o[...] = o[...] * old + contract(block, weights.astype(BF16), 0, 0)[HD:]

    def attend_from(low, high):
        def one(d, carry):
            attend(lax.rem(z + d, nz), lax.rem(z + nz - d, nz))
            return carry

        lax.fori_loop(low, high + 1, one, 0)

    attend(z)
    by_z.relay(6)
    by_z.arrive(1)
    by_z.arrive(3)
    attend_from(1, 4)
    by_z.arrive(5)
    attend_from(5, 6)
    by_z.arrive(7)
    by_z.arrive(8)
    attend_from(7, 7)
    attend(lax.rem(z + nz // 2, nz))
    upright = jnp.transpose(qa[...].astype(F32))
    delta = jnp.sum(upright[HD:] * o[...], axis=0, keepdims=True)
    row = lax.broadcasted_iota(jnp.int32, (8, qa.shape[0]), 0)
    said[...] = jnp.where(row == 0, m[...], jnp.where(row == 1, l[...], delta))
    by_stats = Exchange(("x",), said, heard, ss, sr)
    by_stats.start()
    by_stats.arrive()
    top = jnp.max(heard[:, 0:1], axis=0)
    total = jnp.zeros_like(top)
    both = jnp.zeros_like(top)
    for j in range(4):
        w = jnp.exp(heard[j, 0:1] - top)
        total = total + w * heard[j, 1:2]
        both = both + w * heard[j, 2:3]
    stats[...] = jnp.where(row == 0, top + jnp.log(total), both / total)
    scaled = o[...] * (jnp.exp(m[...] - top) / total)
    upright = jnp.concatenate([scaled, jnp.zeros_like(scaled)], axis=0)
    out[...] = jnp.transpose(upright).astype(BF16).reshape(out.shape)

    by_o = ToOwners(out, outs, o_s, o_r)
    by_o.start()
    dq[...] = jnp.zeros(dq.shape, F32)

    def plane_of(side, j):
        offset = nz // 2 - 1 - j if side else j - nz // 2
        return lax.rem(z + nz + offset, nz)

    def grads(*terms):
        block = blocks_of([plane_of(side, j) for side, j in terms])
        low = lanes_below(block.shape, HD)
        none = jnp.zeros_like(block)
        scores = contract(jnp.where(low, block, none), qa[...], 1, 1)
        probs = jnp.exp(scores - stats[0:1])
        d_probs = contract(jnp.where(low, none, block), qa[...], 1, 1)
        d_scores = (probs * (d_probs - stats[1:2])).astype(BF16)
        for_v = contract(probs.astype(BF16), qa[...], 1, 0)
        for_k = contract(d_scores, qa[...], 1, 0)
        dq[...] += contract(block, d_scores, 0, 0)[:HD]
        both = jnp.where(low, for_k, for_v)
        for i, (side, j) in enumerate(terms):
            mine[side, j] = both[256 * i : 256 * i + 256]

    def both_grads(low, high):
        def one(j, carry):
            grads((0, j), (1, j - 1))
            return carry

        lax.fori_loop(low, high + 1, one, 0)

    main = StrideSum(nz, lambda side, j, at: mine[side, j, at], ring_out, ring_in, g_s, g_r, PIECES)

    def own_weight(side, j, at):
        to = plane_of(side, j)
        return swapped[0, to, at].astype(F32) + swapped[1, to, at].astype(F32)

    weight = StrideSum(nz, own_weight, w_ring_out, w_ring_in, h_s, h_r, 1)

    def two(ring, j):
        ring.step(0, j)
        ring.step(1, j - 1)

    grads((0, 0))
    main.step(0, 0)
    both_grads(1, 1)
    two(main, 1)
    both_grads(2, 2)
    two(main, 2)
    both_grads(3, 3)
    two(main, 3)
    by_o.arrive()
    attended = jnp.sum(outs[...].astype(F32), axis=0).astype(BF16)
    for a in range(2):
        spread = contract(pick[96:], attended[96 * a : 96 * a + 96], 0, 0).astype(BF16)
        product = contract(spread, t_all[...].reshape(256, 2048), 0, 0)[:HD].astype(BF16)
        for i in range(nz):
            o_part[a, i] = product[:, 128 * i : 128 * i + 128]
    swap = Exchange(("c",), o_part, swapped, sw_s, sw_r, lambda at, i: i)
    swap.start()
    both_grads(4, 5)
    swap.arrive()
    weight.step(0, 0)
    two(weight, 1)
    two(main, 4)
    two(main, 5)
    both_grads(6, 7)
    grads((1, nz // 2 - 1))
    upright = jnp.concatenate([dq[...], jnp.zeros_like(dq[...])], axis=0) * HD**-0.5
    dq_block[...] = jnp.transpose(upright).astype(BF16).reshape(4, 192, 128)
    by_dq = ToOwners(dq_block, dqs, dq_s, dq_r)
    by_dq.start()
    two(weight, 2)
    two(weight, 3)
    two(main, 6)
    two(main, 7)
    by_dq.arrive()
    query_grad = jnp.sum(dqs[...].astype(F32), axis=0).astype(BF16)
    d_target = jnp.zeros((128, 2048), F32)
    for a in range(2):
        spread = contract(pick8[...], query_grad[96 * a : 96 * a + 96], 0, 0).astype(BF16)
        d_target = d_target + jnp.dot(spread, pair_all[a], preferred_element_type=F32)
    d_parts[...] = d_target.astype(BF16).reshape(16, 8, 2048)
    by_t = Exchange(("x", "y"), d_parts, t_in, t_s, t_r, lambda at, i: i)
    by_t.start()
    two(weight, 4)
    two(weight, 5)
    piece = 256 // PIECES
    for p in range(PIECES):
        kv_grad[pl.ds(p * piece, piece)] = main.total(p).astype(BF16)
    by_kv = Exchange(("c",), kv_grad, grads2, kv_s, kv_r)
    by_kv.start()
    two(weight, 6)
    two(weight, 7)
    by_kv.arrive()
    g0, g1 = grads2[0].astype(F32), grads2[1].astype(F32)
    k2 = jnp.where(wide_low, g0, swap_halves(g1)).astype(BF16)
    v2 = jnp.where(wide_low, swap_halves(g0), g1).astype(BF16)
    d_rows = contract(k2, w_all[:, :, 0].reshape(1024, 128), 1, 1)
    d_rows = d_rows + contract(v2, w_all[:, :, 1].reshape(1024, 128), 1, 1)
    parts[...] = d_rows.astype(BF16).reshape(8, 32, 1024)
    by_s = Exchange(("y", "c"), parts, s_in, s_s, s_r, lambda at, i: i)
    by_s.start()
    mine_sum[...] = weight.total(0).astype(BF16)
    back = FarGather(nz, mine_sum, all_sums, back_s, back_r)
    back.start()
    by_t.arrive()
    t_out[...] = jnp.sum(t_in[...].astype(F32), axis=0)
    back.relay()
    by_s.arrive()
    got = []
    for core in range(2):
        total = s_in[core].astype(F32)
        for i in range(1, 4):
            total = total + s_in[2 * i + core].astype(F32)
        got.append(total)
    for j in range(8):
        chip = (2 * j % 4) * 4 + j // 2
        a, b = (g[:, 128 * j : 128 * j + 128] for g in got)
        s_out[:, 128 * chip : 128 * chip + 128] = jnp.where(low, a, swap_halves(b))
        s_out[:, 128 * chip + 512 : 128 * chip + 640] = jnp.where(low, swap_halves(a), b)
    back.arrive()
    for by in (by_rows, by_wy, by_wx, by_ya, by_xb, by_xa, by_yb, by_pair, by_part, by_q, by_z, by_stats):
        by.drain()
    for by in (by_o, by_dq, swap, back, by_kv, by_s, by_t, main, weight):
        by.drain()


def whole(args, nz):
    t = 768
    half = nz // 2

    def bf16(*shape):
        return pltpu.VMEM(shape, BF16)

    def f32(*shape):
        return pltpu.VMEM(shape, F32)

    return pl.pallas_call(
        functools.partial(kernel, nz),
        out_shape=(
            jax.ShapeDtypeStruct((32, 2048), F32),
            jax.ShapeDtypeStruct((8, 2048), F32),
            jax.ShapeDtypeStruct((nz, HD, 128), BF16),
        ),
        in_specs=[pl.BlockSpec(memory_space=pl.ANY)] * len(args),
        out_specs=(VMEM,) * 3,
        scratch_shapes=[
            bf16(6, 2048), bf16(32, 2048), f32(1, 2048), f32(1, 2048), bf16(64, 512), bf16(64, 512),
            bf16(6, 2048), bf16(192, 256), bf16(96, 128), dma(len(args)),
            bf16(128, 2048), bf16(nz, 256, 128), f32(8, t), bf16(4, 192, 128), bf16(t, 128),
            bf16(4, 4, 16, 2048), bf16(2, 128, 2048), bf16(4, 4, 2, 64, 128),
            bf16(2, 32, 1024), bf16(4, 2, 32, 1024), f32(2, 256, 128), f32(2, 256, 128),
            bf16(192, 128), bf16(4, 192, 128), f32(1, t), f32(1, t), f32(HD, t), f32(8, t), f32(4, 8, t),
            f32(HD, t), f32(2, half, 256, 128), bf16(2, half, 256, 128), bf16(2, half, 256, 128),
            bf16(2, half, HD, 128), bf16(2, half, HD, 128),
            bf16(4, 192, 128), bf16(4, 192, 128), bf16(4, 192, 128),
            bf16(2, nz, HD, 128), bf16(2, nz, HD, 128), bf16(HD, 128), bf16(256, 128), bf16(2, 256, 128), bf16(8, 32, 1024), bf16(16, 8, 2048),
            bf16(8, 32, 1024), bf16(16, 8, 2048),
            sems(5, 2), sems(5, 2), dma(1), dma(1), dma(1), sems(3, 4),
            dma(1), sems(3, 2), dma(1), sems(3, 2), dma(1), sems(3, 4), dma(1), sems(3, 4), dma(1), dma(1),
            dma(1), dma(1), dma(4), dma(4), dma(1), sems(2, half, PIECES), dma(1), dma(1),
            dma(4), dma(4), dma(4), dma(4), dma(1), dma(1),
            dma(2), sems(2, half, PIECES), dma(2), sems(2, half, 1),
            dma(1), dma(4), dma(1), dma(1), dma(1), dma(1), dma(1), dma(1),
        ],
        compiler_params=params(0),
    )(*args)


def finish_kernel(
    d_source, d_target, sums, target_rows, source_rows, t_gain, s_gain, cot, t_out, s_out, w_out
):
    t_out[...] = cot[...].astype(F32) + norm_back(target_rows[...], t_gain[...], d_target[:6])
    s_out[...] = norm_back(source_rows[...], s_gain[...], d_source[...])
    for i in range(sums.shape[0]):
        w_out[:, 128 * i : 128 * i + 128] = sums[i].astype(F32)


def finish(*args):
    return pl.pallas_call(
        finish_kernel,
        out_shape=(
            jax.ShapeDtypeStruct((6, 2048), F32),
            jax.ShapeDtypeStruct((32, 2048), F32),
            jax.ShapeDtypeStruct((64, 2048), F32),
        ),
        in_specs=[VMEM] * len(args),
        out_specs=(VMEM,) * 3,
    )(*args)


def picks():
    r = np.arange(96)
    at = 16 * (r // 6) + r % 6
    pick = np.concatenate([at, at + 8])[:, None] == np.arange(256)[None]
    pick8 = (8 * (r // 6) + r % 6)[:, None] == np.arange(128)[None]
    return jnp.asarray(pick.astype(BF16)), jnp.asarray(pick8.astype(BF16))


def body(nz, target_rows, source_rows, t_gain, s_gain, wq, wk, wv, wo, cot):
    gains = (t_gain[None], s_gain[None])
    d_source, d_target, sums = whole(
        (target_rows, source_rows, *gains, wq.T, wk, wv, wo, cot, *picks()), nz
    )
    return finish(d_source, d_target, sums, target_rows, source_rows, *gains, cot)


def solution(mesh):
    nz = mesh.shape["sp"]
    SIZES["z"] = nz
    fine = Mesh(mesh.devices.reshape(nz, 4, 4, 2), ("z", "y", "x", "c"))
    every, plane = ("z", "y", "x", "c"), ("y", "x", "c")
    return jax.shard_map(
        functools.partial(body, nz),
        mesh=fine,
        in_specs=(
            P(every, None), P(every, None), P(), P(),
            P(None, plane), P(plane, None), P(plane, None), P(plane, None), P(every, None),
        ),
        out_specs=(P(every, None), P(every, None), P(plane, None)),
        check_vma=False,
    )
```

```python
import functools

import jax
import jax.numpy as jnp
import numpy as np
from jax import lax
from jax.experimental import pallas as pl
from jax.experimental.pallas import tpu as pltpu
from jax.sharding import Mesh
from jax.sharding import PartitionSpec as P

MESH = pl.DeviceIdType.MESH
HD = 64
EPSILON = 1e-06
F32, BF16 = jnp.float32, jnp.bfloat16
VMEM = pl.BlockSpec(memory_space=pltpu.VMEM)
SIZES = {"y": 4, "x": 4, "c": 2}
PIECES = 2
REACH = 4


def dma(n):
    return pltpu.SemaphoreType.DMA((n,))


def params(cid):
    return pltpu.CompilerParams(
        collective_id=cid, has_side_effects=True, vmem_limit_bytes=62 * 1024 * 1024
    )


def group_size(axes):
    n = 1
    for a in axes:
        n *= SIZES[a]
    return n


def group_index(axes):
    i = 0
    for a in axes:
        i = i * SIZES[a] + lax.axis_index(a)
    return i


def coords_of(index, axes):
    out = {}
    for a in reversed(axes):
        out[a] = lax.rem(index, SIZES[a])
        index = index // SIZES[a]
    return out


def greet(axes):
    n, me = group_size(axes), group_index(axes)
    sem = pltpu.get_barrier_semaphore()

    def one(k, carry):
        pl.semaphore_signal(
            sem, inc=1, device_id=coords_of(lax.rem(me + k, n), axes), device_id_type=MESH
        )
        return carry

    lax.fori_loop(1, n, one, 0)
    return n - 1


def greeted(count):
    pl.semaphore_wait(pltpu.get_barrier_semaphore(), count)


class Exchange:
    def __init__(self, axes, src, dst, send, recv, pick=None):
        self.axes, self.src, self.dst, self.send, self.recv = axes, src, dst, send, recv
        self.n, self.me = group_size(axes), group_index(axes)
        self.pick = pick

    def block(self, index):
        if self.pick is None:
            return self.src
        return self.src.at[self.pick(coords_of(index, self.axes), index)]

    def copy(self, k, slot):
        to = lax.rem(self.me + k, self.n)
        return pltpu.make_async_remote_copy(
            src_ref=self.block(to),
            dst_ref=self.dst.at[slot],
            send_sem=self.send.at[0],
            recv_sem=self.recv.at[0],
            device_id=coords_of(to, self.axes),
            device_id_type=MESH,
        )

    def start(self):
        def one(k, carry):
            self.copy(k, self.me).start()
            return carry

        lax.fori_loop(1, self.n, one, 0)
        self.dst[self.me] = self.block(self.me)[...]

    def others(self):
        return bulk(self.dst.at[pl.ds(0, self.n - 1)], self.send, self.recv)

    def arrive(self):
        self.others().wait_recv()

    def drain(self):
        self.others().wait_send()


def bulk(ref, send, recv):
    return pltpu.make_async_remote_copy(
        src_ref=ref,
        dst_ref=ref,
        send_sem=send.at[0],
        recv_sem=recv.at[0],
        device_id={"c": 1 - lax.axis_index("c")},
        device_id_type=MESH,
    )


class ToReaders:
    def __init__(self, src, dst, send, recv):
        self.src, self.dst, self.send, self.recv = src, dst, send, recv
        self.y, self.x, self.c = (lax.axis_index(a) for a in "yxc")
        self.mine = self.x // 2 == self.c

    def copy(self, k, slot):
        return pltpu.make_async_remote_copy(
            src_ref=self.src,
            dst_ref=self.dst.at[slot],
            send_sem=self.send.at[k],
            recv_sem=self.recv.at[slot],
            device_id={"x": lax.rem(self.x + k, 4), "c": self.x // 2},
            device_id_type=MESH,
        )

    def slot(self):
        return lax.rem(self.x, 2) * 2 + self.c

    def start(self):
        for k in range(1, 4):
            self.copy(k, self.slot()).start()

        @pl.when(jnp.logical_not(self.mine))
        def _():
            self.copy(0, self.slot()).start()

        @pl.when(self.mine)
        def _():
            self.dst[self.slot()] = self.src[...]

    def arrive(self):
        for s in range(4):
            own = jnp.logical_and(2 * self.c + s // 2 == self.x, self.c == s % 2)

            @pl.when(jnp.logical_not(own))
            def _():
                self.copy(1, s).wait_recv()

    def drain(self):
        for k in range(1, 4):
            self.copy(k, self.slot()).wait_send()

        @pl.when(jnp.logical_not(self.mine))
        def _():
            self.copy(0, self.slot()).wait_send()


class ToOwners:
    def __init__(self, src, dst, send, recv):
        self.src, self.dst, self.send, self.recv = src, dst, send, recv
        self.y, self.x, self.c = (lax.axis_index(a) for a in "yxc")

    def copy(self, s, slot):
        return pltpu.make_async_remote_copy(
            src_ref=self.src.at[s],
            dst_ref=self.dst.at[slot],
            send_sem=self.send.at[s],
            recv_sem=self.recv.at[slot],
            device_id={"x": 2 * self.c + s // 2, "c": jnp.int32(s % 2)},
            device_id_type=MESH,
        )

    def own(self, s):
        return jnp.logical_and(2 * self.c + s // 2 == self.x, self.c == s % 2)

    def start(self):
        for s in range(4):
            @pl.when(jnp.logical_not(self.own(s)))
            def _():
                self.copy(s, self.x).start()

            @pl.when(self.own(s))
            def _():
                self.dst[self.x] = self.src[s]

    def arrive(self):
        for j in range(4):
            own = jnp.logical_and(self.x == j, self.x // 2 == self.c)

            @pl.when(jnp.logical_not(own))
            def _():
                self.copy(0, j).wait_recv()

    def drain(self):
        for s in range(4):
            @pl.when(jnp.logical_not(self.own(s)))
            def _():
                self.copy(s, self.x).wait_send()


def lanes_below(shape, bound):
    return lax.broadcasted_iota(jnp.int32, shape, 1) < bound


def contract(a, b, da, db):
    return lax.dot_general(a, b, (((da,), (db,)), ((), ())), preferred_element_type=F32)


def ring_greet(nz):
    z = lax.axis_index("z")
    sem = pltpu.get_barrier_semaphore()
    right, left = lax.rem(z + 1, nz), lax.rem(z + nz - 1, nz)
    for to in (left, right):
        pl.semaphore_signal(sem, inc=1, device_id={"z": to}, device_id_type=MESH)
    return 2


class RingGather:
    def __init__(self, axis, piece, count, three, send, recv):
        self.axis, self.piece, self.count, self.send, self.recv = axis, piece, count, send, recv
        self.three = three
        self.me = lax.axis_index(axis)

    def at(self, offset):
        return lax.rem(self.me + offset + 4, 4)

    def copy(self, slot, p, sign, kind):
        ref = self.piece(slot, p)
        return pltpu.make_async_remote_copy(
            src_ref=ref,
            dst_ref=ref,
            send_sem=self.send.at[0],
            recv_sem=self.recv.at[kind, p],
            device_id={self.axis: self.at(sign)},
            device_id_type=MESH,
        )

    def start(self, p):
        self.copy(self.me, p, 1, 0).start()
        self.copy(self.me, p, -1, 1).start()

    def relay(self, p):
        self.copy(self.at(-1), p, 1, 0).wait_recv()
        self.copy(self.at(1), p, -1, 1).wait_recv()
        if p < self.count // 2:
            self.copy(self.at(-1), p, 1, 2).start()
        else:
            self.copy(self.at(1), p, -1, 2).start()

    def arrive(self, p):
        self.copy(self.at(2), p, 1, 2).wait_recv()

    def drain(self):
        bulk(self.three, self.send, self.send).wait_send()


class RowGather:
    def __init__(self, halves, out, send, recv):
        self.halves, self.out, self.send, self.recv = halves, out, send, recv
        self.y, self.c = lax.axis_index("y"), lax.axis_index("c")

    def at(self, offset):
        return lax.rem(self.y + offset + 4, 4)

    def first(self, sign, core, slot_y, slot_c):
        kind = 0 if sign > 0 else 1
        return pltpu.make_async_remote_copy(
            src_ref=self.halves.at[core],
            dst_ref=self.out.at[slot_y, slot_c],
            send_sem=self.send.at[kind, core],
            recv_sem=self.recv.at[kind, slot_c],
            device_id={"y": self.at(sign), "c": jnp.int32(core)},
            device_id_type=MESH,
        )

    def partner(self, slot_c):
        return pltpu.make_async_remote_copy(
            src_ref=self.halves.at[1 - self.c],
            dst_ref=self.out.at[self.y, slot_c],
            send_sem=self.send.at[4, 0],
            recv_sem=self.recv.at[4, 0],
            device_id={"c": 1 - self.c},
            device_id_type=MESH,
        )

    def second(self, sign, slot_y, slot_c):
        kind = 2 if sign > 0 else 3
        ref = self.out.at[slot_y, slot_c, pl.ds(0 if sign > 0 else 16, 16)]
        return pltpu.make_async_remote_copy(
            src_ref=ref,
            dst_ref=ref,
            send_sem=self.send.at[kind, slot_c],
            recv_sem=self.recv.at[kind, slot_c],
            device_id={"y": self.at(sign)},
            device_id_type=MESH,
        )

    def start(self):
        for core in range(2):
            self.first(1, core, self.y, self.c).start()
            self.first(-1, core, self.y, self.c).start()
        self.partner(self.c).start()
        self.out[self.y, self.c] = self.halves[self.c]

    def relay(self):
        for core in range(2):
            self.first(1, 0, self.at(-1), core).wait_recv()
            self.second(1, self.at(-1), core).start()
            self.first(-1, 0, self.at(1), core).wait_recv()
            self.second(-1, self.at(1), core).start()

    def arrive(self):
        self.partner(1 - self.c).wait_recv()
        for core in range(2):
            self.second(1, self.at(2), core).wait_recv()
            self.second(-1, self.at(2), core).wait_recv()

    def drain(self):
        self.partner(self.c).wait_send()
        for core in range(2):
            self.first(1, core, self.y, self.c).wait_send()
            self.first(-1, core, self.y, self.c).wait_send()
            self.second(1, self.y, core).wait_send()
            self.second(-1, self.y, core).wait_send()


class WeightColumn:
    def __init__(self, wk, wv, out, send, recv):
        self.parts, self.out, self.send, self.recv = (wk, wv), out, send, recv
        self.y, self.x = lax.axis_index("y"), lax.axis_index("x")

    def lanes(self, y):
        return pl.ds(pl.multiple_of(y * 128, 128), 128)

    def copy(self, k, i, slot_y):
        to = lax.rem(self.y + k, 4)
        return pltpu.make_async_remote_copy(
            src_ref=self.parts[i].at[:, self.lanes(to)],
            dst_ref=self.out.at[to, self.x, slot_y, :, pl.ds(128 * i, 128)],
            send_sem=self.send.at[0],
            recv_sem=self.recv.at[0],
            device_id={"y": to},
            device_id_type=MESH,
        )

    def start(self):
        for k in (2, 1, 3):
            for i in range(2):
                self.copy(k, i, self.y).start()
        for i in range(2):
            block = self.parts[i][:, self.lanes(self.y)]
            self.out[self.y, self.x, self.y, :, 128 * i : 128 * i + 128] = block

    def others(self):
        return bulk(self.out.at[0, 0, pl.ds(0, 3)], self.send, self.recv)

    def arrive(self):
        self.others().wait_recv()

    def drain(self):
        self.others().wait_send()


def unit_rows(matrix, gain):
    wide = matrix.astype(F32)
    factor = lax.rsqrt(jnp.mean(wide * wide, axis=-1, keepdims=True) + EPSILON)
    return wide * factor * gain


def swap_halves(a):
    return pltpu.roll(a, HD, 1)


class StrideGather:
    def __init__(self, nz, blocks, send, recv):
        self.nz, self.blocks, self.send, self.recv = nz, blocks, send, recv
        self.z = lax.axis_index("z")
        self.rows = blocks.shape[1] // PIECES
        self.far = {1: nz // 2, -1: nz - 1 - nz // 2}

    def at(self, offset):
        return lax.rem(self.z + offset + self.nz, self.nz)

    def copy(self, sign, distance, d, p):
        ref = self.blocks.at[self.at(-sign * distance), pl.ds(p * self.rows, self.rows)]
        return pltpu.make_async_remote_copy(
            src_ref=ref,
            dst_ref=ref,
            send_sem=self.send.at[0],
            recv_sem=self.recv.at[0 if sign > 0 else 1, distance + d - 1, p],
            device_id={"z": self.at(sign * d)},
            device_id_type=MESH,
        )

    def arrived(self, sign, distance, p):
        ref = self.blocks.at[self.at(-sign * distance), pl.ds(p * self.rows, self.rows)]
        return pltpu.make_async_remote_copy(
            src_ref=ref,
            dst_ref=ref,
            send_sem=self.send.at[0],
            recv_sem=self.recv.at[0 if sign > 0 else 1, distance - 1, p],
            device_id={"z": self.at(sign)},
            device_id_type=MESH,
        )

    def start(self):
        for d in (2, 1):
            for p in range(PIECES):
                for sign in (1, -1):
                    self.copy(sign, 0, d, p).start()

    def relay(self, distance):
        for p in range(PIECES):
            for sign in (1, -1):
                if distance <= self.far[sign]:
                    self.arrived(sign, distance, p).wait_recv()
                if distance + 2 <= self.far[sign]:
                    self.copy(sign, distance, 2, p).start()
        for p in range(PIECES):
            for sign in (1, -1):
                if distance + 1 <= self.far[sign]:
                    self.copy(sign, distance, 1, p).start()

    def arrive(self, distance):
        for sign in (1, -1):
            if distance <= self.far[sign]:
                for p in range(PIECES):
                    self.arrived(sign, distance, p).wait_recv()

    def drain(self):
        bulk(self.blocks.at[pl.ds(0, self.nz - 1)], self.send, self.send).wait_send()


class StrideSum:
    def __init__(self, nz, term, out, arrived, send, recv, pieces):
        self.nz, self.term, self.out, self.arrived = nz, term, out, arrived
        self.send, self.recv, self.pieces = send, recv, pieces
        self.rows = out.shape[2] // pieces
        self.z = lax.axis_index("z")

    def chained(self, side, j):
        return (j + side) % 2 == 0

    def hop(self, side, j, p):
        at = pl.ds(p * self.rows, self.rows)
        d = (2 if self.chained(side, j) else 1) * (1 if side else -1)
        return pltpu.make_async_remote_copy(
            src_ref=self.out.at[side, j, at],
            dst_ref=self.arrived.at[side, j, at],
            send_sem=self.send.at[side],
            recv_sem=self.recv.at[side, j, p],
            device_id={"z": lax.rem(self.z + d + self.nz, self.nz)},
            device_id_type=MESH,
        )

    def joined(self, side, j, p, value):
        at = pl.ds(p * self.rows, self.rows)
        for i in (j - 1, j - 2):
            if i >= 0:
                self.hop(side, i, p).wait_recv()
                value = value + self.arrived[side, i, at].astype(F32)
        return value

    def step(self, side, j):
        for p in range(self.pieces):
            at = pl.ds(p * self.rows, self.rows)
            value = self.term(side, j, at)
            if self.chained(side, j):
                value = self.joined(side, j, p, value)
            self.out[side, j, at] = value.astype(BF16)
            self.hop(side, j, p).start()

    def total(self, p):
        half = self.nz // 2
        at = pl.ds(p * self.rows, self.rows)
        value = self.joined(1, half - 1, p, self.term(1, half - 1, at))
        return self.joined(0, half, p, value)

    def drain(self):
        half = self.nz // 2
        for side in range(2):
            sem = self.send.at[pl.ds(side, 1)]
            bulk(self.out.at[side, pl.ds(0, half - side)], sem, sem).wait_send()


class FarGather:
    def __init__(self, nz, src, dst, send, recv):
        self.nz, self.src, self.dst, self.send, self.recv = nz, src, dst, send, recv
        self.z = lax.axis_index("z")
        self.far = {1: nz // 2 - REACH, -1: nz - 1 - nz // 2 - REACH}

    def at(self, offset):
        return lax.rem(self.z + offset + self.nz, self.nz)

    def copy(self, slot, sign, d, relay):
        kind = 3 if relay else 2 if d < REACH else 0 if sign > 0 else 1
        return pltpu.make_async_remote_copy(
            src_ref=self.dst.at[slot] if relay else self.src,
            dst_ref=self.dst.at[slot],
            send_sem=self.send.at[0],
            recv_sem=self.recv.at[kind],
            device_id={"z": self.at(sign * d)},
            device_id_type=MESH,
        )

    def several(self, count, kind):
        return bulk(self.dst.at[pl.ds(0, count)], self.send, self.recv.at[pl.ds(kind, 1)])

    def start(self):
        for d in range(REACH, 0, -1):
            for sign in (1, -1):
                self.copy(self.z, sign, d, False).start()
        self.dst[self.z] = self.src[...]

    def relay(self):
        for sign in (1, -1):
            slot = self.at(-sign * REACH)
            self.copy(slot, sign, REACH, False).wait_recv()
            for d in range(self.far[sign], 0, -1):
                self.copy(slot, sign, d, True).start()

    def arrive(self):
        self.several(2 * REACH - 2, 2).wait_recv()
        self.several(self.nz - 1 - 2 * REACH, 3).wait_recv()

    def drain(self):
        self.several(self.nz - 1, 0).wait_send()


def reach_greet(nz):
    z = lax.axis_index("z")
    for d in range(1, REACH + 1):
        for sign in (1, -1):
            pl.semaphore_signal(
                pltpu.get_barrier_semaphore(),
                inc=1,
                device_id={"z": lax.rem(z + sign * d + nz, nz)},
                device_id_type=MESH,
            )
    return 2 * REACH


def sems(*shape):
    return pltpu.SemaphoreType.DMA(shape)


def norm_back(matrix, gain, upstream):
    wide = matrix.astype(F32)
    factor = lax.rsqrt(jnp.mean(wide * wide, axis=-1, keepdims=True) + EPSILON)
    weighted = upstream * gain
    inner = jnp.mean(weighted * wide, axis=-1, keepdims=True)
    return factor * weighted - wide * factor**3 * inner


def kernel(
    nz, target_rows_h, source_rows_h, t_gain_h, s_gain_h, wq_h, wk_h, wv_h, wo_h, cot_h, pick_h, pick8_h,
    s_out, t_out, all_sums,
    target_rows, source_rows, t_gain, s_gain, wk, wv, cot, pick, pick8, loads,
    pair, kv_all, stats, out, qa, t_all, pair_all, w_all,
    halves, rows_all, part, part_all, block, blocks, m, l, o, said, heard,
    dq, mine, ring_out, ring_in, w_ring_out, w_ring_in, outs, dq_block, dqs, o_part, swapped,
    mine_sum, kv_grad, grads8, parts, d_parts, s_in, t_in,
    row_s, row_r, wy_s, wy_r, wx_s, wx_r, wf_s, wf_r, ya_s, ya_r, xb_s, xb_r, xa_s, xa_r, yb_s, yb_r, pair_s, pair_r,
    part_s, part_r, q_s, q_r, z_s, z_r, ss, sr,
    o_s, o_r, dq_s, dq_r, sw_s, sw_r, g_s, g_r, h_s, h_r, back_s, back_r,
    kv_s, kv_r, s_s, s_r, t_s, t_r,
):
    z, y, x, c = (lax.axis_index(a) for a in "zyxc")
    met = greet(("y", "x", "c")) + reach_greet(nz)

    staged = (
        (source_rows_h, source_rows), (s_gain_h, s_gain), (wk_h, wk), (wv_h, wv),
        (target_rows_h, target_rows), (t_gain_h, t_gain), (cot_h, cot),
        (wq_h, pair.at[pl.ds(0, HD)]), (wo_h, pair.at[pl.ds(HD, HD)]), (pick_h, pick), (pick8_h, pick8),
    )
    copies = [pltpu.make_async_copy(a, b, loads.at[i]) for i, (a, b) in enumerate(staged)]
    for copy in copies:
        copy.start()
    for copy in copies[:2]:
        copy.wait()
    normed = unit_rows(source_rows[...], s_gain[...])
    low = lanes_below((32, 128), HD)
    for j in range(8):
        chip = (2 * j % 4) * 4 + j // 2
        first, second = (normed[:, 128 * i : 128 * i + 128] for i in (chip, chip + 4))
        halves[0, :, 128 * j : 128 * j + 128] = jnp.where(low, first, swap_halves(second)).astype(BF16)
        halves[1, :, 128 * j : 128 * j + 128] = jnp.where(low, swap_halves(first), second).astype(BF16)
    for copy in copies[2:]:
        copy.wait()
    greeted(met)

    by_rows = RowGather(halves, rows_all, row_s, row_r)
    by_wy = WeightColumn(wk, wv, w_all, wy_s, wy_r)
    by_wx = RingGather(
        "x", lambda slot, p: w_all.at[y, slot, p], 4, w_all.at[y, pl.ds(0, 3)], wx_s, wx_r
    )
    by_wf = RingGather("y", lambda slot, p: w_all.at[slot, p], 4, w_all.at[pl.ds(0, 3)], wf_s, wf_r)
    three, first, second = pl.ds(0, 3), pl.ds(0, 1024), pl.ds(1024, 1024)
    by_ya = RingGather(
        "y", lambda slot, p: t_all.at[x, slot, :, pl.ds(512 * p, 512)], 2,
        t_all.at[x, three, :, first], ya_s, ya_r,
    )
    by_xb = RingGather(
        "x", lambda slot, p: t_all.at[slot, y, :, pl.ds(1024 + 512 * p, 512)], 2,
        t_all.at[three, y, :, second], xb_s, xb_r,
    )
    by_xa = RingGather(
        "x", lambda slot, p: t_all.at[slot, p, :, first], 4, t_all.at[three, :, :, first], xa_s, xa_r
    )
    by_yb = RingGather(
        "y", lambda slot, p: t_all.at[p, slot, :, second], 4, t_all.at[:, three, :, second], yb_s, yb_r
    )
    by_pair = Exchange(("c",), pair, pair_all, pair_s, pair_r)
    by_wy.start()
    by_rows.start()
    zero = jnp.zeros((2, target_rows.shape[1]), F32)
    t_all[x, y] = jnp.concatenate(
        [unit_rows(target_rows[...], t_gain[...]), zero, cot[...].astype(F32), zero], axis=0
    ).astype(BF16)
    for p in range(2):
        by_xb.start(p)
        by_ya.start(p)
    by_pair.start()

    by_wy.arrive()
    for p in range(4):
        by_wx.start(p)
    by_rows.relay()
    for p in range(4):
        by_wx.relay(p)
    for p in range(2):
        by_xb.relay(p)
        by_ya.relay(p)
    for p in range(2):
        by_xb.arrive(p)
        by_ya.arrive(p)
    for p in range(4):
        by_xa.start(p)
        by_yb.start(p)
    by_rows.arrive()
    for p in range(4):
        by_wx.arrive(p)

    rows = rows_all[...].reshape(256, 1024)
    kv2 = jnp.dot(rows, w_all[y].reshape(1024, 256), preferred_element_type=F32)
    k2, v2 = kv2[:, :128], kv2[:, 128:]
    wide_low = lanes_below((256, 128), HD)
    part[0] = jnp.where(wide_low, k2, swap_halves(v2))
    part[1] = jnp.where(wide_low, swap_halves(k2), v2)
    by_part = Exchange(("c",), part, part_all, part_s, part_r, lambda at, i: i)
    by_part.start()
    by_part.arrive()
    kv_all[z] = (part_all[0] + part_all[1]).astype(BF16)

    by_z = StrideGather(nz, kv_all, z_s, z_r)
    by_z.start()
    for p in range(4):
        by_xa.relay(p)
        by_yb.relay(p)
    for p in range(4):
        by_wf.start(p)
    by_z.relay(2)
    by_pair.arrive()
    for p in range(4):
        by_xa.arrive(p)
        by_yb.arrive(p)
    everything = t_all[...].reshape(256, 2048)
    wide = lax.broadcasted_iota(jnp.int32, (256, 256), 1)
    scale = jnp.where(lax.rem(wide, 128) < HD, HD**-0.5, 1.0)
    projected = contract(everything, pair_all[...].reshape(256, 2048), 1, 1) * scale
    chosen = jnp.dot(pick[...], projected.astype(BF16), preferred_element_type=F32)
    narrow = lanes_below((96, 128), HD)
    for a in range(2):
        at = slice(128 * a, 128 * a + 128)
        block[96 * a : 96 * a + 96] = jnp.where(narrow, chosen[:96, at], chosen[96:, at]).astype(BF16)
    by_q = ToReaders(block, blocks, q_s, q_r)
    by_q.start()
    by_z.relay(4)
    m[...] = jnp.full(m.shape, -1e30, F32)
    l[...] = jnp.zeros(l.shape, F32)
    o[...] = jnp.zeros(o.shape, F32)
    by_q.arrive()
    qa[...] = blocks[...].reshape(qa.shape)

    def blocks_of(planes):
        return jnp.concatenate([kv_all[at] for at in planes], axis=0)

    def attend(*planes):
        block = blocks_of(planes)
        keys = jnp.where(lanes_below(block.shape, HD), block, jnp.zeros_like(block))
        scores = contract(keys, qa[...], 1, 1)
        top = jnp.maximum(m[...], jnp.max(scores, axis=0, keepdims=True))
        weights = jnp.exp(scores - top)
        old = jnp.exp(m[...] - top)
        m[...] = top
        l[...] = l[...] * old + jnp.sum(weights, axis=0, keepdims=True)
        o[...] = o[...] * old + contract(block, weights.astype(BF16), 0, 0)[HD:]

    def attend_from(low, high):
        def one(d, carry):
            attend(lax.rem(z + d, nz), lax.rem(z + nz - d, nz))
            return carry

        lax.fori_loop(low, high + 1, one, 0)

    attend(z)
    by_z.arrive(1)
    attend_from(1, 2)
    by_z.relay(6)
    by_z.arrive(3)
    by_z.arrive(5)
    attend_from(3, 6)
    by_z.arrive(7)
    by_z.arrive(8)
    attend_from(7, 7)
    attend(lax.rem(z + nz // 2, nz))
    upright = jnp.transpose(qa[...].astype(F32))
    delta = jnp.sum(upright[HD:] * o[...], axis=0, keepdims=True)
    row = lax.broadcasted_iota(jnp.int32, (8, qa.shape[0]), 0)
    said[...] = jnp.where(row == 0, m[...], jnp.where(row == 1, l[...], delta))
    by_stats = Exchange(("x",), said, heard, ss, sr)
    by_stats.start()
    log_sum = m[...] + jnp.log(l[...])
    high = log_sum.astype(BF16)
    rest = log_sum - high.astype(F32)
    middle = rest.astype(BF16)
    low_part = rest - middle.astype(F32)
    line = lax.broadcasted_iota(jnp.int32, (HD, qa.shape[0]), 0)
    parts3 = jnp.where(line == 0, high.astype(F32), jnp.where(line == 1, middle.astype(F32), low_part))
    upright = jnp.concatenate([o[...] / l[...], jnp.where(line < 3, parts3, 0.0)], axis=0)
    out[...] = jnp.transpose(upright).astype(BF16).reshape(out.shape)
    by_o = ToOwners(out, outs, o_s, o_r)
    by_o.start()
    for p in range(4):
        by_wf.relay(p)
    by_stats.arrive()
    top = jnp.max(heard[:, 0:1], axis=0)
    total = jnp.zeros_like(top)
    both = jnp.zeros_like(top)
    for j in range(4):
        w = jnp.exp(heard[j, 0:1] - top)
        total = total + w * heard[j, 1:2]
        both = both + w * heard[j, 2:3]
    stats[...] = jnp.where(row == 0, top + jnp.log(total), both / total)
    dq[...] = jnp.zeros(dq.shape, F32)

    def plane_of(side, j):
        offset = nz // 2 - 1 - j if side else j - nz // 2
        return lax.rem(z + nz + offset, nz)

    def grads(*terms):
        block = blocks_of([plane_of(side, j) for side, j in terms])
        low = lanes_below(block.shape, HD)
        none = jnp.zeros_like(block)
        scores = contract(jnp.where(low, block, none), qa[...], 1, 1)
        probs = jnp.exp(scores - stats[0:1])
        d_probs = contract(jnp.where(low, none, block), qa[...], 1, 1)
        d_scores = (probs * (d_probs - stats[1:2])).astype(BF16)
        for_v = contract(probs.astype(BF16), qa[...], 1, 0)
        for_k = contract(d_scores, qa[...], 1, 0)
        dq[...] += contract(block, d_scores, 0, 0)[:HD]
        both = jnp.where(low, for_k, for_v)
        for i, (side, j) in enumerate(terms):
            mine[side, j] = both[256 * i : 256 * i + 256]

    def both_grads(low, high):
        def one(j, carry):
            grads((0, j), (1, j - 1))
            return carry

        lax.fori_loop(low, high + 1, one, 0)

    main = StrideSum(nz, lambda side, j, at: mine[side, j, at], ring_out, ring_in, g_s, g_r, PIECES)

    def own_weight(side, j, at):
        to = plane_of(side, j)
        return swapped[0, to, at].astype(F32) + swapped[1, to, at].astype(F32)

    weight = StrideSum(nz, own_weight, w_ring_out, w_ring_in, h_s, h_r, 1)

    def two(ring, j):
        ring.step(0, j)
        ring.step(1, j - 1)

    grads((0, 0))
    main.step(0, 0)
    by_o.arrive()
    lanes = lax.broadcasted_iota(jnp.int32, (192, 128), 1)
    given = [outs[i].astype(F32) for i in range(4)]
    log_sums = [
        jnp.sum(jnp.where(jnp.logical_and(lanes >= HD, lanes < HD + 3), g, 0.0), axis=1, keepdims=True)
        for g in given
    ]
    largest = functools.reduce(jnp.maximum, log_sums)
    shares = [jnp.exp(part_sum - largest) for part_sum in log_sums]
    whole_sum = sum(g * w for g, w in zip(given, shares)) / sum(shares)
    attended = jnp.where(lanes < HD, whole_sum, 0.0).astype(BF16)
    for a in range(2):
        spread = contract(pick[96:], attended[96 * a : 96 * a + 96], 0, 0).astype(BF16)
        product = contract(spread, t_all[...].reshape(256, 2048), 0, 0)[:HD].astype(BF16)
        for i in range(nz):
            o_part[a, i] = product[:, 128 * i : 128 * i + 128]
    swap = Exchange(("c",), o_part, swapped, sw_s, sw_r, lambda at, i: i)
    swap.start()
    both_grads(1, 1)
    two(main, 1)
    swap.arrive()
    weight.step(0, 0)
    two(weight, 1)
    both_grads(2, 3)
    two(main, 2)
    two(main, 3)
    both_grads(4, 5)
    two(weight, 2)
    two(weight, 3)
    two(main, 4)
    two(main, 5)
    both_grads(6, 7)
    grads((1, nz // 2 - 1))
    upright = jnp.concatenate([dq[...], jnp.zeros_like(dq[...])], axis=0) * HD**-0.5
    dq_block[...] = jnp.transpose(upright).astype(BF16).reshape(4, 192, 128)
    by_dq = ToOwners(dq_block, dqs, dq_s, dq_r)
    by_dq.start()
    two(weight, 4)
    two(weight, 5)
    two(main, 6)
    two(main, 7)
    by_dq.arrive()
    query_grad = jnp.sum(dqs[...].astype(F32), axis=0).astype(BF16)
    d_target = jnp.zeros((128, 2048), F32)
    for a in range(2):
        spread = contract(pick8[...], query_grad[96 * a : 96 * a + 96], 0, 0).astype(BF16)
        d_target = d_target + jnp.dot(spread, pair_all[a], preferred_element_type=F32)
    d_parts[...] = d_target.astype(BF16).reshape(16, 8, 2048)
    by_t = Exchange(("x", "y"), d_parts, t_in, t_s, t_r, lambda at, i: i)
    by_t.start()
    two(weight, 6)
    two(weight, 7)
    for p in range(4):
        by_wf.arrive(p)
    mine_sum[...] = weight.total(0).astype(BF16)
    back = FarGather(nz, mine_sum, all_sums, back_s, back_r)
    back.start()
    piece = 256 // PIECES
    for p in range(PIECES):
        kv_grad[2 * p : 2 * p + 2] = main.total(p).astype(BF16).reshape(2, 64, 128)
    by_kv = Exchange(("y", "c"), kv_grad, grads8, kv_s, kv_r, lambda at, i: at["y"])
    by_kv.start()
    by_t.arrive()
    t_out[...] = jnp.sum(t_in[...].astype(F32), axis=0)
    by_kv.arrive()
    narrow = lanes_below((64, 128), HD)
    d_rows = jnp.zeros((64, 1024), F32)
    for i in range(4):
        g0, g1 = grads8[2 * i].astype(F32), grads8[2 * i + 1].astype(F32)
        k2 = jnp.where(narrow, g0, swap_halves(g1)).astype(BF16)
        v2 = jnp.where(narrow, swap_halves(g0), g1).astype(BF16)
        kv2 = jnp.concatenate([k2, v2], axis=1)
        d_rows = d_rows + contract(kv2, w_all[i].reshape(1024, 256), 1, 1)
    parts[...] = d_rows.astype(BF16).reshape(2, 32, 1024)
    by_s = Exchange(("c",), parts, s_in, s_s, s_r, lambda at, i: i)
    by_s.start()
    back.relay()
    by_s.arrive()
    got = [s_in[core].astype(F32) for core in range(2)]
    for j in range(8):
        chip = (2 * j % 4) * 4 + j // 2
        a, b = (g[:, 128 * j : 128 * j + 128] for g in got)
        s_out[:, 128 * chip : 128 * chip + 128] = jnp.where(low, a, swap_halves(b))
        s_out[:, 128 * chip + 512 : 128 * chip + 640] = jnp.where(low, swap_halves(a), b)
    back.arrive()
    for by in (by_rows, by_wy, by_wx, by_wf, by_ya, by_xb, by_xa, by_yb, by_pair, by_part, by_q, by_z, by_stats):
        by.drain()
    for by in (by_o, by_dq, swap, back, by_kv, by_s, by_t, main, weight):
        by.drain()


def whole(args, nz):
    t = 768
    half = nz // 2

    def bf16(*shape):
        return pltpu.VMEM(shape, BF16)

    def f32(*shape):
        return pltpu.VMEM(shape, F32)

    return pl.pallas_call(
        functools.partial(kernel, nz),
        out_shape=(
            jax.ShapeDtypeStruct((32, 2048), F32),
            jax.ShapeDtypeStruct((8, 2048), F32),
            jax.ShapeDtypeStruct((nz, HD, 128), BF16),
        ),
        in_specs=[pl.BlockSpec(memory_space=pl.ANY)] * len(args),
        out_specs=(VMEM,) * 3,
        scratch_shapes=[
            bf16(6, 2048), bf16(32, 2048), f32(1, 2048), f32(1, 2048), bf16(64, 512), bf16(64, 512),
            bf16(6, 2048), bf16(192, 256), bf16(96, 128), dma(len(args)),
            bf16(128, 2048), bf16(nz, 256, 128), f32(8, t), bf16(4, 192, 128), bf16(t, 128),
            bf16(4, 4, 16, 2048), bf16(2, 128, 2048), bf16(4, 4, 4, 64, 256),
            bf16(2, 32, 1024), bf16(4, 2, 32, 1024), f32(2, 256, 128), f32(2, 256, 128),
            bf16(192, 128), bf16(4, 192, 128), f32(1, t), f32(1, t), f32(HD, t), f32(8, t), f32(4, 8, t),
            f32(HD, t), f32(2, half, 256, 128), bf16(2, half, 256, 128), bf16(2, half, 256, 128),
            bf16(2, half, HD, 128), bf16(2, half, HD, 128),
            bf16(4, 192, 128), bf16(4, 192, 128), bf16(4, 192, 128),
            bf16(2, nz, HD, 128), bf16(2, nz, HD, 128), bf16(HD, 128), bf16(4, 64, 128), bf16(8, 64, 128), bf16(2, 32, 1024), bf16(16, 8, 2048),
            bf16(2, 32, 1024), bf16(16, 8, 2048),
            sems(5, 2), sems(5, 2), dma(1), dma(1), dma(1), sems(3, 4), dma(1), sems(3, 4),
            dma(1), sems(3, 2), dma(1), sems(3, 2), dma(1), sems(3, 4), dma(1), sems(3, 4), dma(1), dma(1),
            dma(1), dma(1), dma(4), dma(4), dma(1), sems(2, half, PIECES), dma(1), dma(1),
            dma(4), dma(4), dma(4), dma(4), dma(1), dma(1),
            dma(2), sems(2, half, PIECES), dma(2), sems(2, half, 1),
            dma(1), dma(4), dma(1), dma(1), dma(1), dma(1), dma(1), dma(1),
        ],
        compiler_params=params(0),
    )(*args)


def finish_kernel(
    d_source, d_target, sums, target_rows, source_rows, t_gain, s_gain, cot, t_out, s_out, w_out
):
    t_out[...] = cot[...].astype(F32) + norm_back(target_rows[...], t_gain[...], d_target[:6])
    s_out[...] = norm_back(source_rows[...], s_gain[...], d_source[...])
    for i in range(sums.shape[0]):
        w_out[:, 128 * i : 128 * i + 128] = sums[i].astype(F32)


def finish(*args):
    return pl.pallas_call(
        finish_kernel,
        out_shape=(
            jax.ShapeDtypeStruct((6, 2048), F32),
            jax.ShapeDtypeStruct((32, 2048), F32),
            jax.ShapeDtypeStruct((64, 2048), F32),
        ),
        in_specs=[VMEM] * len(args),
        out_specs=(VMEM,) * 3,
    )(*args)


def picks():
    r = np.arange(96)
    at = 16 * (r // 6) + r % 6
    pick = np.concatenate([at, at + 8])[:, None] == np.arange(256)[None]
    pick8 = (8 * (r // 6) + r % 6)[:, None] == np.arange(128)[None]
    return jnp.asarray(pick.astype(BF16)), jnp.asarray(pick8.astype(BF16))


def body(nz, target_rows, source_rows, t_gain, s_gain, wq, wk, wv, wo, cot):
    gains = (t_gain[None], s_gain[None])
    d_source, d_target, sums = whole(
        (target_rows, source_rows, *gains, wq.T, wk, wv, wo, cot, *picks()), nz
    )
    return finish(d_source, d_target, sums, target_rows, source_rows, *gains, cot)


def solution(mesh):
    nz = mesh.shape["sp"]
    SIZES["z"] = nz
    fine = Mesh(mesh.devices.reshape(nz, 4, 4, 2), ("z", "y", "x", "c"))
    every, plane = ("z", "y", "x", "c"), ("y", "x", "c")
    return jax.shard_map(
        functools.partial(body, nz),
        mesh=fine,
        in_specs=(
            P(every, None), P(every, None), P(), P(),
            P(None, plane), P(plane, None), P(plane, None), P(plane, None), P(every, None),
        ),
        out_specs=(P(every, None), P(every, None), P(plane, None)),
        check_vma=False,
    )
```

```python
import functools

import jax
import jax.numpy as jnp
import numpy as np
from jax import lax
from jax.experimental import pallas as pl
from jax.experimental.pallas import tpu as pltpu
from jax.sharding import Mesh
from jax.sharding import PartitionSpec as P

MESH = pl.DeviceIdType.MESH
HD = 64
EPSILON = 1e-06
F32, BF16 = jnp.float32, jnp.bfloat16
VMEM = pl.BlockSpec(memory_space=pltpu.VMEM)
SIZES = {"y": 4, "x": 4, "c": 2}
PIECES = 2
REACH = 4


def dma(n):
    return pltpu.SemaphoreType.DMA((n,))


def params(cid):
    return pltpu.CompilerParams(
        collective_id=cid, has_side_effects=True, vmem_limit_bytes=62 * 1024 * 1024
    )


def group_size(axes):
    n = 1
    for a in axes:
        n *= SIZES[a]
    return n


def group_index(axes):
    i = 0
    for a in axes:
        i = i * SIZES[a] + lax.axis_index(a)
    return i


def coords_of(index, axes):
    out = {}
    for a in reversed(axes):
        out[a] = lax.rem(index, SIZES[a])
        index = index // SIZES[a]
    return out


def greet(axes):
    n, me = group_size(axes), group_index(axes)
    sem = pltpu.get_barrier_semaphore()

    def one(k, carry):
        pl.semaphore_signal(
            sem, inc=1, device_id=coords_of(lax.rem(me + k, n), axes), device_id_type=MESH
        )
        return carry

    lax.fori_loop(1, n, one, 0)
    return n - 1


def greeted(count):
    pl.semaphore_wait(pltpu.get_barrier_semaphore(), count)


class Exchange:
    def __init__(self, axes, src, dst, send, recv, pick=None):
        self.axes, self.src, self.dst, self.send, self.recv = axes, src, dst, send, recv
        self.n, self.me = group_size(axes), group_index(axes)
        self.pick = pick

    def block(self, index):
        if self.pick is None:
            return self.src
        return self.src.at[self.pick(coords_of(index, self.axes), index)]

    def copy(self, k, slot):
        to = lax.rem(self.me + k, self.n)
        return pltpu.make_async_remote_copy(
            src_ref=self.block(to),
            dst_ref=self.dst.at[slot],
            send_sem=self.send.at[0],
            recv_sem=self.recv.at[0],
            device_id=coords_of(to, self.axes),
            device_id_type=MESH,
        )

    def start(self):
        def one(k, carry):
            self.copy(k, self.me).start()
            return carry

        lax.fori_loop(1, self.n, one, 0)
        self.dst[self.me] = self.block(self.me)[...]

    def others(self):
        return bulk(self.dst.at[pl.ds(0, self.n - 1)], self.send, self.recv)

    def arrive(self):
        self.others().wait_recv()

    def drain(self):
        self.others().wait_send()


def bulk(ref, send, recv):
    return pltpu.make_async_remote_copy(
        src_ref=ref,
        dst_ref=ref,
        send_sem=send.at[0],
        recv_sem=recv.at[0],
        device_id={"c": 1 - lax.axis_index("c")},
        device_id_type=MESH,
    )


class ToReaders:
    def __init__(self, src, dst, send, recv):
        self.src, self.dst, self.send, self.recv = src, dst, send, recv
        self.y, self.x, self.c = (lax.axis_index(a) for a in "yxc")
        self.mine = self.x // 2 == self.c

    def copy(self, k, slot):
        return pltpu.make_async_remote_copy(
            src_ref=self.src,
            dst_ref=self.dst.at[slot],
            send_sem=self.send.at[k],
            recv_sem=self.recv.at[slot],
            device_id={"x": lax.rem(self.x + k, 4), "c": self.x // 2},
            device_id_type=MESH,
        )

    def slot(self):
        return lax.rem(self.x, 2) * 2 + self.c

    def start(self):
        for k in range(1, 4):
            self.copy(k, self.slot()).start()

        @pl.when(jnp.logical_not(self.mine))
        def _():
            self.copy(0, self.slot()).start()

        @pl.when(self.mine)
        def _():
            self.dst[self.slot()] = self.src[...]

    def arrive(self):
        for s in range(4):
            own = jnp.logical_and(2 * self.c + s // 2 == self.x, self.c == s % 2)

            @pl.when(jnp.logical_not(own))
            def _():
                self.copy(1, s).wait_recv()

    def drain(self):
        for k in range(1, 4):
            self.copy(k, self.slot()).wait_send()

        @pl.when(jnp.logical_not(self.mine))
        def _():
            self.copy(0, self.slot()).wait_send()


class ToOwners:
    def __init__(self, src, dst, send, recv):
        self.src, self.dst, self.send, self.recv = src, dst, send, recv
        self.y, self.x, self.c = (lax.axis_index(a) for a in "yxc")

    def copy(self, s, slot):
        return pltpu.make_async_remote_copy(
            src_ref=self.src.at[s],
            dst_ref=self.dst.at[slot],
            send_sem=self.send.at[s],
            recv_sem=self.recv.at[slot],
            device_id={"x": 2 * self.c + s // 2, "c": jnp.int32(s % 2)},
            device_id_type=MESH,
        )

    def own(self, s):
        return jnp.logical_and(2 * self.c + s // 2 == self.x, self.c == s % 2)

    def start(self):
        for s in range(4):
            @pl.when(jnp.logical_not(self.own(s)))
            def _():
                self.copy(s, self.x).start()

            @pl.when(self.own(s))
            def _():
                self.dst[self.x] = self.src[s]

    def arrive(self):
        for j in range(4):
            own = jnp.logical_and(self.x == j, self.x // 2 == self.c)

            @pl.when(jnp.logical_not(own))
            def _():
                self.copy(0, j).wait_recv()

    def drain(self):
        for s in range(4):
            @pl.when(jnp.logical_not(self.own(s)))
            def _():
                self.copy(s, self.x).wait_send()


def lanes_below(shape, bound):
    return lax.broadcasted_iota(jnp.int32, shape, 1) < bound


def contract(a, b, da, db):
    return lax.dot_general(a, b, (((da,), (db,)), ((), ())), preferred_element_type=F32)


def ring_greet(nz):
    z = lax.axis_index("z")
    sem = pltpu.get_barrier_semaphore()
    right, left = lax.rem(z + 1, nz), lax.rem(z + nz - 1, nz)
    for to in (left, right):
        pl.semaphore_signal(sem, inc=1, device_id={"z": to}, device_id_type=MESH)
    return 2


class RingGather:
    def __init__(self, axis, piece, count, three, send, recv):
        self.axis, self.piece, self.count, self.send, self.recv = axis, piece, count, send, recv
        self.three = three
        self.me = lax.axis_index(axis)

    def at(self, offset):
        return lax.rem(self.me + offset + 4, 4)

    def copy(self, slot, p, sign, kind):
        ref = self.piece(slot, p)
        return pltpu.make_async_remote_copy(
            src_ref=ref,
            dst_ref=ref,
            send_sem=self.send.at[0],
            recv_sem=self.recv.at[kind, p],
            device_id={self.axis: self.at(sign)},
            device_id_type=MESH,
        )

    def start(self, p):
        self.copy(self.me, p, 1, 0).start()
        self.copy(self.me, p, -1, 1).start()

    def relay(self, p):
        self.copy(self.at(-1), p, 1, 0).wait_recv()
        self.copy(self.at(1), p, -1, 1).wait_recv()
        if p < self.count // 2:
            self.copy(self.at(-1), p, 1, 2).start()
        else:
            self.copy(self.at(1), p, -1, 2).start()

    def arrive(self, p):
        self.copy(self.at(2), p, 1, 2).wait_recv()

    def drain(self):
        bulk(self.three, self.send, self.send).wait_send()


class RowGather:
    def __init__(self, halves, out, send, recv):
        self.halves, self.out, self.send, self.recv = halves, out, send, recv
        self.y, self.c = lax.axis_index("y"), lax.axis_index("c")

    def at(self, offset):
        return lax.rem(self.y + offset + 4, 4)

    def first(self, sign, core, slot_y, slot_c):
        kind = 0 if sign > 0 else 1
        return pltpu.make_async_remote_copy(
            src_ref=self.halves.at[core],
            dst_ref=self.out.at[slot_y, slot_c],
            send_sem=self.send.at[kind, core],
            recv_sem=self.recv.at[kind, slot_c],
            device_id={"y": self.at(sign), "c": jnp.int32(core)},
            device_id_type=MESH,
        )

    def partner(self, slot_c):
        return pltpu.make_async_remote_copy(
            src_ref=self.halves.at[1 - self.c],
            dst_ref=self.out.at[self.y, slot_c],
            send_sem=self.send.at[4, 0],
            recv_sem=self.recv.at[4, 0],
            device_id={"c": 1 - self.c},
            device_id_type=MESH,
        )

    def second(self, sign, slot_y, slot_c):
        kind = 2 if sign > 0 else 3
        ref = self.out.at[slot_y, slot_c, pl.ds(0 if sign > 0 else 16, 16)]
        return pltpu.make_async_remote_copy(
            src_ref=ref,
            dst_ref=ref,
            send_sem=self.send.at[kind, slot_c],
            recv_sem=self.recv.at[kind, slot_c],
            device_id={"y": self.at(sign)},
            device_id_type=MESH,
        )

    def start(self):
        for core in range(2):
            self.first(1, core, self.y, self.c).start()
            self.first(-1, core, self.y, self.c).start()
        self.partner(self.c).start()
        self.out[self.y, self.c] = self.halves[self.c]

    def relay(self):
        for core in range(2):
            self.first(1, 0, self.at(-1), core).wait_recv()
            self.second(1, self.at(-1), core).start()
            self.first(-1, 0, self.at(1), core).wait_recv()
            self.second(-1, self.at(1), core).start()

    def arrive(self):
        self.partner(1 - self.c).wait_recv()
        for core in range(2):
            self.second(1, self.at(2), core).wait_recv()
            self.second(-1, self.at(2), core).wait_recv()

    def drain(self):
        self.partner(self.c).wait_send()
        for core in range(2):
            self.first(1, core, self.y, self.c).wait_send()
            self.first(-1, core, self.y, self.c).wait_send()
            self.second(1, self.y, core).wait_send()
            self.second(-1, self.y, core).wait_send()


class WeightColumn:
    def __init__(self, wk, wv, out, send, recv):
        self.parts, self.out, self.send, self.recv = (wk, wv), out, send, recv
        self.y, self.x = lax.axis_index("y"), lax.axis_index("x")

    def lanes(self, y):
        return pl.ds(pl.multiple_of(y * 128, 128), 128)

    def copy(self, k, i, slot_y):
        to = lax.rem(self.y + k, 4)
        return pltpu.make_async_remote_copy(
            src_ref=self.parts[i].at[:, self.lanes(to)],
            dst_ref=self.out.at[to, self.x, slot_y, :, pl.ds(128 * i, 128)],
            send_sem=self.send.at[0],
            recv_sem=self.recv.at[0],
            device_id={"y": to},
            device_id_type=MESH,
        )

    def start(self):
        for k in (2, 1, 3):
            for i in range(2):
                self.copy(k, i, self.y).start()
        for i in range(2):
            block = self.parts[i][:, self.lanes(self.y)]
            self.out[self.y, self.x, self.y, :, 128 * i : 128 * i + 128] = block

    def others(self):
        return bulk(self.out.at[0, 0, pl.ds(0, 3)], self.send, self.recv)

    def arrive(self):
        self.others().wait_recv()

    def drain(self):
        self.others().wait_send()


def unit_rows(matrix, gain):
    wide = matrix.astype(F32)
    factor = lax.rsqrt(jnp.mean(wide * wide, axis=-1, keepdims=True) + EPSILON)
    return wide * factor * gain


def swap_halves(a):
    return pltpu.roll(a, HD, 1)


class StrideGather:
    def __init__(self, nz, blocks, send, recv):
        self.nz, self.blocks, self.send, self.recv = nz, blocks, send, recv
        self.z = lax.axis_index("z")
        self.rows = blocks.shape[1] // PIECES
        self.far = nz // 2

    def at(self, offset):
        return lax.rem(self.z + offset + self.nz, self.nz)

    def pieces(self, sign, distance):
        if distance < self.far:
            return range(PIECES)
        half = PIECES // 2
        return range(half) if sign > 0 else range(half, PIECES)

    def copy(self, sign, distance, d, p):
        ref = self.blocks.at[self.at(-sign * distance), pl.ds(p * self.rows, self.rows)]
        return pltpu.make_async_remote_copy(
            src_ref=ref,
            dst_ref=ref,
            send_sem=self.send.at[0],
            recv_sem=self.recv.at[0 if sign > 0 else 1, distance + d - 1, p],
            device_id={"z": self.at(sign * d)},
            device_id_type=MESH,
        )

    def arrived(self, sign, distance, p):
        ref = self.blocks.at[self.at(-sign * distance), pl.ds(p * self.rows, self.rows)]
        return pltpu.make_async_remote_copy(
            src_ref=ref,
            dst_ref=ref,
            send_sem=self.send.at[0],
            recv_sem=self.recv.at[0 if sign > 0 else 1, distance - 1, p],
            device_id={"z": self.at(sign)},
            device_id_type=MESH,
        )

    def start(self):
        for d in (2, 1):
            for p in range(PIECES):
                for sign in (1, -1):
                    self.copy(sign, 0, d, p).start()

    def relay(self, distance):
        for p in range(PIECES):
            for sign in (1, -1):
                self.arrived(sign, distance, p).wait_recv()
                if p in self.pieces(sign, distance + 2):
                    self.copy(sign, distance, 2, p).start()
        for p in range(PIECES):
            for sign in (1, -1):
                self.copy(sign, distance, 1, p).start()

    def arrive(self, distance):
        for sign in (1, -1):
            for p in self.pieces(sign, distance):
                self.arrived(sign, distance, p).wait_recv()

    def drain(self):
        bulk(self.blocks.at[pl.ds(0, self.nz - 1)], self.send, self.send).wait_send()


class StrideSum:
    def __init__(self, nz, term, out, arrived, send, recv):
        self.nz, self.term, self.out, self.arrived = nz, term, out, arrived
        self.send, self.recv = send, recv
        self.rows = out.shape[2] // PIECES
        self.z = lax.axis_index("z")

    def pieces(self, side, j):
        half = PIECES // 2
        return range(PIECES) if j else range(side * half, side * half + half)

    def hop(self, side, j, p):
        at = pl.ds(p * self.rows, self.rows)
        d = (1 if j % 2 else 2) * (1 if side else -1)
        return pltpu.make_async_remote_copy(
            src_ref=self.out.at[side, j, at],
            dst_ref=self.arrived.at[side, j, at],
            send_sem=self.send.at[side if j else 2 + side],
            recv_sem=self.recv.at[side, j, p],
            device_id={"z": lax.rem(self.z + d + self.nz, self.nz)},
            device_id_type=MESH,
        )

    def joined(self, side, j, p, value):
        at = pl.ds(p * self.rows, self.rows)
        for i in (j - 1, j - 2):
            if i >= 0 and p in self.pieces(side, i):
                self.hop(side, i, p).wait_recv()
                value = value + self.arrived[side, i, at].astype(F32)
        return value

    def step(self, j):
        for p in range(PIECES):
            for side in range(2):
                if p in self.pieces(side, j):
                    at = pl.ds(p * self.rows, self.rows)
                    value = self.term(side, j, at)
                    if j % 2 == 0:
                        value = self.joined(side, j, p, value)
                    self.out[side, j, at] = value.astype(BF16)
                    self.hop(side, j, p).start()

    def total(self, p):
        half = self.nz // 2
        value = self.term(0, half, pl.ds(p * self.rows, self.rows))
        return self.joined(1, half, p, self.joined(0, half, p, value))

    def drain(self):
        half = self.nz // 2
        for side in range(2):
            sem = self.send.at[pl.ds(side, 1)]
            bulk(self.out.at[side, pl.ds(0, half - 1)], sem, sem).wait_send()
            sem = self.send.at[pl.ds(2 + side, 1)]
            bulk(self.out.at[side, 0, pl.ds(0, self.rows * (PIECES // 2))], sem, sem).wait_send()


class FarGather:
    def __init__(self, nz, src, dst, send, recv):
        self.nz, self.src, self.dst, self.send, self.recv = nz, src, dst, send, recv
        self.z = lax.axis_index("z")
        self.far = {1: nz // 2 - REACH, -1: nz - 1 - nz // 2 - REACH}

    def at(self, offset):
        return lax.rem(self.z + offset + self.nz, self.nz)

    def copy(self, slot, sign, d, relay):
        kind = 3 if relay else 2 if d < REACH else 0 if sign > 0 else 1
        return pltpu.make_async_remote_copy(
            src_ref=self.dst.at[slot] if relay else self.src,
            dst_ref=self.dst.at[slot],
            send_sem=self.send.at[0],
            recv_sem=self.recv.at[kind],
            device_id={"z": self.at(sign * d)},
            device_id_type=MESH,
        )

    def several(self, count, kind):
        return bulk(self.dst.at[pl.ds(0, count)], self.send, self.recv.at[pl.ds(kind, 1)])

    def start(self):
        for d in range(REACH, 0, -1):
            for sign in (1, -1):
                self.copy(self.z, sign, d, False).start()
        self.dst[self.z] = self.src[...]

    def relay(self):
        for sign in (1, -1):
            slot = self.at(-sign * REACH)
            self.copy(slot, sign, REACH, False).wait_recv()
            for d in range(self.far[sign], 0, -1):
                self.copy(slot, sign, d, True).start()

    def arrive(self):
        self.several(2 * REACH - 2, 2).wait_recv()
        self.several(self.nz - 1 - 2 * REACH, 3).wait_recv()

    def drain(self):
        self.several(self.nz - 1, 0).wait_send()


def reach_greet(nz):
    z = lax.axis_index("z")
    for d in range(1, REACH + 1):
        for sign in (1, -1):
            pl.semaphore_signal(
                pltpu.get_barrier_semaphore(),
                inc=1,
                device_id={"z": lax.rem(z + sign * d + nz, nz)},
                device_id_type=MESH,
            )
    return 2 * REACH


def sems(*shape):
    return pltpu.SemaphoreType.DMA(shape)


def norm_back(matrix, gain, upstream):
    wide = matrix.astype(F32)
    factor = lax.rsqrt(jnp.mean(wide * wide, axis=-1, keepdims=True) + EPSILON)
    weighted = upstream * gain
    inner = jnp.mean(weighted * wide, axis=-1, keepdims=True)
    return factor * weighted - wide * factor**3 * inner


def kernel(
    nz, target_rows_h, source_rows_h, t_gain_h, s_gain_h, wq_h, wk_h, wv_h, wo_h, cot_h, pick_h, pick8_h,
    s_out, t_out, all_sums,
    target_rows, source_rows, t_gain, s_gain, wk, wv, cot, pick, pick8, loads,
    pair, kv_all, stats, out, qa, t_all, pair_all, w_all,
    halves, rows_all, part, part_all, block, blocks, m, l, o, said, heard,
    dq, mine, ring_out, ring_in, w_ring_out, w_ring_in, outs, dq_block, dqs, o_part, swapped,
    mine_sum, kv_grad, grads8, parts, d_parts, s_in, t_in,
    row_s, row_r, wy_s, wy_r, wx_s, wx_r, wf_s, wf_r, ya_s, ya_r, xb_s, xb_r, xa_s, xa_r, yb_s, yb_r, pair_s, pair_r,
    part_s, part_r, q_s, q_r, z_s, z_r, ss, sr,
    o_s, o_r, dq_s, dq_r, sw_s, sw_r, g_s, g_r, h_s, h_r, back_s, back_r,
    kv_s, kv_r, s_s, s_r, t_s, t_r,
):
    z, y, x, c = (lax.axis_index(a) for a in "zyxc")
    met = greet(("y", "x", "c")) + reach_greet(nz)

    staged = (
        (source_rows_h, source_rows), (s_gain_h, s_gain), (wk_h, wk), (wv_h, wv),
        (target_rows_h, target_rows), (t_gain_h, t_gain), (cot_h, cot),
        (wq_h, pair.at[pl.ds(0, HD)]), (wo_h, pair.at[pl.ds(HD, HD)]), (pick_h, pick), (pick8_h, pick8),
    )
    copies = [pltpu.make_async_copy(a, b, loads.at[i]) for i, (a, b) in enumerate(staged)]
    for copy in copies:
        copy.start()
    for copy in copies[:2]:
        copy.wait()
    normed = unit_rows(source_rows[...], s_gain[...])
    low = lanes_below((32, 128), HD)
    for j in range(8):
        chip = (2 * j % 4) * 4 + j // 2
        first, second = (normed[:, 128 * i : 128 * i + 128] for i in (chip, chip + 4))
        halves[0, :, 128 * j : 128 * j + 128] = jnp.where(low, first, swap_halves(second)).astype(BF16)
        halves[1, :, 128 * j : 128 * j + 128] = jnp.where(low, swap_halves(first), second).astype(BF16)
    for copy in copies[2:]:
        copy.wait()
    greeted(met)

    by_rows = RowGather(halves, rows_all, row_s, row_r)
    by_wy = WeightColumn(wk, wv, w_all, wy_s, wy_r)
    by_wx = RingGather(
        "x", lambda slot, p: w_all.at[y, slot, p], 4, w_all.at[y, pl.ds(0, 3)], wx_s, wx_r
    )
    by_wf = RingGather("y", lambda slot, p: w_all.at[slot, p], 4, w_all.at[pl.ds(0, 3)], wf_s, wf_r)
    three, first, second = pl.ds(0, 3), pl.ds(0, 1024), pl.ds(1024, 1024)
    by_ya = RingGather(
        "y", lambda slot, p: t_all.at[x, slot, :, pl.ds(512 * p, 512)], 2,
        t_all.at[x, three, :, first], ya_s, ya_r,
    )
    by_xb = RingGather(
        "x", lambda slot, p: t_all.at[slot, y, :, pl.ds(1024 + 512 * p, 512)], 2,
        t_all.at[three, y, :, second], xb_s, xb_r,
    )
    by_xa = RingGather(
        "x", lambda slot, p: t_all.at[slot, p, :, first], 4, t_all.at[three, :, :, first], xa_s, xa_r
    )
    by_yb = RingGather(
        "y", lambda slot, p: t_all.at[p, slot, :, second], 4, t_all.at[:, three, :, second], yb_s, yb_r
    )
    by_pair = Exchange(("c",), pair, pair_all, pair_s, pair_r)
    by_wy.start()
    by_rows.start()
    zero = jnp.zeros((2, target_rows.shape[1]), F32)
    t_all[x, y] = jnp.concatenate(
        [unit_rows(target_rows[...], t_gain[...]), zero, cot[...].astype(F32), zero], axis=0
    ).astype(BF16)
    for p in range(2):
        by_xb.start(p)
        by_ya.start(p)
    by_pair.start()

    by_wy.arrive()
    for p in range(4):
        by_wx.start(p)
    by_rows.relay()
    for p in range(4):
        by_wx.relay(p)
    for p in range(2):
        by_xb.relay(p)
        by_ya.relay(p)
    for p in range(2):
        by_xb.arrive(p)
        by_ya.arrive(p)
    for p in range(4):
        by_xa.start(p)
        by_yb.start(p)
    by_rows.arrive()
    for p in range(4):
        by_wx.arrive(p)

    rows = rows_all[...].reshape(256, 1024)
    kv2 = jnp.dot(rows, w_all[y].reshape(1024, 256), preferred_element_type=F32)
    k2, v2 = kv2[:, :128], kv2[:, 128:]
    wide_low = lanes_below((256, 128), HD)
    part[0] = jnp.where(wide_low, k2, swap_halves(v2))
    part[1] = jnp.where(wide_low, swap_halves(k2), v2)
    by_part = Exchange(("c",), part, part_all, part_s, part_r, lambda at, i: i)
    by_part.start()
    by_part.arrive()
    kv_all[z] = (part_all[0] + part_all[1]).astype(BF16)

    by_z = StrideGather(nz, kv_all, z_s, z_r)
    by_z.start()
    for p in range(4):
        by_xa.relay(p)
        by_yb.relay(p)
    for p in range(4):
        by_wf.start(p)
    by_z.relay(2)
    by_pair.arrive()
    for p in range(4):
        by_xa.arrive(p)
        by_yb.arrive(p)
    everything = t_all[...].reshape(256, 2048)
    wide = lax.broadcasted_iota(jnp.int32, (256, 256), 1)
    scale = jnp.where(lax.rem(wide, 128) < HD, HD**-0.5, 1.0)
    projected = contract(everything, pair_all[...].reshape(256, 2048), 1, 1) * scale
    chosen = jnp.dot(pick[...], projected.astype(BF16), preferred_element_type=F32)
    narrow = lanes_below((96, 128), HD)
    for a in range(2):
        at = slice(128 * a, 128 * a + 128)
        block[96 * a : 96 * a + 96] = jnp.where(narrow, chosen[:96, at], chosen[96:, at]).astype(BF16)
    by_q = ToReaders(block, blocks, q_s, q_r)
    by_q.start()
    by_z.relay(4)
    m[...] = jnp.full(m.shape, -1e30, F32)
    l[...] = jnp.zeros(l.shape, F32)
    o[...] = jnp.zeros(o.shape, F32)
    by_q.arrive()
    qa[...] = blocks[...].reshape(qa.shape)

    def blocks_of(planes):
        return jnp.concatenate([kv_all[at] for at in planes], axis=0)

    def attend(*planes):
        block = blocks_of(planes)
        keys = jnp.where(lanes_below(block.shape, HD), block, jnp.zeros_like(block))
        scores = contract(keys, qa[...], 1, 1)
        top = jnp.maximum(m[...], jnp.max(scores, axis=0, keepdims=True))
        weights = jnp.exp(scores - top)
        old = jnp.exp(m[...] - top)
        m[...] = top
        l[...] = l[...] * old + jnp.sum(weights, axis=0, keepdims=True)
        o[...] = o[...] * old + contract(block, weights.astype(BF16), 0, 0)[HD:]

    def attend_from(low, high):
        def one(d, carry):
            attend(lax.rem(z + d, nz), lax.rem(z + nz - d, nz))
            return carry

        lax.fori_loop(low, high + 1, one, 0)

    attend(z)
    by_z.arrive(1)
    attend_from(1, 2)
    by_z.relay(6)
    by_z.arrive(3)
    by_z.arrive(5)
    attend_from(3, 6)
    by_z.arrive(7)
    by_z.arrive(8)
    attend_from(7, 7)
    attend(lax.rem(z + nz // 2, nz))
    upright = jnp.transpose(qa[...].astype(F32))
    delta = jnp.sum(upright[HD:] * o[...], axis=0, keepdims=True)
    row = lax.broadcasted_iota(jnp.int32, (8, qa.shape[0]), 0)
    said[...] = jnp.where(row == 0, m[...], jnp.where(row == 1, l[...], delta))
    by_stats = Exchange(("x",), said, heard, ss, sr)
    by_stats.start()
    log_sum = m[...] + jnp.log(l[...])
    high = log_sum.astype(BF16)
    rest = log_sum - high.astype(F32)
    middle = rest.astype(BF16)
    low_part = rest - middle.astype(F32)
    line = lax.broadcasted_iota(jnp.int32, (HD, qa.shape[0]), 0)
    parts3 = jnp.where(line == 0, high.astype(F32), jnp.where(line == 1, middle.astype(F32), low_part))
    upright = jnp.concatenate([o[...] / l[...], jnp.where(line < 3, parts3, 0.0)], axis=0)
    out[...] = jnp.transpose(upright).astype(BF16).reshape(out.shape)
    by_o = ToOwners(out, outs, o_s, o_r)
    by_o.start()
    for p in range(4):
        by_wf.relay(p)
    by_stats.arrive()
    top = jnp.max(heard[:, 0:1], axis=0)
    total = jnp.zeros_like(top)
    both = jnp.zeros_like(top)
    for j in range(4):
        w = jnp.exp(heard[j, 0:1] - top)
        total = total + w * heard[j, 1:2]
        both = both + w * heard[j, 2:3]
    stats[...] = jnp.where(row == 0, top + jnp.log(total), both / total)
    dq[...] = jnp.zeros(dq.shape, F32)

    def plane_of(side, j):
        offset = nz // 2 - j if side else j - nz // 2
        return lax.rem(z + nz + offset, nz)

    def grads(*terms):
        block = blocks_of([plane_of(side, j) for side, j in terms])
        low = lanes_below(block.shape, HD)
        none = jnp.zeros_like(block)
        scores = contract(jnp.where(low, block, none), qa[...], 1, 1)
        probs = jnp.exp(scores - stats[0:1])
        d_probs = contract(jnp.where(low, none, block), qa[...], 1, 1)
        d_scores = (probs * (d_probs - stats[1:2])).astype(BF16)
        for_v = contract(probs.astype(BF16), qa[...], 1, 0)
        for_k = contract(d_scores, qa[...], 1, 0)
        dq[...] += contract(block, d_scores, 0, 0)[:HD]
        both = jnp.where(low, for_k, for_v)
        for i, (side, j) in enumerate(terms):
            mine[j, side] = both[256 * i : 256 * i + 256]

    def both_grads(low, high):
        def one(j, carry):
            grads((0, j), (1, j))
            return carry

        lax.fori_loop(low, high + 1, one, 0)

    main = StrideSum(
        nz, lambda side, j, at: mine[j, side if j else 0, at], ring_out, ring_in, g_s, g_r
    )

    def own_weight(side, j, at):
        to = plane_of(side, j)
        return swapped[0, to, at].astype(F32) + swapped[1, to, at].astype(F32)

    weight = StrideSum(nz, own_weight, w_ring_out, w_ring_in, h_s, h_r)

    grads((0, 0))
    main.step(0)
    by_o.arrive()
    lanes = lax.broadcasted_iota(jnp.int32, (192, 128), 1)
    given = [outs[i].astype(F32) for i in range(4)]
    log_sums = [
        jnp.sum(jnp.where(jnp.logical_and(lanes >= HD, lanes < HD + 3), g, 0.0), axis=1, keepdims=True)
        for g in given
    ]
    largest = functools.reduce(jnp.maximum, log_sums)
    shares = [jnp.exp(part_sum - largest) for part_sum in log_sums]
    whole_sum = sum(g * w for g, w in zip(given, shares)) / sum(shares)
    attended = jnp.where(lanes < HD, whole_sum, 0.0).astype(BF16)
    for a in range(2):
        spread = contract(pick[96:], attended[96 * a : 96 * a + 96], 0, 0).astype(BF16)
        product = contract(spread, t_all[...].reshape(256, 2048), 0, 0)[:HD].astype(BF16)
        for i in range(nz):
            o_part[a, i] = product[:, 128 * i : 128 * i + 128]
    swap = Exchange(("c",), o_part, swapped, sw_s, sw_r, lambda at, i: i)
    swap.start()
    both_grads(1, 1)
    main.step(1)
    swap.arrive()
    weight.step(0)
    weight.step(1)
    both_grads(2, 3)
    weight.step(2)
    main.step(2)
    weight.step(3)
    main.step(3)
    both_grads(4, 7)
    grads((0, nz // 2))
    upright = jnp.concatenate([dq[...], jnp.zeros_like(dq[...])], axis=0) * HD**-0.5
    straight = jnp.transpose(upright)
    for i in range(4):
        first_head, second_head = (straight[192 * i + 96 * a : 192 * i + 96 * a + 96] for a in range(2))
        dq_block[i] = (first_head + swap_halves(second_head)).astype(BF16)
    by_dq = ToOwners(dq_block, dqs, dq_s, dq_r)
    by_dq.start()
    weight.step(4)
    main.step(4)
    weight.step(5)
    main.step(5)
    by_dq.arrive()
    query_grad = jnp.sum(dqs[...].astype(F32), axis=0).astype(BF16)
    spread = contract(pick8[...], query_grad, 0, 0).astype(BF16)
    heads = jnp.concatenate([pair_all[a, :HD] for a in range(2)], axis=0)
    d_target = jnp.dot(spread, heads, preferred_element_type=F32)
    d_parts[...] = d_target.astype(BF16).reshape(16, 8, 2048)
    by_t = Exchange(("x", "y"), d_parts, t_in, t_s, t_r, lambda at, i: i)
    by_t.start()
    weight.step(6)
    weight.step(7)
    main.step(6)
    main.step(7)
    for p in range(PIECES):
        mine_sum[pl.ds(32 * p, 32)] = weight.total(p).astype(BF16)
    back = FarGather(nz, mine_sum, all_sums, back_s, back_r)
    back.start()
    for p in range(4):
        by_wf.arrive(p)
    for p in range(PIECES):
        kv_grad[2 * p : 2 * p + 2] = main.total(p).astype(BF16).reshape(2, 64, 128)
    by_kv = Exchange(("y", "c"), kv_grad, grads8, kv_s, kv_r, lambda at, i: at["y"])
    by_kv.start()
    back.relay()
    by_kv.arrive()
    narrow = lanes_below((64, 128), HD)
    d_rows = jnp.zeros((64, 1024), F32)
    for i in range(4):
        g0, g1 = grads8[2 * i].astype(F32), grads8[2 * i + 1].astype(F32)
        k2 = jnp.where(narrow, g0, swap_halves(g1)).astype(BF16)
        v2 = jnp.where(narrow, swap_halves(g0), g1).astype(BF16)
        kv2 = jnp.concatenate([k2, v2], axis=1)
        d_rows = d_rows + contract(kv2, w_all[i].reshape(1024, 256), 1, 1)
    parts[...] = d_rows.astype(BF16).reshape(2, 32, 1024)
    by_s = Exchange(("c",), parts, s_in, s_s, s_r, lambda at, i: i)
    by_s.start()
    by_t.arrive()
    t_out[...] = jnp.sum(t_in[...].astype(F32), axis=0)
    by_s.arrive()
    got = [s_in[core].astype(F32) for core in range(2)]
    for j in range(8):
        chip = (2 * j % 4) * 4 + j // 2
        a, b = (g[:, 128 * j : 128 * j + 128] for g in got)
        s_out[:, 128 * chip : 128 * chip + 128] = jnp.where(low, a, swap_halves(b))
        s_out[:, 128 * chip + 512 : 128 * chip + 640] = jnp.where(low, swap_halves(a), b)
    back.arrive()
    for by in (by_rows, by_wy, by_wx, by_wf, by_ya, by_xb, by_xa, by_yb, by_pair, by_part, by_q, by_z, by_stats):
        by.drain()
    for by in (by_o, by_dq, swap, back, by_kv, by_s, by_t, main, weight):
        by.drain()


def whole(args, nz):
    t = 768
    half = nz // 2

    def bf16(*shape):
        return pltpu.VMEM(shape, BF16)

    def f32(*shape):
        return pltpu.VMEM(shape, F32)

    return pl.pallas_call(
        functools.partial(kernel, nz),
        out_shape=(
            jax.ShapeDtypeStruct((32, 2048), F32),
            jax.ShapeDtypeStruct((8, 2048), F32),
            jax.ShapeDtypeStruct((nz, HD, 128), BF16),
        ),
        in_specs=[pl.BlockSpec(memory_space=pl.ANY)] * len(args),
        out_specs=(VMEM,) * 3,
        scratch_shapes=[
            bf16(6, 2048), bf16(32, 2048), f32(1, 2048), f32(1, 2048), bf16(64, 512), bf16(64, 512),
            bf16(6, 2048), bf16(192, 256), bf16(96, 128), dma(len(args)),
            bf16(128, 2048), bf16(nz, 256, 128), f32(8, t), bf16(4, 192, 128), bf16(t, 128),
            bf16(4, 4, 16, 2048), bf16(2, 128, 2048), bf16(4, 4, 4, 64, 256),
            bf16(2, 32, 1024), bf16(4, 2, 32, 1024), f32(2, 256, 128), f32(2, 256, 128),
            bf16(192, 128), bf16(4, 192, 128), f32(1, t), f32(1, t), f32(HD, t), f32(8, t), f32(4, 8, t),
            f32(HD, t), f32(half + 1, 2, 256, 128), bf16(2, half, 256, 128), bf16(2, half, 256, 128),
            bf16(2, half, HD, 128), bf16(2, half, HD, 128),
            bf16(4, 192, 128), bf16(4, 96, 128), bf16(4, 96, 128),
            bf16(2, nz, HD, 128), bf16(2, nz, HD, 128), bf16(HD, 128), bf16(4, 64, 128), bf16(8, 64, 128), bf16(2, 32, 1024), bf16(16, 8, 2048),
            bf16(2, 32, 1024), bf16(16, 8, 2048),
            sems(5, 2), sems(5, 2), dma(1), dma(1), dma(1), sems(3, 4), dma(1), sems(3, 4),
            dma(1), sems(3, 2), dma(1), sems(3, 2), dma(1), sems(3, 4), dma(1), sems(3, 4), dma(1), dma(1),
            dma(1), dma(1), dma(4), dma(4), dma(1), sems(2, half, PIECES), dma(1), dma(1),
            dma(4), dma(4), dma(4), dma(4), dma(1), dma(1),
            dma(4), sems(2, half, PIECES), dma(4), sems(2, half, PIECES),
            dma(1), dma(4), dma(1), dma(1), dma(1), dma(1), dma(1), dma(1),
        ],
        compiler_params=params(0),
    )(*args)


def finish_kernel(
    d_source, d_target, sums, target_rows, source_rows, t_gain, s_gain, cot, t_out, s_out, w_out
):
    t_out[...] = cot[...].astype(F32) + norm_back(target_rows[...], t_gain[...], d_target[:6])
    s_out[...] = norm_back(source_rows[...], s_gain[...], d_source[...])
    for i in range(sums.shape[0]):
        w_out[:, 128 * i : 128 * i + 128] = sums[i].astype(F32)


def finish(*args):
    return pl.pallas_call(
        finish_kernel,
        out_shape=(
            jax.ShapeDtypeStruct((6, 2048), F32),
            jax.ShapeDtypeStruct((32, 2048), F32),
            jax.ShapeDtypeStruct((64, 2048), F32),
        ),
        in_specs=[VMEM] * len(args),
        out_specs=(VMEM,) * 3,
    )(*args)


def picks():
    r = np.arange(96)
    at = 16 * (r // 6) + r % 6
    pick = np.concatenate([at, at + 8])[:, None] == np.arange(256)[None]
    pick8 = (8 * (r // 6) + r % 6)[:, None] == np.arange(128)[None]
    return jnp.asarray(pick.astype(BF16)), jnp.asarray(pick8.astype(BF16))


def body(nz, target_rows, source_rows, t_gain, s_gain, wq, wk, wv, wo, cot):
    gains = (t_gain[None], s_gain[None])
    d_source, d_target, sums = whole(
        (target_rows, source_rows, *gains, wq.T, wk, wv, wo, cot, *picks()), nz
    )
    return finish(d_source, d_target, sums, target_rows, source_rows, *gains, cot)


def solution(mesh):
    nz = mesh.shape["sp"]
    SIZES["z"] = nz
    fine = Mesh(mesh.devices.reshape(nz, 4, 4, 2), ("z", "y", "x", "c"))
    every, plane = ("z", "y", "x", "c"), ("y", "x", "c")
    return jax.shard_map(
        functools.partial(body, nz),
        mesh=fine,
        in_specs=(
            P(every, None), P(every, None), P(), P(),
            P(None, plane), P(plane, None), P(plane, None), P(plane, None), P(every, None),
        ),
        out_specs=(P(every, None), P(every, None), P(plane, None)),
        check_vma=False,
    )
```

```python
import functools

import jax
import jax.numpy as jnp
import numpy as np
from jax import lax
from jax.experimental import pallas as pl
from jax.experimental.pallas import tpu as pltpu
from jax.sharding import Mesh
from jax.sharding import PartitionSpec as P

MESH = pl.DeviceIdType.MESH
HD = 64
EPSILON = 1e-06
F32, BF16 = jnp.float32, jnp.bfloat16
VMEM = pl.BlockSpec(memory_space=pltpu.VMEM)
SIZES = {"y": 4, "x": 4, "c": 2}
PIECES = 2
REACH = 4


def dma(n):
    return pltpu.SemaphoreType.DMA((n,))


def params(cid):
    return pltpu.CompilerParams(
        collective_id=cid, has_side_effects=True, vmem_limit_bytes=62 * 1024 * 1024
    )


def group_size(axes):
    n = 1
    for a in axes:
        n *= SIZES[a]
    return n


def group_index(axes):
    i = 0
    for a in axes:
        i = i * SIZES[a] + lax.axis_index(a)
    return i


def coords_of(index, axes):
    out = {}
    for a in reversed(axes):
        out[a] = lax.rem(index, SIZES[a])
        index = index // SIZES[a]
    return out


def greet(axes):
    n, me = group_size(axes), group_index(axes)
    sem = pltpu.get_barrier_semaphore()

    def one(k, carry):
        pl.semaphore_signal(
            sem, inc=1, device_id=coords_of(lax.rem(me + k, n), axes), device_id_type=MESH
        )
        return carry

    lax.fori_loop(1, n, one, 0)
    return n - 1


def greeted(count):
    pl.semaphore_wait(pltpu.get_barrier_semaphore(), count)


class Exchange:
    def __init__(self, axes, src, dst, send, recv, pick=None):
        self.axes, self.src, self.dst, self.send, self.recv = axes, src, dst, send, recv
        self.n, self.me = group_size(axes), group_index(axes)
        self.pick = pick

    def block(self, index):
        if self.pick is None:
            return self.src
        return self.src.at[self.pick(coords_of(index, self.axes), index)]

    def copy(self, k, slot):
        to = lax.rem(self.me + k, self.n)
        return pltpu.make_async_remote_copy(
            src_ref=self.block(to),
            dst_ref=self.dst.at[slot],
            send_sem=self.send.at[0],
            recv_sem=self.recv.at[0],
            device_id=coords_of(to, self.axes),
            device_id_type=MESH,
        )

    def start(self):
        def one(k, carry):
            self.copy(k, self.me).start()
            return carry

        lax.fori_loop(1, self.n, one, 0)
        self.dst[self.me] = self.block(self.me)[...]

    def others(self):
        return bulk(self.dst.at[pl.ds(0, self.n - 1)], self.send, self.recv)

    def arrive(self):
        self.others().wait_recv()

    def drain(self):
        self.others().wait_send()


def bulk(ref, send, recv):
    return pltpu.make_async_remote_copy(
        src_ref=ref,
        dst_ref=ref,
        send_sem=send.at[0],
        recv_sem=recv.at[0],
        device_id={"c": 1 - lax.axis_index("c")},
        device_id_type=MESH,
    )


class ToReaders:
    def __init__(self, src, dst, send, recv):
        self.src, self.dst, self.send, self.recv = src, dst, send, recv
        self.y, self.x, self.c = (lax.axis_index(a) for a in "yxc")
        self.mine = self.x // 2 == self.c

    def copy(self, k, slot):
        return pltpu.make_async_remote_copy(
            src_ref=self.src,
            dst_ref=self.dst.at[slot],
            send_sem=self.send.at[k],
            recv_sem=self.recv.at[slot],
            device_id={"x": lax.rem(self.x + k, 4), "c": self.x // 2},
            device_id_type=MESH,
        )

    def slot(self):
        return lax.rem(self.x, 2) * 2 + self.c

    def start(self):
        for k in range(1, 4):
            self.copy(k, self.slot()).start()

        @pl.when(jnp.logical_not(self.mine))
        def _():
            self.copy(0, self.slot()).start()

        @pl.when(self.mine)
        def _():
            self.dst[self.slot()] = self.src[...]

    def arrive(self):
        for s in range(4):
            own = jnp.logical_and(2 * self.c + s // 2 == self.x, self.c == s % 2)

            @pl.when(jnp.logical_not(own))
            def _():
                self.copy(1, s).wait_recv()

    def drain(self):
        for k in range(1, 4):
            self.copy(k, self.slot()).wait_send()

        @pl.when(jnp.logical_not(self.mine))
        def _():
            self.copy(0, self.slot()).wait_send()


class ToOwners:
    def __init__(self, src, dst, send, recv):
        self.src, self.dst, self.send, self.recv = src, dst, send, recv
        self.y, self.x, self.c = (lax.axis_index(a) for a in "yxc")

    def copy(self, s, slot):
        return pltpu.make_async_remote_copy(
            src_ref=self.src.at[s],
            dst_ref=self.dst.at[slot],
            send_sem=self.send.at[s],
            recv_sem=self.recv.at[slot],
            device_id={"x": 2 * self.c + s // 2, "c": jnp.int32(s % 2)},
            device_id_type=MESH,
        )

    def own(self, s):
        return jnp.logical_and(2 * self.c + s // 2 == self.x, self.c == s % 2)

    def start(self):
        for s in range(4):
            @pl.when(jnp.logical_not(self.own(s)))
            def _():
                self.copy(s, self.x).start()

            @pl.when(self.own(s))
            def _():
                self.dst[self.x] = self.src[s]

    def arrive(self):
        for j in range(4):
            own = jnp.logical_and(self.x == j, self.x // 2 == self.c)

            @pl.when(jnp.logical_not(own))
            def _():
                self.copy(0, j).wait_recv()

    def drain(self):
        for s in range(4):
            @pl.when(jnp.logical_not(self.own(s)))
            def _():
                self.copy(s, self.x).wait_send()


def lanes_below(shape, bound):
    return lax.broadcasted_iota(jnp.int32, shape, 1) < bound


def contract(a, b, da, db):
    return lax.dot_general(a, b, (((da,), (db,)), ((), ())), preferred_element_type=F32)


def ring_greet(nz):
    z = lax.axis_index("z")
    sem = pltpu.get_barrier_semaphore()
    right, left = lax.rem(z + 1, nz), lax.rem(z + nz - 1, nz)
    for to in (left, right):
        pl.semaphore_signal(sem, inc=1, device_id={"z": to}, device_id_type=MESH)
    return 2


class RingGather:
    def __init__(self, axis, piece, count, three, send, recv):
        self.axis, self.piece, self.count, self.send, self.recv = axis, piece, count, send, recv
        self.three = three
        self.me = lax.axis_index(axis)

    def at(self, offset):
        return lax.rem(self.me + offset + 4, 4)

    def copy(self, slot, p, sign, kind):
        ref = self.piece(slot, p)
        return pltpu.make_async_remote_copy(
            src_ref=ref,
            dst_ref=ref,
            send_sem=self.send.at[0],
            recv_sem=self.recv.at[kind, p],
            device_id={self.axis: self.at(sign)},
            device_id_type=MESH,
        )

    def start(self, p):
        self.copy(self.me, p, 1, 0).start()
        self.copy(self.me, p, -1, 1).start()

    def relay(self, p):
        self.copy(self.at(-1), p, 1, 0).wait_recv()
        self.copy(self.at(1), p, -1, 1).wait_recv()
        if p < self.count // 2:
            self.copy(self.at(-1), p, 1, 2).start()
        else:
            self.copy(self.at(1), p, -1, 2).start()

    def arrive(self, p):
        self.copy(self.at(2), p, 1, 2).wait_recv()

    def drain(self):
        bulk(self.three, self.send, self.send).wait_send()


class RowGather:
    def __init__(self, halves, out, send, recv):
        self.halves, self.out, self.send, self.recv = halves, out, send, recv
        self.y, self.c = lax.axis_index("y"), lax.axis_index("c")

    def at(self, offset):
        return lax.rem(self.y + offset + 4, 4)

    def first(self, sign, core, slot_y, slot_c):
        kind = 0 if sign > 0 else 1
        return pltpu.make_async_remote_copy(
            src_ref=self.halves.at[core],
            dst_ref=self.out.at[slot_y, slot_c],
            send_sem=self.send.at[kind, core],
            recv_sem=self.recv.at[kind, slot_c],
            device_id={"y": self.at(sign), "c": jnp.int32(core)},
            device_id_type=MESH,
        )

    def partner(self, slot_c):
        return pltpu.make_async_remote_copy(
            src_ref=self.halves.at[1 - self.c],
            dst_ref=self.out.at[self.y, slot_c],
            send_sem=self.send.at[4, 0],
            recv_sem=self.recv.at[4, 0],
            device_id={"c": 1 - self.c},
            device_id_type=MESH,
        )

    def second(self, sign, slot_y, slot_c):
        kind = 2 if sign > 0 else 3
        ref = self.out.at[slot_y, slot_c, pl.ds(0 if sign > 0 else 16, 16)]
        return pltpu.make_async_remote_copy(
            src_ref=ref,
            dst_ref=ref,
            send_sem=self.send.at[kind, slot_c],
            recv_sem=self.recv.at[kind, slot_c],
            device_id={"y": self.at(sign)},
            device_id_type=MESH,
        )

    def start(self):
        for core in range(2):
            self.first(1, core, self.y, self.c).start()
            self.first(-1, core, self.y, self.c).start()
        self.partner(self.c).start()
        self.out[self.y, self.c] = self.halves[self.c]

    def relay(self):
        for core in range(2):
            self.first(1, 0, self.at(-1), core).wait_recv()
            self.second(1, self.at(-1), core).start()
            self.first(-1, 0, self.at(1), core).wait_recv()
            self.second(-1, self.at(1), core).start()

    def arrive(self):
        self.partner(1 - self.c).wait_recv()
        for core in range(2):
            self.second(1, self.at(2), core).wait_recv()
            self.second(-1, self.at(2), core).wait_recv()

    def drain(self):
        self.partner(self.c).wait_send()
        for core in range(2):
            self.first(1, core, self.y, self.c).wait_send()
            self.first(-1, core, self.y, self.c).wait_send()
            self.second(1, self.y, core).wait_send()
            self.second(-1, self.y, core).wait_send()


class WeightColumn:
    def __init__(self, wk, wv, out, send, recv):
        self.parts, self.out, self.send, self.recv = (wk, wv), out, send, recv
        self.y, self.x = lax.axis_index("y"), lax.axis_index("x")

    def lanes(self, y):
        return pl.ds(pl.multiple_of(y * 128, 128), 128)

    def copy(self, k, i, slot_y):
        to = lax.rem(self.y + k, 4)
        return pltpu.make_async_remote_copy(
            src_ref=self.parts[i].at[:, self.lanes(to)],
            dst_ref=self.out.at[to, self.x, slot_y, :, pl.ds(128 * i, 128)],
            send_sem=self.send.at[0],
            recv_sem=self.recv.at[0],
            device_id={"y": to},
            device_id_type=MESH,
        )

    def start(self):
        for k in (2, 1, 3):
            for i in range(2):
                self.copy(k, i, self.y).start()
        for i in range(2):
            block = self.parts[i][:, self.lanes(self.y)]
            self.out[self.y, self.x, self.y, :, 128 * i : 128 * i + 128] = block

    def others(self):
        return bulk(self.out.at[0, 0, pl.ds(0, 3)], self.send, self.recv)

    def arrive(self):
        self.others().wait_recv()

    def drain(self):
        self.others().wait_send()


def unit_rows(matrix, gain):
    wide = matrix.astype(F32)
    factor = lax.rsqrt(jnp.mean(wide * wide, axis=-1, keepdims=True) + EPSILON)
    return wide * factor * gain


def swap_halves(a):
    return pltpu.roll(a, HD, 1)


class StrideGather:
    def __init__(self, nz, blocks, send, recv):
        self.nz, self.blocks, self.send, self.recv = nz, blocks, send, recv
        self.z = lax.axis_index("z")
        self.rows = blocks.shape[1] // PIECES
        self.far = nz // 2

    def at(self, offset):
        return lax.rem(self.z + offset + self.nz, self.nz)

    def pieces(self, sign, distance):
        if distance < self.far:
            return range(PIECES)
        half = PIECES // 2
        return range(half) if sign > 0 else range(half, PIECES)

    def copy(self, sign, distance, d, p):
        ref = self.blocks.at[self.at(-sign * distance), pl.ds(p * self.rows, self.rows)]
        return pltpu.make_async_remote_copy(
            src_ref=ref,
            dst_ref=ref,
            send_sem=self.send.at[0],
            recv_sem=self.recv.at[0 if sign > 0 else 1, distance + d - 1, p],
            device_id={"z": self.at(sign * d)},
            device_id_type=MESH,
        )

    def arrived(self, sign, distance, p):
        ref = self.blocks.at[self.at(-sign * distance), pl.ds(p * self.rows, self.rows)]
        return pltpu.make_async_remote_copy(
            src_ref=ref,
            dst_ref=ref,
            send_sem=self.send.at[0],
            recv_sem=self.recv.at[0 if sign > 0 else 1, distance - 1, p],
            device_id={"z": self.at(sign)},
            device_id_type=MESH,
        )

    def start(self):
        for d in (2, 1):
            for p in range(PIECES):
                for sign in (1, -1):
                    self.copy(sign, 0, d, p).start()

    def relay(self, distance):
        for p in range(PIECES):
            for sign in (1, -1):
                self.arrived(sign, distance, p).wait_recv()
                if p in self.pieces(sign, distance + 2):
                    self.copy(sign, distance, 2, p).start()
        for p in range(PIECES):
            for sign in (1, -1):
                self.copy(sign, distance, 1, p).start()

    def arrive(self, distance):
        for sign in (1, -1):
            for p in self.pieces(sign, distance):
                self.arrived(sign, distance, p).wait_recv()

    def drain(self):
        bulk(self.blocks.at[pl.ds(0, self.nz - 1)], self.send, self.send).wait_send()


class StrideSum:
    def __init__(self, nz, term, out, arrived, send, recv):
        self.nz, self.term, self.out, self.arrived = nz, term, out, arrived
        self.send, self.recv = send, recv
        self.rows = out.shape[2] // PIECES
        self.z = lax.axis_index("z")

    def pieces(self, side, j):
        half = PIECES // 2
        return range(PIECES) if j else range(side * half, side * half + half)

    def hop(self, side, j, p):
        at = pl.ds(p * self.rows, self.rows)
        d = (1 if j % 2 else 2) * (1 if side else -1)
        return pltpu.make_async_remote_copy(
            src_ref=self.out.at[side, j, at],
            dst_ref=self.arrived.at[side, j, at],
            send_sem=self.send.at[side if j else 2 + side],
            recv_sem=self.recv.at[side, j, p],
            device_id={"z": lax.rem(self.z + d + self.nz, self.nz)},
            device_id_type=MESH,
        )

    def joined(self, side, j, p, value):
        at = pl.ds(p * self.rows, self.rows)
        for i in (j - 1, j - 2):
            if i >= 0 and p in self.pieces(side, i):
                self.hop(side, i, p).wait_recv()
                value = value + self.arrived[side, i, at].astype(F32)
        return value

    def step(self, j):
        for p in range(PIECES):
            for side in range(2):
                if p in self.pieces(side, j):
                    at = pl.ds(p * self.rows, self.rows)
                    value = self.term(side, j, at)
                    if j % 2 == 0:
                        value = self.joined(side, j, p, value)
                    self.out[side, j, at] = value.astype(BF16)
                    self.hop(side, j, p).start()

    def total(self, p):
        half = self.nz // 2
        value = self.term(0, half, pl.ds(p * self.rows, self.rows))
        return self.joined(1, half, p, self.joined(0, half, p, value))

    def drain(self):
        half = self.nz // 2
        for side in range(2):
            sem = self.send.at[pl.ds(side, 1)]
            bulk(self.out.at[side, pl.ds(0, half - 1)], sem, sem).wait_send()
            sem = self.send.at[pl.ds(2 + side, 1)]
            bulk(self.out.at[side, 0, pl.ds(0, self.rows * (PIECES // 2))], sem, sem).wait_send()


class FarGather:
    def __init__(self, nz, src, dst, send, recv):
        self.nz, self.src, self.dst, self.send, self.recv = nz, src, dst, send, recv
        self.z = lax.axis_index("z")
        self.far = {1: nz // 2 - REACH, -1: nz - 1 - nz // 2 - REACH}

    def at(self, offset):
        return lax.rem(self.z + offset + self.nz, self.nz)

    def copy(self, slot, sign, d, relay):
        kind = 3 if relay else 2 if d < REACH else 0 if sign > 0 else 1
        return pltpu.make_async_remote_copy(
            src_ref=self.dst.at[slot] if relay else self.src,
            dst_ref=self.dst.at[slot],
            send_sem=self.send.at[0],
            recv_sem=self.recv.at[kind],
            device_id={"z": self.at(sign * d)},
            device_id_type=MESH,
        )

    def several(self, count, kind):
        return bulk(self.dst.at[pl.ds(0, count)], self.send, self.recv.at[pl.ds(kind, 1)])

    def start(self):
        for d in range(REACH, 0, -1):
            for sign in (1, -1):
                self.copy(self.z, sign, d, False).start()
        self.dst[self.z] = self.src[...]

    def relay(self):
        for sign in (1, -1):
            slot = self.at(-sign * REACH)
            self.copy(slot, sign, REACH, False).wait_recv()
            for d in range(self.far[sign], 0, -1):
                self.copy(slot, sign, d, True).start()

    def arrive(self):
        self.several(2 * REACH - 2, 2).wait_recv()
        self.several(self.nz - 1 - 2 * REACH, 3).wait_recv()

    def drain(self):
        self.several(self.nz - 1, 0).wait_send()


def reach_greet(nz):
    z = lax.axis_index("z")
    for d in range(1, REACH + 1):
        for sign in (1, -1):
            pl.semaphore_signal(
                pltpu.get_barrier_semaphore(),
                inc=1,
                device_id={"z": lax.rem(z + sign * d + nz, nz)},
                device_id_type=MESH,
            )
    return 2 * REACH


def sems(*shape):
    return pltpu.SemaphoreType.DMA(shape)


def norm_back(matrix, gain, upstream):
    wide = matrix.astype(F32)
    factor = lax.rsqrt(jnp.mean(wide * wide, axis=-1, keepdims=True) + EPSILON)
    weighted = upstream * gain
    inner = jnp.mean(weighted * wide, axis=-1, keepdims=True)
    return factor * weighted - wide * factor**3 * inner


def kernel(
    nz, target_rows_h, source_rows_h, t_gain_h, s_gain_h, wq_h, wk_h, wv_h, wo_h, cot_h, pick_h, pick8_h,
    s_out, t_out, all_sums,
    target_rows, source_rows, t_gain, s_gain, wk, wv, cot, pick, pick8, loads,
    pair, kv_all, stats, out, qa, t_all, pair_all, w_all,
    halves, rows_all, part, part_all, block, blocks, m, l, o, said, heard,
    dq, mine, ring_out, ring_in, w_ring_out, w_ring_in, outs, dq_block, dqs, o_part, swapped,
    mine_sum, kv_grad, grads8, parts, d_parts, s_in, t_in,
    row_s, row_r, wy_s, wy_r, wx_s, wx_r, wf_s, wf_r, ya_s, ya_r, xb_s, xb_r, xa_s, xa_r, yb_s, yb_r, pair_s, pair_r,
    part_s, part_r, q_s, q_r, z_s, z_r, ss, sr,
    o_s, o_r, dq_s, dq_r, sw_s, sw_r, g_s, g_r, h_s, h_r, back_s, back_r,
    kv_s, kv_r, s_s, s_r, t_s, t_r,
):
    z, y, x, c = (lax.axis_index(a) for a in "zyxc")
    met = greet(("y", "x", "c")) + reach_greet(nz)

    staged = (
        (source_rows_h, source_rows), (s_gain_h, s_gain), (wk_h, wk), (wv_h, wv),
        (target_rows_h, target_rows), (t_gain_h, t_gain), (cot_h, cot),
        (wq_h, pair.at[pl.ds(0, HD)]), (wo_h, pair.at[pl.ds(HD, HD)]), (pick_h, pick), (pick8_h, pick8),
    )
    copies = [pltpu.make_async_copy(a, b, loads.at[i]) for i, (a, b) in enumerate(staged)]
    for copy in copies:
        copy.start()
    for copy in copies[:2]:
        copy.wait()
    normed = unit_rows(source_rows[...], s_gain[...])
    low = lanes_below((32, 128), HD)
    for j in range(8):
        chip = (2 * j % 4) * 4 + j // 2
        first, second = (normed[:, 128 * i : 128 * i + 128] for i in (chip, chip + 4))
        halves[0, :, 128 * j : 128 * j + 128] = jnp.where(low, first, swap_halves(second)).astype(BF16)
        halves[1, :, 128 * j : 128 * j + 128] = jnp.where(low, swap_halves(first), second).astype(BF16)
    for copy in copies[2:]:
        copy.wait()
    greeted(met)

    by_rows = RowGather(halves, rows_all, row_s, row_r)
    by_wy = WeightColumn(wk, wv, w_all, wy_s, wy_r)
    by_wx = RingGather(
        "x", lambda slot, p: w_all.at[y, slot, p], 4, w_all.at[y, pl.ds(0, 3)], wx_s, wx_r
    )
    by_wf = RingGather("y", lambda slot, p: w_all.at[slot, p], 4, w_all.at[pl.ds(0, 3)], wf_s, wf_r)
    three, first, second = pl.ds(0, 3), pl.ds(0, 1024), pl.ds(1024, 1024)
    by_ya = RingGather(
        "y", lambda slot, p: t_all.at[x, slot, :, pl.ds(512 * p, 512)], 2,
        t_all.at[x, three, :, first], ya_s, ya_r,
    )
    by_xb = RingGather(
        "x", lambda slot, p: t_all.at[slot, y, :, pl.ds(1024 + 512 * p, 512)], 2,
        t_all.at[three, y, :, second], xb_s, xb_r,
    )
    by_xa = RingGather(
        "x", lambda slot, p: t_all.at[slot, p, :, first], 4, t_all.at[three, :, :, first], xa_s, xa_r
    )
    by_yb = RingGather(
        "y", lambda slot, p: t_all.at[p, slot, :, second], 4, t_all.at[:, three, :, second], yb_s, yb_r
    )
    by_pair = Exchange(("c",), pair, pair_all, pair_s, pair_r)
    by_wy.start()
    by_rows.start()
    zero = jnp.zeros((2, target_rows.shape[1]), F32)
    t_all[x, y] = jnp.concatenate(
        [unit_rows(target_rows[...], t_gain[...]), zero, cot[...].astype(F32), zero], axis=0
    ).astype(BF16)
    for p in range(2):
        by_xb.start(p)
        by_ya.start(p)
    by_pair.start()

    by_wy.arrive()
    for p in range(4):
        by_wx.start(p)
    by_rows.relay()
    for p in range(4):
        by_wx.relay(p)
    for p in range(2):
        by_xb.relay(p)
        by_ya.relay(p)
    for p in range(2):
        by_xb.arrive(p)
        by_ya.arrive(p)
    for p in range(4):
        by_xa.start(p)
        by_yb.start(p)
    by_rows.arrive()
    for p in range(4):
        by_wx.arrive(p)

    rows = rows_all[...].reshape(256, 1024)
    kv2 = jnp.dot(rows, w_all[y].reshape(1024, 256), preferred_element_type=F32)
    k2, v2 = kv2[:, :128], kv2[:, 128:]
    wide_low = lanes_below((256, 128), HD)
    part[0] = jnp.where(wide_low, k2, swap_halves(v2))
    part[1] = jnp.where(wide_low, swap_halves(k2), v2)
    by_part = Exchange(("c",), part, part_all, part_s, part_r, lambda at, i: i)
    by_part.start()
    by_part.arrive()
    kv_all[z] = (part_all[0] + part_all[1]).astype(BF16)

    by_z = StrideGather(nz, kv_all, z_s, z_r)
    by_z.start()
    for p in range(4):
        by_xa.relay(p)
        by_yb.relay(p)
    for p in range(4):
        by_wf.start(p)
    by_z.relay(2)
    by_pair.arrive()
    for p in range(4):
        by_xa.arrive(p)
        by_yb.arrive(p)
    everything = t_all[...].reshape(256, 2048)
    wide = lax.broadcasted_iota(jnp.int32, (256, 256), 1)
    scale = jnp.where(lax.rem(wide, 128) < HD, HD**-0.5, 1.0)
    projected = contract(everything, pair_all[...].reshape(256, 2048), 1, 1) * scale
    chosen = jnp.dot(pick[...], projected.astype(BF16), preferred_element_type=F32)
    narrow = lanes_below((96, 128), HD)
    for a in range(2):
        at = slice(128 * a, 128 * a + 128)
        block[96 * a : 96 * a + 96] = jnp.where(narrow, chosen[:96, at], chosen[96:, at]).astype(BF16)
    by_q = ToReaders(block, blocks, q_s, q_r)
    by_q.start()
    by_z.relay(4)
    m[...] = jnp.full(m.shape, -1e30, F32)
    l[...] = jnp.zeros(l.shape, F32)
    o[...] = jnp.zeros(o.shape, F32)
    by_q.arrive()
    qa[...] = blocks[...].reshape(qa.shape)

    def blocks_of(planes):
        return jnp.concatenate([kv_all[at] for at in planes], axis=0)

    def attend(*planes):
        block = blocks_of(planes)
        keys = jnp.where(lanes_below(block.shape, HD), block, jnp.zeros_like(block))
        scores = contract(keys, qa[...], 1, 1)
        top = jnp.maximum(m[...], jnp.max(scores, axis=0, keepdims=True))
        weights = jnp.exp(scores - top)
        old = jnp.exp(m[...] - top)
        m[...] = top
        l[...] = l[...] * old + jnp.sum(weights, axis=0, keepdims=True)
        o[...] = o[...] * old + contract(block, weights.astype(BF16), 0, 0)[HD:]

    def attend_from(low, high):
        def one(d, carry):
            attend(lax.rem(z + d, nz), lax.rem(z + nz - d, nz))
            return carry

        lax.fori_loop(low, high + 1, one, 0)

    attend(z)
    by_z.arrive(1)
    attend_from(1, 2)
    by_z.relay(6)
    by_z.arrive(3)
    by_z.arrive(5)
    attend_from(3, 6)
    by_z.arrive(7)
    by_z.arrive(8)
    attend_from(7, 7)
    attend(lax.rem(z + nz // 2, nz))
    upright = jnp.transpose(qa[...].astype(F32))
    delta = jnp.sum(upright[HD:] * o[...], axis=0, keepdims=True)
    row = lax.broadcasted_iota(jnp.int32, (8, qa.shape[0]), 0)
    said[...] = jnp.where(row == 0, m[...], jnp.where(row == 1, l[...], delta))
    by_stats = Exchange(("x",), said, heard, ss, sr)
    by_stats.start()
    log_sum = m[...] + jnp.log(l[...])
    high = log_sum.astype(BF16)
    rest = log_sum - high.astype(F32)
    middle = rest.astype(BF16)
    low_part = rest - middle.astype(F32)
    line = lax.broadcasted_iota(jnp.int32, (HD, qa.shape[0]), 0)
    parts3 = jnp.where(line == 0, high.astype(F32), jnp.where(line == 1, middle.astype(F32), low_part))
    upright = jnp.concatenate([o[...] / l[...], jnp.where(line < 3, parts3, 0.0)], axis=0)
    out[...] = jnp.transpose(upright).astype(BF16).reshape(out.shape)
    by_o = ToOwners(out, outs, o_s, o_r)
    by_o.start()
    for p in range(4):
        by_wf.relay(p)
    by_stats.arrive()
    top = jnp.max(heard[:, 0:1], axis=0)
    total = jnp.zeros_like(top)
    both = jnp.zeros_like(top)
    for j in range(4):
        w = jnp.exp(heard[j, 0:1] - top)
        total = total + w * heard[j, 1:2]
        both = both + w * heard[j, 2:3]
    stats[...] = jnp.where(row == 0, top + jnp.log(total), both / total)
    dq[...] = jnp.zeros(dq.shape, F32)

    def plane_of(side, j):
        offset = nz // 2 - j if side else j - nz // 2
        return lax.rem(z + nz + offset, nz)

    def grads(*terms):
        block = blocks_of([plane_of(side, j) for side, j in terms])
        low = lanes_below(block.shape, HD)
        none = jnp.zeros_like(block)
        scores = contract(jnp.where(low, block, none), qa[...], 1, 1)
        probs = jnp.exp(scores - stats[0:1])
        d_probs = contract(jnp.where(low, none, block), qa[...], 1, 1)
        d_scores = (probs * (d_probs - stats[1:2])).astype(BF16)
        for_v = contract(probs.astype(BF16), qa[...], 1, 0)
        for_k = contract(d_scores, qa[...], 1, 0)
        dq[...] += contract(block, d_scores, 0, 0)[:HD]
        both = jnp.where(low, for_k, for_v)
        for i, (side, j) in enumerate(terms):
            mine[j, side] = both[256 * i : 256 * i + 256]

    def both_grads(low, high):
        def one(j, carry):
            grads((0, j), (1, j))
            return carry

        lax.fori_loop(low, high + 1, one, 0)

    main = StrideSum(
        nz, lambda side, j, at: mine[j, side if j else 0, at], ring_out, ring_in, g_s, g_r
    )

    def own_weight(side, j, at):
        to = plane_of(side, j)
        return swapped[0, to, at].astype(F32) + swapped[1, to, at].astype(F32)

    weight = StrideSum(nz, own_weight, w_ring_out, w_ring_in, h_s, h_r)

    grads((0, 0))
    main.step(0)
    by_o.arrive()
    lanes = lax.broadcasted_iota(jnp.int32, (192, 128), 1)
    given = [outs[i].astype(F32) for i in range(4)]
    log_sums = [
        jnp.sum(jnp.where(jnp.logical_and(lanes >= HD, lanes < HD + 3), g, 0.0), axis=1, keepdims=True)
        for g in given
    ]
    largest = functools.reduce(jnp.maximum, log_sums)
    shares = [jnp.exp(part_sum - largest) for part_sum in log_sums]
    whole_sum = sum(g * w for g, w in zip(given, shares)) / sum(shares)
    attended = jnp.where(lanes < HD, whole_sum, 0.0).astype(BF16)
    for a in range(2):
        spread = contract(pick[96:], attended[96 * a : 96 * a + 96], 0, 0).astype(BF16)
        product = contract(spread, t_all[...].reshape(256, 2048), 0, 0)[:HD].astype(BF16)
        for i in range(nz):
            o_part[a, i] = product[:, 128 * i : 128 * i + 128]
    swap = Exchange(("c",), o_part, swapped, sw_s, sw_r, lambda at, i: i)
    swap.start()
    both_grads(1, 1)
    main.step(1)
    both_grads(2, 2)
    swap.arrive()
    for j in (0, 1, 3, 5, 7):
        weight.step(j)
    both_grads(3, 3)
    main.step(2)
    main.step(3)
    both_grads(5, 5)
    main.step(5)
    weight.step(2)
    both_grads(7, 7)
    main.step(7)
    both_grads(4, 4)
    both_grads(6, 6)
    grads((0, nz // 2))
    upright = jnp.concatenate([dq[...], jnp.zeros_like(dq[...])], axis=0) * HD**-0.5
    straight = jnp.transpose(upright)
    for i in range(4):
        first_head, second_head = (straight[192 * i + 96 * a : 192 * i + 96 * a + 96] for a in range(2))
        dq_block[i] = (first_head + swap_halves(second_head)).astype(BF16)
    by_dq = ToOwners(dq_block, dqs, dq_s, dq_r)
    by_dq.start()
    main.step(4)
    weight.step(4)
    main.step(6)
    weight.step(6)
    by_dq.arrive()
    query_grad = jnp.sum(dqs[...].astype(F32), axis=0).astype(BF16)
    spread = contract(pick8[...], query_grad, 0, 0).astype(BF16)
    heads = jnp.concatenate([pair_all[a, :HD] for a in range(2)], axis=0)
    d_target = jnp.dot(spread, heads, preferred_element_type=F32)
    d_parts[...] = d_target.astype(BF16).reshape(16, 8, 2048)
    by_t = Exchange(("x", "y"), d_parts, t_in, t_s, t_r, lambda at, i: i)
    by_t.start()
    for p in range(PIECES):
        mine_sum[pl.ds(32 * p, 32)] = weight.total(p).astype(BF16)
    back = FarGather(nz, mine_sum, all_sums, back_s, back_r)
    back.start()
    for p in range(4):
        by_wf.arrive(p)
    for p in range(PIECES):
        kv_grad[2 * p : 2 * p + 2] = main.total(p).astype(BF16).reshape(2, 64, 128)
    by_kv = Exchange(("y", "c"), kv_grad, grads8, kv_s, kv_r, lambda at, i: at["y"])
    by_kv.start()
    back.relay()
    by_kv.arrive()
    narrow = lanes_below((64, 128), HD)
    d_rows = jnp.zeros((64, 1024), F32)
    for i in range(4):
        g0, g1 = grads8[2 * i].astype(F32), grads8[2 * i + 1].astype(F32)
        k2 = jnp.where(narrow, g0, swap_halves(g1)).astype(BF16)
        v2 = jnp.where(narrow, swap_halves(g0), g1).astype(BF16)
        kv2 = jnp.concatenate([k2, v2], axis=1)
        d_rows = d_rows + contract(kv2, w_all[i].reshape(1024, 256), 1, 1)
    parts[...] = d_rows.astype(BF16).reshape(2, 32, 1024)
    by_s = Exchange(("c",), parts, s_in, s_s, s_r, lambda at, i: i)
    by_s.start()
    by_t.arrive()
    t_out[...] = jnp.sum(t_in[...].astype(F32), axis=0)
    by_s.arrive()
    got = [s_in[core].astype(F32) for core in range(2)]
    for j in range(8):
        chip = (2 * j % 4) * 4 + j // 2
        a, b = (g[:, 128 * j : 128 * j + 128] for g in got)
        s_out[:, 128 * chip : 128 * chip + 128] = jnp.where(low, a, swap_halves(b))
        s_out[:, 128 * chip + 512 : 128 * chip + 640] = jnp.where(low, swap_halves(a), b)
    back.arrive()
    for by in (by_rows, by_wy, by_wx, by_wf, by_ya, by_xb, by_xa, by_yb, by_pair, by_part, by_q, by_z, by_stats):
        by.drain()
    for by in (by_o, by_dq, swap, back, by_kv, by_s, by_t, main, weight):
        by.drain()


def whole(args, nz):
    t = 768
    half = nz // 2

    def bf16(*shape):
        return pltpu.VMEM(shape, BF16)

    def f32(*shape):
        return pltpu.VMEM(shape, F32)

    return pl.pallas_call(
        functools.partial(kernel, nz),
        out_shape=(
            jax.ShapeDtypeStruct((32, 2048), F32),
            jax.ShapeDtypeStruct((8, 2048), F32),
            jax.ShapeDtypeStruct((nz, HD, 128), BF16),
        ),
        in_specs=[pl.BlockSpec(memory_space=pl.ANY)] * len(args),
        out_specs=(VMEM,) * 3,
        scratch_shapes=[
            bf16(6, 2048), bf16(32, 2048), f32(1, 2048), f32(1, 2048), bf16(64, 512), bf16(64, 512),
            bf16(6, 2048), bf16(192, 256), bf16(96, 128), dma(len(args)),
            bf16(128, 2048), bf16(nz, 256, 128), f32(8, t), bf16(4, 192, 128), bf16(t, 128),
            bf16(4, 4, 16, 2048), bf16(2, 128, 2048), bf16(4, 4, 4, 64, 256),
            bf16(2, 32, 1024), bf16(4, 2, 32, 1024), f32(2, 256, 128), f32(2, 256, 128),
            bf16(192, 128), bf16(4, 192, 128), f32(1, t), f32(1, t), f32(HD, t), f32(8, t), f32(4, 8, t),
            f32(HD, t), f32(half + 1, 2, 256, 128), bf16(2, half, 256, 128), bf16(2, half, 256, 128),
            bf16(2, half, HD, 128), bf16(2, half, HD, 128),
            bf16(4, 192, 128), bf16(4, 96, 128), bf16(4, 96, 128),
            bf16(2, nz, HD, 128), bf16(2, nz, HD, 128), bf16(HD, 128), bf16(4, 64, 128), bf16(8, 64, 128), bf16(2, 32, 1024), bf16(16, 8, 2048),
            bf16(2, 32, 1024), bf16(16, 8, 2048),
            sems(5, 2), sems(5, 2), dma(1), dma(1), dma(1), sems(3, 4), dma(1), sems(3, 4),
            dma(1), sems(3, 2), dma(1), sems(3, 2), dma(1), sems(3, 4), dma(1), sems(3, 4), dma(1), dma(1),
            dma(1), dma(1), dma(4), dma(4), dma(1), sems(2, half, PIECES), dma(1), dma(1),
            dma(4), dma(4), dma(4), dma(4), dma(1), dma(1),
            dma(4), sems(2, half, PIECES), dma(4), sems(2, half, PIECES),
            dma(1), dma(4), dma(1), dma(1), dma(1), dma(1), dma(1), dma(1),
        ],
        compiler_params=params(0),
    )(*args)


def finish_kernel(
    d_source, d_target, sums, target_rows, source_rows, t_gain, s_gain, cot, t_out, s_out, w_out
):
    t_out[...] = cot[...].astype(F32) + norm_back(target_rows[...], t_gain[...], d_target[:6])
    s_out[...] = norm_back(source_rows[...], s_gain[...], d_source[...])
    for i in range(sums.shape[0]):
        w_out[:, 128 * i : 128 * i + 128] = sums[i].astype(F32)


def finish(*args):
    return pl.pallas_call(
        finish_kernel,
        out_shape=(
            jax.ShapeDtypeStruct((6, 2048), F32),
            jax.ShapeDtypeStruct((32, 2048), F32),
            jax.ShapeDtypeStruct((64, 2048), F32),
        ),
        in_specs=[VMEM] * len(args),
        out_specs=(VMEM,) * 3,
    )(*args)


def picks():
    r = np.arange(96)
    at = 16 * (r // 6) + r % 6
    pick = np.concatenate([at, at + 8])[:, None] == np.arange(256)[None]
    pick8 = (8 * (r // 6) + r % 6)[:, None] == np.arange(128)[None]
    return jnp.asarray(pick.astype(BF16)), jnp.asarray(pick8.astype(BF16))


def body(nz, target_rows, source_rows, t_gain, s_gain, wq, wk, wv, wo, cot):
    gains = (t_gain[None], s_gain[None])
    d_source, d_target, sums = whole(
        (target_rows, source_rows, *gains, wq.T, wk, wv, wo, cot, *picks()), nz
    )
    return finish(d_source, d_target, sums, target_rows, source_rows, *gains, cot)


def solution(mesh):
    nz = mesh.shape["sp"]
    SIZES["z"] = nz
    fine = Mesh(mesh.devices.reshape(nz, 4, 4, 2), ("z", "y", "x", "c"))
    every, plane = ("z", "y", "x", "c"), ("y", "x", "c")
    return jax.shard_map(
        functools.partial(body, nz),
        mesh=fine,
        in_specs=(
            P(every, None), P(every, None), P(), P(),
            P(None, plane), P(plane, None), P(plane, None), P(plane, None), P(every, None),
        ),
        out_specs=(P(every, None), P(every, None), P(plane, None)),
        check_vma=False,
    )
```

```python
import functools

import jax
import jax.numpy as jnp
import numpy as np
from jax import lax
from jax.experimental import pallas as pl
from jax.experimental.pallas import tpu as pltpu
from jax.sharding import Mesh
from jax.sharding import PartitionSpec as P

MESH = pl.DeviceIdType.MESH
HD = 64
EPSILON = 1e-06
F32, BF16 = jnp.float32, jnp.bfloat16
VMEM = pl.BlockSpec(memory_space=pltpu.VMEM)
SIZES = {"y": 4, "x": 4, "c": 2}
PIECES = 2
REACH = 4


def dma(n):
    return pltpu.SemaphoreType.DMA((n,))


def params(cid):
    return pltpu.CompilerParams(
        collective_id=cid, has_side_effects=True, vmem_limit_bytes=62 * 1024 * 1024
    )


def group_size(axes):
    n = 1
    for a in axes:
        n *= SIZES[a]
    return n


def group_index(axes):
    i = 0
    for a in axes:
        i = i * SIZES[a] + lax.axis_index(a)
    return i


def coords_of(index, axes):
    out = {}
    for a in reversed(axes):
        out[a] = lax.rem(index, SIZES[a])
        index = index // SIZES[a]
    return out


def greet(axes):
    n, me = group_size(axes), group_index(axes)
    sem = pltpu.get_barrier_semaphore()

    def one(k, carry):
        pl.semaphore_signal(
            sem, inc=1, device_id=coords_of(lax.rem(me + k, n), axes), device_id_type=MESH
        )
        return carry

    lax.fori_loop(1, n, one, 0)
    return n - 1


def greeted(count):
    pl.semaphore_wait(pltpu.get_barrier_semaphore(), count)


class Exchange:
    def __init__(self, axes, src, dst, send, recv, pick=None):
        self.axes, self.src, self.dst, self.send, self.recv = axes, src, dst, send, recv
        self.n, self.me = group_size(axes), group_index(axes)
        self.pick = pick

    def block(self, index):
        if self.pick is None:
            return self.src
        return self.src.at[self.pick(coords_of(index, self.axes), index)]

    def copy(self, k, slot):
        to = lax.rem(self.me + k, self.n)
        return pltpu.make_async_remote_copy(
            src_ref=self.block(to),
            dst_ref=self.dst.at[slot],
            send_sem=self.send.at[0],
            recv_sem=self.recv.at[0],
            device_id=coords_of(to, self.axes),
            device_id_type=MESH,
        )

    def start(self):
        def one(k, carry):
            self.copy(k, self.me).start()
            return carry

        lax.fori_loop(1, self.n, one, 0)
        self.dst[self.me] = self.block(self.me)[...]

    def others(self):
        return bulk(self.dst.at[pl.ds(0, self.n - 1)], self.send, self.recv)

    def arrive(self):
        self.others().wait_recv()

    def drain(self):
        self.others().wait_send()


def bulk(ref, send, recv):
    return pltpu.make_async_remote_copy(
        src_ref=ref,
        dst_ref=ref,
        send_sem=send.at[0],
        recv_sem=recv.at[0],
        device_id={"c": 1 - lax.axis_index("c")},
        device_id_type=MESH,
    )


class ToReaders:
    def __init__(self, src, dst, send, recv):
        self.src, self.dst, self.send, self.recv = src, dst, send, recv
        self.y, self.x, self.c = (lax.axis_index(a) for a in "yxc")
        self.mine = self.x // 2 == self.c

    def copy(self, k, slot):
        return pltpu.make_async_remote_copy(
            src_ref=self.src,
            dst_ref=self.dst.at[slot],
            send_sem=self.send.at[k],
            recv_sem=self.recv.at[slot],
            device_id={"x": lax.rem(self.x + k, 4), "c": self.x // 2},
            device_id_type=MESH,
        )

    def slot(self):
        return lax.rem(self.x, 2) * 2 + self.c

    def start(self):
        for k in range(1, 4):
            self.copy(k, self.slot()).start()

        @pl.when(jnp.logical_not(self.mine))
        def _():
            self.copy(0, self.slot()).start()

        @pl.when(self.mine)
        def _():
            self.dst[self.slot()] = self.src[...]

    def arrive(self):
        for s in range(4):
            own = jnp.logical_and(2 * self.c + s // 2 == self.x, self.c == s % 2)

            @pl.when(jnp.logical_not(own))
            def _():
                self.copy(1, s).wait_recv()

    def drain(self):
        for k in range(1, 4):
            self.copy(k, self.slot()).wait_send()

        @pl.when(jnp.logical_not(self.mine))
        def _():
            self.copy(0, self.slot()).wait_send()


class ToOwners:
    def __init__(self, src, dst, send, recv):
        self.src, self.dst, self.send, self.recv = src, dst, send, recv
        self.y, self.x, self.c = (lax.axis_index(a) for a in "yxc")

    def copy(self, s, slot):
        return pltpu.make_async_remote_copy(
            src_ref=self.src.at[s],
            dst_ref=self.dst.at[slot],
            send_sem=self.send.at[s],
            recv_sem=self.recv.at[slot],
            device_id={"x": 2 * self.c + s // 2, "c": jnp.int32(s % 2)},
            device_id_type=MESH,
        )

    def own(self, s):
        return jnp.logical_and(2 * self.c + s // 2 == self.x, self.c == s % 2)

    def start(self):
        for s in range(4):
            @pl.when(jnp.logical_not(self.own(s)))
            def _():
                self.copy(s, self.x).start()

            @pl.when(self.own(s))
            def _():
                self.dst[self.x] = self.src[s]

    def arrive(self):
        for j in range(4):
            own = jnp.logical_and(self.x == j, self.x // 2 == self.c)

            @pl.when(jnp.logical_not(own))
            def _():
                self.copy(0, j).wait_recv()

    def drain(self):
        for s in range(4):
            @pl.when(jnp.logical_not(self.own(s)))
            def _():
                self.copy(s, self.x).wait_send()


def lanes_below(shape, bound):
    return lax.broadcasted_iota(jnp.int32, shape, 1) < bound


def contract(a, b, da, db):
    return lax.dot_general(a, b, (((da,), (db,)), ((), ())), preferred_element_type=F32)


def ring_greet(nz):
    z = lax.axis_index("z")
    sem = pltpu.get_barrier_semaphore()
    right, left = lax.rem(z + 1, nz), lax.rem(z + nz - 1, nz)
    for to in (left, right):
        pl.semaphore_signal(sem, inc=1, device_id={"z": to}, device_id_type=MESH)
    return 2


class RingGather:
    def __init__(self, axis, piece, count, three, send, recv):
        self.axis, self.piece, self.count, self.send, self.recv = axis, piece, count, send, recv
        self.three = three
        self.me = lax.axis_index(axis)

    def at(self, offset):
        return lax.rem(self.me + offset + 4, 4)

    def copy(self, slot, p, sign, kind):
        ref = self.piece(slot, p)
        return pltpu.make_async_remote_copy(
            src_ref=ref,
            dst_ref=ref,
            send_sem=self.send.at[0],
            recv_sem=self.recv.at[kind, p],
            device_id={self.axis: self.at(sign)},
            device_id_type=MESH,
        )

    def start(self, p):
        self.copy(self.me, p, 1, 0).start()
        self.copy(self.me, p, -1, 1).start()

    def relay(self, p):
        self.copy(self.at(-1), p, 1, 0).wait_recv()
        self.copy(self.at(1), p, -1, 1).wait_recv()
        if p < self.count // 2:
            self.copy(self.at(-1), p, 1, 2).start()
        else:
            self.copy(self.at(1), p, -1, 2).start()

    def arrive(self, p):
        self.copy(self.at(2), p, 1, 2).wait_recv()

    def drain(self):
        bulk(self.three, self.send, self.send).wait_send()


class RowGather:
    def __init__(self, halves, out, send, recv):
        self.halves, self.out, self.send, self.recv = halves, out, send, recv
        self.y, self.c = lax.axis_index("y"), lax.axis_index("c")

    def at(self, offset):
        return lax.rem(self.y + offset + 4, 4)

    def first(self, sign, core, slot_y, slot_c):
        kind = 0 if sign > 0 else 1
        return pltpu.make_async_remote_copy(
            src_ref=self.halves.at[core],
            dst_ref=self.out.at[slot_y, slot_c],
            send_sem=self.send.at[kind, core],
            recv_sem=self.recv.at[kind, slot_c],
            device_id={"y": self.at(sign), "c": jnp.int32(core)},
            device_id_type=MESH,
        )

    def partner(self, slot_c):
        return pltpu.make_async_remote_copy(
            src_ref=self.halves.at[1 - self.c],
            dst_ref=self.out.at[self.y, slot_c],
            send_sem=self.send.at[4, 0],
            recv_sem=self.recv.at[4, 0],
            device_id={"c": 1 - self.c},
            device_id_type=MESH,
        )

    def second(self, sign, slot_y, slot_c):
        kind = 2 if sign > 0 else 3
        ref = self.out.at[slot_y, slot_c, pl.ds(0 if sign > 0 else 16, 16)]
        return pltpu.make_async_remote_copy(
            src_ref=ref,
            dst_ref=ref,
            send_sem=self.send.at[kind, slot_c],
            recv_sem=self.recv.at[kind, slot_c],
            device_id={"y": self.at(sign)},
            device_id_type=MESH,
        )

    def start(self):
        for core in range(2):
            self.first(1, core, self.y, self.c).start()
            self.first(-1, core, self.y, self.c).start()
        self.partner(self.c).start()
        self.out[self.y, self.c] = self.halves[self.c]

    def relay(self):
        for core in range(2):
            self.first(1, 0, self.at(-1), core).wait_recv()
            self.second(1, self.at(-1), core).start()
            self.first(-1, 0, self.at(1), core).wait_recv()
            self.second(-1, self.at(1), core).start()

    def arrive(self):
        self.partner(1 - self.c).wait_recv()
        for core in range(2):
            self.second(1, self.at(2), core).wait_recv()
            self.second(-1, self.at(2), core).wait_recv()

    def drain(self):
        self.partner(self.c).wait_send()
        for core in range(2):
            self.first(1, core, self.y, self.c).wait_send()
            self.first(-1, core, self.y, self.c).wait_send()
            self.second(1, self.y, core).wait_send()
            self.second(-1, self.y, core).wait_send()


class WeightColumn:
    def __init__(self, wk, wv, out, send, recv):
        self.parts, self.out, self.send, self.recv = (wk, wv), out, send, recv
        self.y, self.x = lax.axis_index("y"), lax.axis_index("x")

    def lanes(self, y):
        return pl.ds(pl.multiple_of(y * 128, 128), 128)

    def copy(self, k, i, slot_y):
        to = lax.rem(self.y + k, 4)
        return pltpu.make_async_remote_copy(
            src_ref=self.parts[i].at[:, self.lanes(to)],
            dst_ref=self.out.at[to, self.x, slot_y, :, pl.ds(128 * i, 128)],
            send_sem=self.send.at[0],
            recv_sem=self.recv.at[0],
            device_id={"y": to},
            device_id_type=MESH,
        )

    def start(self):
        for k in (2, 1, 3):
            for i in range(2):
                self.copy(k, i, self.y).start()
        for i in range(2):
            block = self.parts[i][:, self.lanes(self.y)]
            self.out[self.y, self.x, self.y, :, 128 * i : 128 * i + 128] = block

    def others(self):
        return bulk(self.out.at[0, 0, pl.ds(0, 3)], self.send, self.recv)

    def arrive(self):
        self.others().wait_recv()

    def drain(self):
        self.others().wait_send()


def unit_rows(matrix, gain):
    wide = matrix.astype(F32)
    factor = lax.rsqrt(jnp.mean(wide * wide, axis=-1, keepdims=True) + EPSILON)
    return wide * factor * gain


def swap_halves(a):
    return pltpu.roll(a, HD, 1)


class StrideGather:
    def __init__(self, nz, blocks, send, recv):
        self.nz, self.blocks, self.send, self.recv = nz, blocks, send, recv
        self.z = lax.axis_index("z")
        self.rows = blocks.shape[1] // PIECES
        self.far = nz // 2

    def at(self, offset):
        return lax.rem(self.z + offset + self.nz, self.nz)

    def pieces(self, sign, distance):
        if distance < self.far:
            return range(PIECES)
        half = PIECES // 2
        return range(half) if sign > 0 else range(half, PIECES)

    def copy(self, sign, distance, d, p):
        ref = self.blocks.at[self.at(-sign * distance), pl.ds(p * self.rows, self.rows)]
        return pltpu.make_async_remote_copy(
            src_ref=ref,
            dst_ref=ref,
            send_sem=self.send.at[0],
            recv_sem=self.recv.at[0 if sign > 0 else 1, distance + d - 1, p],
            device_id={"z": self.at(sign * d)},
            device_id_type=MESH,
        )

    def arrived(self, sign, distance, p):
        ref = self.blocks.at[self.at(-sign * distance), pl.ds(p * self.rows, self.rows)]
        return pltpu.make_async_remote_copy(
            src_ref=ref,
            dst_ref=ref,
            send_sem=self.send.at[0],
            recv_sem=self.recv.at[0 if sign > 0 else 1, distance - 1, p],
            device_id={"z": self.at(sign)},
            device_id_type=MESH,
        )

    def start(self):
        for d in (2, 1):
            for p in range(PIECES):
                for sign in (1, -1):
                    self.copy(sign, 0, d, p).start()

    def relay(self, distance):
        for p in range(PIECES):
            for sign in (1, -1):
                self.arrived(sign, distance, p).wait_recv()
                if p in self.pieces(sign, distance + 2):
                    self.copy(sign, distance, 2, p).start()
        for p in range(PIECES):
            for sign in (1, -1):
                self.copy(sign, distance, 1, p).start()

    def arrive(self, distance):
        for sign in (1, -1):
            for p in self.pieces(sign, distance):
                self.arrived(sign, distance, p).wait_recv()

    def drain(self):
        bulk(self.blocks.at[pl.ds(0, self.nz - 1)], self.send, self.send).wait_send()


class StrideSum:
    def __init__(self, nz, term, out, arrived, send, recv):
        self.nz, self.term, self.out, self.arrived = nz, term, out, arrived
        self.send, self.recv = send, recv
        self.rows = out.shape[2] // PIECES
        self.z = lax.axis_index("z")

    def pieces(self, side, j):
        half = PIECES // 2
        return range(PIECES) if j else range(side * half, side * half + half)

    def hop(self, side, j, p):
        at = pl.ds(p * self.rows, self.rows)
        d = (1 if j % 2 else 2) * (1 if side else -1)
        return pltpu.make_async_remote_copy(
            src_ref=self.out.at[side, j, at],
            dst_ref=self.arrived.at[side, j, at],
            send_sem=self.send.at[side if j else 2 + side],
            recv_sem=self.recv.at[side, j, p],
            device_id={"z": lax.rem(self.z + d + self.nz, self.nz)},
            device_id_type=MESH,
        )

    def joined(self, side, j, p, value):
        at = pl.ds(p * self.rows, self.rows)
        for i in (j - 1, j - 2):
            if i >= 0 and p in self.pieces(side, i):
                self.hop(side, i, p).wait_recv()
                value = value + self.arrived[side, i, at].astype(F32)
        return value

    def step(self, j):
        for p in range(PIECES):
            for side in range(2):
                if p in self.pieces(side, j):
                    at = pl.ds(p * self.rows, self.rows)
                    value = self.term(side, j, at)
                    if j % 2 == 0:
                        value = self.joined(side, j, p, value)
                    self.out[side, j, at] = value.astype(BF16)
                    self.hop(side, j, p).start()

    def total(self, p):
        half = self.nz // 2
        value = self.term(0, half, pl.ds(p * self.rows, self.rows))
        return self.joined(1, half, p, self.joined(0, half, p, value))

    def drain(self):
        half = self.nz // 2
        for side in range(2):
            sem = self.send.at[pl.ds(side, 1)]
            bulk(self.out.at[side, pl.ds(0, half - 1)], sem, sem).wait_send()
            sem = self.send.at[pl.ds(2 + side, 1)]
            bulk(self.out.at[side, 0, pl.ds(0, self.rows * (PIECES // 2))], sem, sem).wait_send()


class FarGather:
    def __init__(self, nz, src, dst, send, recv):
        self.nz, self.src, self.dst, self.send, self.recv = nz, src, dst, send, recv
        self.z = lax.axis_index("z")
        self.far = {1: nz // 2 - REACH, -1: nz - 1 - nz // 2 - REACH}

    def at(self, offset):
        return lax.rem(self.z + offset + self.nz, self.nz)

    def copy(self, slot, sign, d, relay):
        kind = 3 if relay else 2 if d < REACH else 0 if sign > 0 else 1
        return pltpu.make_async_remote_copy(
            src_ref=self.dst.at[slot] if relay else self.src,
            dst_ref=self.dst.at[slot],
            send_sem=self.send.at[0],
            recv_sem=self.recv.at[kind],
            device_id={"z": self.at(sign * d)},
            device_id_type=MESH,
        )

    def several(self, count, kind):
        return bulk(self.dst.at[pl.ds(0, count)], self.send, self.recv.at[pl.ds(kind, 1)])

    def start(self):
        for d in range(REACH, 0, -1):
            for sign in (1, -1):
                self.copy(self.z, sign, d, False).start()
        self.dst[self.z] = self.src[...]

    def relay(self):
        for sign in (1, -1):
            slot = self.at(-sign * REACH)
            self.copy(slot, sign, REACH, False).wait_recv()
            for d in range(self.far[sign], 0, -1):
                self.copy(slot, sign, d, True).start()

    def arrive(self):
        self.several(2 * REACH - 2, 2).wait_recv()
        self.several(self.nz - 1 - 2 * REACH, 3).wait_recv()

    def drain(self):
        self.several(self.nz - 1, 0).wait_send()


def reach_greet(nz):
    z = lax.axis_index("z")
    for d in range(1, REACH + 1):
        for sign in (1, -1):
            pl.semaphore_signal(
                pltpu.get_barrier_semaphore(),
                inc=1,
                device_id={"z": lax.rem(z + sign * d + nz, nz)},
                device_id_type=MESH,
            )
    return 2 * REACH


def sems(*shape):
    return pltpu.SemaphoreType.DMA(shape)


def norm_back(matrix, gain, upstream):
    wide = matrix.astype(F32)
    factor = lax.rsqrt(jnp.mean(wide * wide, axis=-1, keepdims=True) + EPSILON)
    weighted = upstream * gain
    inner = jnp.mean(weighted * wide, axis=-1, keepdims=True)
    return factor * weighted - wide * factor**3 * inner


def kernel(
    nz, target_rows_h, source_rows_h, t_gain_h, s_gain_h, wq_h, wk_h, wv_h, wo_h, cot_h, pick_h, pick8_h,
    s_out, t_out, all_sums,
    target_rows, source_rows, t_gain, s_gain, wk, wv, cot, pick, pick8, loads,
    pair, kv_all, stats, out, qa, t_all, pair_all, w_all,
    halves, rows_all, part, part_all, block, blocks, m, l, o, said, heard,
    dq, mine, ring_out, ring_in, w_ring_out, w_ring_in, outs, dq_block, dqs, o_part, swapped,
    mine_sum, kv_grad, grads8, parts, d_parts, s_in, t_in,
    row_s, row_r, wy_s, wy_r, wx_s, wx_r, wf_s, wf_r, ya_s, ya_r, xb_s, xb_r, xa_s, xa_r, yb_s, yb_r, pair_s, pair_r,
    part_s, part_r, q_s, q_r, z_s, z_r, ss, sr,
    o_s, o_r, dq_s, dq_r, sw_s, sw_r, g_s, g_r, h_s, h_r, back_s, back_r,
    kv_s, kv_r, s_s, s_r, t_s, t_r,
):
    z, y, x, c = (lax.axis_index(a) for a in "zyxc")
    met = greet(("y", "x", "c")) + reach_greet(nz)

    staged = (
        (source_rows_h, source_rows), (s_gain_h, s_gain), (wk_h, wk), (wv_h, wv),
        (target_rows_h, target_rows), (t_gain_h, t_gain), (cot_h, cot),
        (wq_h, pair.at[pl.ds(0, HD)]), (wo_h, pair.at[pl.ds(HD, HD)]), (pick_h, pick), (pick8_h, pick8),
    )
    copies = [pltpu.make_async_copy(a, b, loads.at[i]) for i, (a, b) in enumerate(staged)]
    for copy in copies:
        copy.start()
    for copy in copies[:2]:
        copy.wait()
    normed = unit_rows(source_rows[...], s_gain[...])
    low = lanes_below((32, 128), HD)
    for j in range(8):
        chip = (2 * j % 4) * 4 + j // 2
        first, second = (normed[:, 128 * i : 128 * i + 128] for i in (chip, chip + 4))
        halves[0, :, 128 * j : 128 * j + 128] = jnp.where(low, first, swap_halves(second)).astype(BF16)
        halves[1, :, 128 * j : 128 * j + 128] = jnp.where(low, swap_halves(first), second).astype(BF16)
    for copy in copies[2:]:
        copy.wait()
    greeted(met)

    by_rows = RowGather(halves, rows_all, row_s, row_r)
    by_wy = WeightColumn(wk, wv, w_all, wy_s, wy_r)
    by_wx = RingGather(
        "x", lambda slot, p: w_all.at[y, slot, p], 4, w_all.at[y, pl.ds(0, 3)], wx_s, wx_r
    )
    by_wf = RingGather("y", lambda slot, p: w_all.at[slot, p], 4, w_all.at[pl.ds(0, 3)], wf_s, wf_r)
    three, first, second = pl.ds(0, 3), pl.ds(0, 1024), pl.ds(1024, 1024)
    by_ya = RingGather(
        "y", lambda slot, p: t_all.at[x, slot, :, pl.ds(512 * p, 512)], 2,
        t_all.at[x, three, :, first], ya_s, ya_r,
    )
    by_xb = RingGather(
        "x", lambda slot, p: t_all.at[slot, y, :, pl.ds(1024 + 512 * p, 512)], 2,
        t_all.at[three, y, :, second], xb_s, xb_r,
    )
    by_xa = RingGather(
        "x", lambda slot, p: t_all.at[slot, p, :, first], 4, t_all.at[three, :, :, first], xa_s, xa_r
    )
    by_yb = RingGather(
        "y", lambda slot, p: t_all.at[p, slot, :, second], 4, t_all.at[:, three, :, second], yb_s, yb_r
    )
    by_pair = Exchange(("c",), pair, pair_all, pair_s, pair_r)
    by_wy.start()
    by_rows.start()
    zero = jnp.zeros((2, target_rows.shape[1]), F32)
    t_all[x, y] = jnp.concatenate(
        [unit_rows(target_rows[...], t_gain[...]), zero, cot[...].astype(F32), zero], axis=0
    ).astype(BF16)
    for p in range(2):
        by_xb.start(p)
        by_ya.start(p)
    by_pair.start()

    by_wy.arrive()
    for p in range(4):
        by_wx.start(p)
    by_rows.relay()
    for p in range(4):
        by_wx.relay(p)
    for p in range(2):
        by_xb.relay(p)
        by_ya.relay(p)
    for p in range(2):
        by_xb.arrive(p)
        by_ya.arrive(p)
    for p in range(4):
        by_xa.start(p)
        by_yb.start(p)
    by_rows.arrive()
    for p in range(4):
        by_wx.arrive(p)

    rows = rows_all[...].reshape(256, 1024)
    kv2 = jnp.dot(rows, w_all[y].reshape(1024, 256), preferred_element_type=F32)
    k2, v2 = kv2[:, :128], kv2[:, 128:]
    wide_low = lanes_below((256, 128), HD)
    part[0] = jnp.where(wide_low, k2, swap_halves(v2))
    part[1] = jnp.where(wide_low, swap_halves(k2), v2)
    by_part = Exchange(("c",), part, part_all, part_s, part_r, lambda at, i: i)
    by_part.start()
    by_part.arrive()
    kv_all[z] = (part_all[0] + part_all[1]).astype(BF16)

    by_z = StrideGather(nz, kv_all, z_s, z_r)
    by_z.start()
    for p in range(4):
        by_xa.relay(p)
        by_yb.relay(p)
    for p in range(4):
        by_wf.start(p)
    by_z.relay(2)
    by_pair.arrive()
    for p in range(4):
        by_xa.arrive(p)
        by_yb.arrive(p)
    everything = t_all[...].reshape(256, 2048)
    wide = lax.broadcasted_iota(jnp.int32, (256, 256), 1)
    scale = jnp.where(lax.rem(wide, 128) < HD, HD**-0.5, 1.0)
    projected = contract(everything, pair_all[...].reshape(256, 2048), 1, 1) * scale
    chosen = jnp.dot(pick[...], projected.astype(BF16), preferred_element_type=F32)
    narrow = lanes_below((96, 128), HD)
    for a in range(2):
        at = slice(128 * a, 128 * a + 128)
        block[96 * a : 96 * a + 96] = jnp.where(narrow, chosen[:96, at], chosen[96:, at]).astype(BF16)
    by_q = ToReaders(block, blocks, q_s, q_r)
    by_q.start()
    by_z.relay(4)
    m[...] = jnp.full(m.shape, -1e30, F32)
    l[...] = jnp.zeros(l.shape, F32)
    o[...] = jnp.zeros(o.shape, F32)
    by_q.arrive()
    qa[...] = blocks[...].reshape(qa.shape)

    def blocks_of(planes):
        return jnp.concatenate([kv_all[at] for at in planes], axis=0)

    def attend(*planes):
        block = blocks_of(planes)
        keys = jnp.where(lanes_below(block.shape, HD), block, jnp.zeros_like(block))
        scores = contract(keys, qa[...], 1, 1)
        top = jnp.maximum(m[...], jnp.max(scores, axis=0, keepdims=True))
        weights = jnp.exp(scores - top)
        old = jnp.exp(m[...] - top)
        m[...] = top
        l[...] = l[...] * old + jnp.sum(weights, axis=0, keepdims=True)
        o[...] = o[...] * old + contract(block, weights.astype(BF16), 0, 0)[HD:]

    def attend_from(low, high):
        def one(d, carry):
            attend(lax.rem(z + d, nz), lax.rem(z + nz - d, nz))
            return carry

        lax.fori_loop(low, high + 1, one, 0)

    attend(z)
    by_z.arrive(1)
    attend_from(1, 2)
    by_z.relay(6)
    by_z.arrive(3)
    by_z.arrive(5)
    attend_from(3, 6)
    by_z.arrive(7)
    by_z.arrive(8)
    attend(*(lax.rem(z + nz + d, nz) for d in (7, -7, nz // 2)))
    upright = jnp.transpose(qa[...].astype(F32))
    delta = jnp.sum(upright[HD:] * o[...], axis=0, keepdims=True)
    row = lax.broadcasted_iota(jnp.int32, (8, qa.shape[0]), 0)
    said[...] = jnp.where(row == 0, m[...], jnp.where(row == 1, l[...], delta))
    by_stats = Exchange(("x",), said, heard, ss, sr)
    by_stats.start()
    log_sum = m[...] + jnp.log(l[...])
    high = log_sum.astype(BF16)
    rest = log_sum - high.astype(F32)
    middle = rest.astype(BF16)
    low_part = rest - middle.astype(F32)
    line = lax.broadcasted_iota(jnp.int32, (HD, qa.shape[0]), 0)
    parts3 = jnp.where(line == 0, high.astype(F32), jnp.where(line == 1, middle.astype(F32), low_part))
    upright = jnp.concatenate([o[...] / l[...], jnp.where(line < 3, parts3, 0.0)], axis=0)
    out[...] = jnp.transpose(upright).astype(BF16).reshape(out.shape)
    by_o = ToOwners(out, outs, o_s, o_r)
    by_o.start()
    for p in range(4):
        by_wf.relay(p)
    by_stats.arrive()
    top = jnp.max(heard[:, 0:1], axis=0)
    total = jnp.zeros_like(top)
    both = jnp.zeros_like(top)
    for j in range(4):
        w = jnp.exp(heard[j, 0:1] - top)
        total = total + w * heard[j, 1:2]
        both = both + w * heard[j, 2:3]
    stats[...] = jnp.where(row == 0, top + jnp.log(total), both / total)
    dq[...] = jnp.zeros(dq.shape, F32)

    def plane_of(side, j):
        offset = nz // 2 - j if side else j - nz // 2
        return lax.rem(z + nz + offset, nz)

    def grads(*terms):
        block = blocks_of([plane_of(side, j) for side, j in terms])
        low = lanes_below(block.shape, HD)
        none = jnp.zeros_like(block)
        scores = contract(jnp.where(low, block, none), qa[...], 1, 1)
        probs = jnp.exp(scores - stats[0:1])
        d_probs = contract(jnp.where(low, none, block), qa[...], 1, 1)
        d_scores = (probs * (d_probs - stats[1:2])).astype(BF16)
        for_v = contract(probs.astype(BF16), qa[...], 1, 0)
        for_k = contract(d_scores, qa[...], 1, 0)
        dq[...] += contract(block, d_scores, 0, 0)[:HD]
        both = jnp.where(low, for_k, for_v)
        for i, (side, j) in enumerate(terms):
            mine[j, side] = both[256 * i : 256 * i + 256]

    def both_grads(low, high):
        def one(j, carry):
            grads((0, j), (1, j))
            return carry

        lax.fori_loop(low, high + 1, one, 0)

    main = StrideSum(
        nz, lambda side, j, at: mine[j, side if j else 0, at], ring_out, ring_in, g_s, g_r
    )

    def own_weight(side, j, at):
        to = plane_of(side, j)
        return swapped[0, to, at].astype(F32) + swapped[1, to, at].astype(F32)

    weight = StrideSum(nz, own_weight, w_ring_out, w_ring_in, h_s, h_r)

    grads((0, 0))
    main.step(0)
    by_o.arrive()
    lanes = lax.broadcasted_iota(jnp.int32, (192, 128), 1)
    given = [outs[i].astype(F32) for i in range(4)]
    log_sums = [
        jnp.sum(jnp.where(jnp.logical_and(lanes >= HD, lanes < HD + 3), g, 0.0), axis=1, keepdims=True)
        for g in given
    ]
    largest = functools.reduce(jnp.maximum, log_sums)
    shares = [jnp.exp(part_sum - largest) for part_sum in log_sums]
    whole_sum = sum(g * w for g, w in zip(given, shares)) / sum(shares)
    attended = jnp.where(lanes < HD, whole_sum, 0.0).astype(BF16)
    for a in range(2):
        spread = contract(pick[96:], attended[96 * a : 96 * a + 96], 0, 0).astype(BF16)
        product = contract(spread, t_all[...].reshape(256, 2048), 0, 0)[:HD].astype(BF16)
        for i in range(nz):
            o_part[a, i] = product[:, 128 * i : 128 * i + 128]
    swap = Exchange(("c",), o_part, swapped, sw_s, sw_r, lambda at, i: i)
    swap.start()
    both_grads(1, 1)
    main.step(1)
    both_grads(2, 2)
    swap.arrive()
    for j in (0, 1, 3, 5, 7):
        weight.step(j)
    both_grads(3, 3)
    main.step(2)
    main.step(3)
    both_grads(5, 5)
    main.step(5)
    weight.step(2)
    both_grads(7, 7)
    main.step(7)
    both_grads(4, 4)
    both_grads(6, 6)
    grads((0, nz // 2))
    upright = jnp.concatenate([dq[...], jnp.zeros_like(dq[...])], axis=0) * HD**-0.5
    straight = jnp.transpose(upright)
    for i in range(4):
        first_head, second_head = (straight[192 * i + 96 * a : 192 * i + 96 * a + 96] for a in range(2))
        dq_block[i] = (first_head + swap_halves(second_head)).astype(BF16)
    by_dq = ToOwners(dq_block, dqs, dq_s, dq_r)
    by_dq.start()
    main.step(4)
    weight.step(4)
    main.step(6)
    weight.step(6)
    by_dq.arrive()
    query_grad = jnp.sum(dqs[...].astype(F32), axis=0).astype(BF16)
    spread = contract(pick8[...], query_grad, 0, 0).astype(BF16)
    heads = jnp.concatenate([pair_all[a, :HD] for a in range(2)], axis=0)
    d_target = jnp.dot(spread, heads, preferred_element_type=F32)
    d_parts[...] = d_target.astype(BF16).reshape(16, 8, 2048)
    by_t = Exchange(("x", "y"), d_parts, t_in, t_s, t_r, lambda at, i: i)
    by_t.start()
    for p in range(PIECES):
        mine_sum[pl.ds(32 * p, 32)] = weight.total(p).astype(BF16)
    back = FarGather(nz, mine_sum, all_sums, back_s, back_r)
    back.start()
    for p in range(4):
        by_wf.arrive(p)
    for p in range(PIECES):
        kv_grad[2 * p : 2 * p + 2] = main.total(p).astype(BF16).reshape(2, 64, 128)
    by_kv = Exchange(("y", "c"), kv_grad, grads8, kv_s, kv_r, lambda at, i: at["y"])
    by_kv.start()
    for by in (by_rows, by_wy, by_wx, by_wf, by_ya, by_xb, by_xa, by_yb, by_pair, by_part, by_q, by_z, by_stats):
        by.drain()
    back.relay()
    by_kv.arrive()
    narrow = lanes_below((64, 128), HD)
    d_rows = jnp.zeros((64, 1024), F32)
    for i in range(4):
        g0, g1 = grads8[2 * i].astype(F32), grads8[2 * i + 1].astype(F32)
        k2 = jnp.where(narrow, g0, swap_halves(g1)).astype(BF16)
        v2 = jnp.where(narrow, swap_halves(g0), g1).astype(BF16)
        kv2 = jnp.concatenate([k2, v2], axis=1)
        d_rows = d_rows + contract(kv2, w_all[i].reshape(1024, 256), 1, 1)
    parts[...] = d_rows.astype(BF16).reshape(2, 32, 1024)
    by_s = Exchange(("c",), parts, s_in, s_s, s_r, lambda at, i: i)
    by_s.start()
    by_t.arrive()
    t_out[...] = jnp.sum(t_in[...].astype(F32), axis=0)
    by_s.arrive()
    got = [s_in[core].astype(F32) for core in range(2)]
    for j in range(8):
        chip = (2 * j % 4) * 4 + j // 2
        a, b = (g[:, 128 * j : 128 * j + 128] for g in got)
        s_out[:, 128 * chip : 128 * chip + 128] = jnp.where(low, a, swap_halves(b))
        s_out[:, 128 * chip + 512 : 128 * chip + 640] = jnp.where(low, swap_halves(a), b)
    back.arrive()
    for by in (by_o, by_dq, swap, back, by_kv, by_s, by_t, main, weight):
        by.drain()


def whole(args, nz):
    t = 768
    half = nz // 2

    def bf16(*shape):
        return pltpu.VMEM(shape, BF16)

    def f32(*shape):
        return pltpu.VMEM(shape, F32)

    return pl.pallas_call(
        functools.partial(kernel, nz),
        out_shape=(
            jax.ShapeDtypeStruct((32, 2048), F32),
            jax.ShapeDtypeStruct((8, 2048), F32),
            jax.ShapeDtypeStruct((nz, HD, 128), BF16),
        ),
        in_specs=[pl.BlockSpec(memory_space=pl.ANY)] * len(args),
        out_specs=(VMEM,) * 3,
        scratch_shapes=[
            bf16(6, 2048), bf16(32, 2048), f32(1, 2048), f32(1, 2048), bf16(64, 512), bf16(64, 512),
            bf16(6, 2048), bf16(192, 256), bf16(96, 128), dma(len(args)),
            bf16(128, 2048), bf16(nz, 256, 128), f32(8, t), bf16(4, 192, 128), bf16(t, 128),
            bf16(4, 4, 16, 2048), bf16(2, 128, 2048), bf16(4, 4, 4, 64, 256),
            bf16(2, 32, 1024), bf16(4, 2, 32, 1024), f32(2, 256, 128), f32(2, 256, 128),
            bf16(192, 128), bf16(4, 192, 128), f32(1, t), f32(1, t), f32(HD, t), f32(8, t), f32(4, 8, t),
            f32(HD, t), f32(half + 1, 2, 256, 128), bf16(2, half, 256, 128), bf16(2, half, 256, 128),
            bf16(2, half, HD, 128), bf16(2, half, HD, 128),
            bf16(4, 192, 128), bf16(4, 96, 128), bf16(4, 96, 128),
            bf16(2, nz, HD, 128), bf16(2, nz, HD, 128), bf16(HD, 128), bf16(4, 64, 128), bf16(8, 64, 128), bf16(2, 32, 1024), bf16(16, 8, 2048),
            bf16(2, 32, 1024), bf16(16, 8, 2048),
            sems(5, 2), sems(5, 2), dma(1), dma(1), dma(1), sems(3, 4), dma(1), sems(3, 4),
            dma(1), sems(3, 2), dma(1), sems(3, 2), dma(1), sems(3, 4), dma(1), sems(3, 4), dma(1), dma(1),
            dma(1), dma(1), dma(4), dma(4), dma(1), sems(2, half, PIECES), dma(1), dma(1),
            dma(4), dma(4), dma(4), dma(4), dma(1), dma(1),
            dma(4), sems(2, half, PIECES), dma(4), sems(2, half, PIECES),
            dma(1), dma(4), dma(1), dma(1), dma(1), dma(1), dma(1), dma(1),
        ],
        compiler_params=params(0),
    )(*args)


def finish_kernel(
    d_source, d_target, sums, target_rows, source_rows, t_gain, s_gain, cot, t_out, s_out, w_out
):
    t_out[...] = cot[...].astype(F32) + norm_back(target_rows[...], t_gain[...], d_target[:6])
    s_out[...] = norm_back(source_rows[...], s_gain[...], d_source[...])
    for i in range(sums.shape[0]):
        w_out[:, 128 * i : 128 * i + 128] = sums[i].astype(F32)


def finish(*args):
    return pl.pallas_call(
        finish_kernel,
        out_shape=(
            jax.ShapeDtypeStruct((6, 2048), F32),
            jax.ShapeDtypeStruct((32, 2048), F32),
            jax.ShapeDtypeStruct((64, 2048), F32),
        ),
        in_specs=[VMEM] * len(args),
        out_specs=(VMEM,) * 3,
    )(*args)


def picks():
    r = np.arange(96)
    at = 16 * (r // 6) + r % 6
    pick = np.concatenate([at, at + 8])[:, None] == np.arange(256)[None]
    pick8 = (8 * (r // 6) + r % 6)[:, None] == np.arange(128)[None]
    return jnp.asarray(pick.astype(BF16)), jnp.asarray(pick8.astype(BF16))


def body(nz, target_rows, source_rows, t_gain, s_gain, wq, wk, wv, wo, cot):
    gains = (t_gain[None], s_gain[None])
    d_source, d_target, sums = whole(
        (target_rows, source_rows, *gains, wq.T, wk, wv, wo, cot, *picks()), nz
    )
    return finish(d_source, d_target, sums, target_rows, source_rows, *gains, cot)


def solution(mesh):
    nz = mesh.shape["sp"]
    SIZES["z"] = nz
    fine = Mesh(mesh.devices.reshape(nz, 4, 4, 2), ("z", "y", "x", "c"))
    every, plane = ("z", "y", "x", "c"), ("y", "x", "c")
    return jax.shard_map(
        functools.partial(body, nz),
        mesh=fine,
        in_specs=(
            P(every, None), P(every, None), P(), P(),
            P(None, plane), P(plane, None), P(plane, None), P(plane, None), P(every, None),
        ),
        out_specs=(P(every, None), P(every, None), P(plane, None)),
        check_vma=False,
    )
```
